32 devices in a mesh: sp: 8 (over z, y), tp: 4 (over x, core).
Axes of the slice: x: 2, y: 2, z: 4, core: 2. Of those that a mesh axis runs over, the one named last changes fastest.
Arguments:
- tokens: bfloat16 [8192, 2048], P(('sp', 'tp')), may hold values from -6 to 6
- norm_gain: float32 [2048], replicated, may hold values from 0.1 to 1.9
- w_query: bfloat16 [2048, 2048], P(None, 'tp'), may hold values from -0.125 to 0.125
- w_forget: bfloat16 [2048, 2048], P(None, 'tp'), may hold values from -0.125 to 0.125
- w_value: bfloat16 [2048, 2048], P(None, 'tp'), may hold values from -0.125 to 0.125
- w_rgate: bfloat16 [2048, 2048], P(None, 'tp'), may hold values from -0.125 to 0.125
- w_glu_value: bfloat16 [2048, 2048], P(None, 'tp'), may hold values from -0.125 to 0.125
- w_glu_gate: bfloat16 [2048, 2048], P(None, 'tp'), may hold values from -0.125 to 0.125
- forget_gap: float32 [2048], P('tp'), may hold values from 6.1035156e-05 to 0.1
- decay_shift: float32 [8192, 16], P('sp', 'tp'), may hold values from -0.6 to 0, as said below
- head_gain: float32 [128], replicated, may hold values from 0.1 to 1.9
- conv_taps: float32 [31, 2048], P(None, 'tp'), may hold values from -12 to 12
- conv_gain: float32 [2048], P('tp'), may hold values from 0.1 to 1.9
- out_rec: bfloat16 [2048, 2048], P('tp'), may hold values from -0.09375 to 0.09375
- out_conv: bfloat16 [2048, 2048], P('tp'), may hold values from -0.09375 to 0.09375
Outputs:
- mixed: bfloat16 [8192, 2048], P(('sp', 'tp'))
The draws below stay inside these ranges and needn't reach their ends.
Inputs may be any that keep to these rules, and one draw needn't show every extreme that they name: `decay_shift`: at most zero everywhere.
All inputs are finite; a program needn't handle non-finite values.
Results may differ from the reference program's by a relative error of at most 0.015.
Values may be sent and summed in bfloat16 or wider, within the bound.
A program may use at most 128 MiB of HBM per device.

```python
import jax
import jax.numpy as jnp
from jax import lax

D = 2048
HEADS = 16
HEAD = 128
DC = 2048
CW = 31
BLOCK = 64
TOK_DEV = 1024
DH = 2048
TOKENS = 8192
N_TP = 4


def draw_forget_gap(key, part):
    order = jax.random.permutation(jax.random.fold_in(key, 3), HEADS)
    fast_count = HEADS // 2
    fast = order < fast_count
    spread = jax.random.uniform(jax.random.fold_in(key, 5), (HEADS, HEAD), jnp.float32)
    slow_gap = jnp.exp(jnp.log(0.5) + spread * jnp.log(3.0)) / TOKENS
    fast_gap = jnp.exp(jnp.log(0.03) + spread * jnp.log(10.0 / 3.0))
    return jnp.where(fast[:, None], fast_gap, slow_gap).reshape(HEADS * HEAD)


def draw_decay_shift(key, part):
    block_total = TOKENS // TOK_DEV
    spread = jax.random.uniform(jax.random.fold_in(key, 7), (block_total, 1), jnp.float32)
    rate = jnp.exp(jnp.log(0.2) + spread * jnp.log(5.0)) / TOKENS
    smooth_part = -jnp.repeat(rate, TOK_DEV, axis=0) * jnp.ones((1, HEADS), jnp.float32)
    positions = jax.random.randint(jax.random.fold_in(key, 11), (2,), 0, TOKENS)
    depth = jax.random.uniform(jax.random.fold_in(key, 13), (2, HEADS), jnp.float32, 0.2, 0.4)
    hits = (jnp.arange(TOKENS)[:, None] == positions[None, :]).astype(jnp.float32)
    return smooth_part + jnp.dot(hits, jnp.log(1.0 - depth))


def draw_conv_taps(key, part):
    channel_rise = jnp.exp(jnp.log(3.0) * jnp.arange(DC).astype(jnp.float32) / DC)
    base = jnp.clip(jax.random.normal(jax.random.fold_in(key, 17), (CW, DC), jnp.float32), -4.0, 4.0)
    spread = jnp.exp(jax.random.uniform(jax.random.fold_in(key, 19), (DC,), jnp.float32, 0.0, jnp.log(10.0)))
    scale = 0.1
    return base * channel_rise * spread * scale


def levels(rng, shape, split, least, top_value):
    factor_of = 1.0
    for dim, blocks in split:
        steps = jax.random.uniform(jax.random.fold_in(jax.random.fold_in(rng, 6), dim), (blocks,), jnp.float32, least / len(split), top_value / len(split))
        factor_of = factor_of * jnp.repeat(jnp.exp(steps), shape[dim] // blocks).reshape((-1,) + (1,) * (len(shape) - 1 - dim))
    return factor_of


def gaussian(rng, dims, scale, most, split=(), kind=jnp.bfloat16):
    level = levels(rng, dims, split, -0.22, 0.18) if split else 1.0
    values = jax.random.normal(rng, dims, jnp.float32) * scale * level
    return jnp.minimum(jnp.maximum(values, -most), most).astype(kind)


def setup_inputs(seed: int = 0) -> dict:
    streams_of = jax.random.split(jax.random.key(seed), 16)
    tokens = gaussian(streams_of[0], (TOKENS, D), 1.0, 6.0, ((0, 32),))
    norm_gain = jnp.clip(1.0 + 0.18 * jax.random.normal(streams_of[1], (D,), jnp.float32), 0.1, 1.9)
    w_query = gaussian(streams_of[2], (D, DH), D ** -0.5, 0.125, ((1, 4),))
    w_forget = gaussian(streams_of[3], (D, DH), D ** -0.5, 0.125, ((1, 4),))
    w_value = gaussian(streams_of[4], (D, DH), D ** -0.5, 0.125, ((1, 4),))
    w_rgate = gaussian(streams_of[5], (D, DH), D ** -0.5, 0.125, ((1, 4),))
    w_glu_value = gaussian(streams_of[6], (D, DC), D ** -0.5, 0.125, ((1, 4),))
    w_glu_gate = gaussian(streams_of[7], (D, DC), D ** -0.5, 0.125, ((1, 4),))
    forget_gap = draw_forget_gap(jax.random.fold_in(streams_of[15], 71), 0)
    decay_shift = draw_decay_shift(jax.random.fold_in(streams_of[15], 71), 0)
    head_gain = jnp.clip(1.0 + 0.18 * jax.random.normal(streams_of[10], (HEAD,), jnp.float32), 0.1, 1.9)
    conv_taps = draw_conv_taps(jax.random.fold_in(streams_of[15], 71), 0)
    conv_gain = jnp.clip(1.0 + 0.18 * jax.random.normal(streams_of[12], (DC,), jnp.float32), 0.1, 1.9)
    out_rec = gaussian(streams_of[13], (DH, D), (DH + DC) ** -0.5, 0.09375, ((0, 4),))
    out_conv = gaussian(streams_of[14], (DC, D), (DH + DC) ** -0.5, 0.09375, ((0, 4),))
    return {"tokens": tokens, "norm_gain": norm_gain, "w_query": w_query, "w_forget": w_forget, "w_value": w_value, "w_rgate": w_rgate, "w_glu_value": w_glu_value, "w_glu_gate": w_glu_gate, "forget_gap": forget_gap, "decay_shift": decay_shift, "head_gain": head_gain, "conv_taps": conv_taps, "conv_gain": conv_gain, "out_rec": out_rec, "out_conv": out_conv}


precise_setting = lax.Precision.HIGHEST
norm_epsilon = 1e-05
head_epsilon = 1e-06

def layer_norm(values, gain):
    widened = values.astype(jnp.float32)
    row_mean = lax.optimization_barrier(jnp.mean(widened, axis=-1, keepdims=True))
    centred = widened - row_mean
    row_var = lax.optimization_barrier(jnp.mean(centred * centred, axis=-1, keepdims=True))
    return centred * lax.rsqrt(row_var + norm_epsilon) * gain.astype(jnp.float32)

def block_scan(query, key_gate, values, log_forget):
    row_count, head_count, key_width = query.shape
    value_width = values.shape[2]
    block_count = row_count // BLOCK

    def to_blocks(array):
        return array.reshape(block_count, BLOCK, head_count, array.shape[2]).transpose(0, 2, 1, 3)
    causal = lax.broadcasted_iota(jnp.int32, (BLOCK, BLOCK), 0) >= lax.broadcasted_iota(jnp.int32, (BLOCK, BLOCK), 1)

    def advance(current_state, inputs):
        query_blk, key_block, value_block, log_blk = inputs
        running_total = jnp.cumsum(log_blk, axis=1)
        closing_log = running_total[:, -1:, :]
        query_decayed = query_blk * jnp.exp(running_total)
        scores = jnp.einsum('htk,hsk->hts', query_decayed, key_block * jnp.exp(-running_total), precision=precise_setting)
        scores = jnp.where(causal[None], scores, 0.0)
        output_rows = jnp.einsum('hts,hsv->htv', scores, value_block, precision=precise_setting)
        output_rows = output_rows + jnp.einsum('ori,oiq->orq', query_decayed, current_state, precision=precise_setting)
        current_state = jnp.exp(closing_log[:, 0, :])[:, :, None] * current_state + jnp.einsum('itp,ito->ipo', key_block * jnp.exp(closing_log - running_total), value_block, precision=precise_setting)
        return (current_state, output_rows)
    start_state = jnp.zeros((head_count, key_width, value_width), jnp.float32)
    final_state, output_rows = lax.scan(advance, start_state, (to_blocks(query), to_blocks(key_gate), to_blocks(values), to_blocks(log_forget)))
    return output_rows.transpose(0, 2, 1, 3).reshape(row_count, head_count, value_width)

def reference(tokens, norm_gain, w_query, w_forget, w_value, w_rgate, w_glu_value, w_glu_gate, forget_gap, decay_shift, head_gain, conv_taps, conv_gain, out_rec, out_conv):
    normed = layer_norm(tokens, norm_gain).astype(jnp.bfloat16)

    def project(weight):
        return jnp.dot(normed, weight, preferred_element_type=jnp.float32).astype(jnp.bfloat16)
    query_raw = project(w_query)
    forget_raw = project(w_forget)
    value_raw = project(w_value)
    rgate_raw = project(w_rgate)
    glu_value = project(w_glu_value)
    glu_gate = project(w_glu_gate)
    seq_len = tokens.shape[0]
    query = jax.nn.silu(query_raw.astype(jnp.float32)).reshape(seq_len, HEADS, HEAD)
    key_gate = forget_gap * jax.nn.sigmoid(-forget_raw.astype(jnp.float32))
    log_forget = jnp.log1p(-key_gate).reshape(seq_len, HEADS, HEAD) + decay_shift[:, :, None]
    values = value_raw.astype(jnp.float32).reshape(seq_len, HEADS, HEAD)
    recurrent_branch = block_scan(query, key_gate.reshape(seq_len, HEADS, HEAD), values, log_forget)
    recurrent_branch = recurrent_branch * lax.rsqrt(lax.optimization_barrier(jnp.mean(recurrent_branch * recurrent_branch, axis=-1, keepdims=True)) + head_epsilon) * head_gain
    rec_out = (recurrent_branch.reshape(seq_len, HEADS * HEAD) * jax.nn.silu(rgate_raw.astype(jnp.float32))).astype(jnp.bfloat16)
    mixed_in = (glu_value.astype(jnp.float32) * jax.nn.sigmoid(glu_gate.astype(jnp.float32))).astype(jnp.bfloat16)
    padded = lax.optimization_barrier(jnp.concatenate([jnp.zeros((CW - 1, DC), jnp.bfloat16), mixed_in], axis=0)).astype(jnp.float32)
    filtered = jnp.zeros((seq_len, DC), jnp.float32)
    for tap_index in range(CW):
        filtered = filtered + conv_taps[tap_index] * padded[tap_index:tap_index + seq_len]
    conv_out = jax.nn.silu(layer_norm(filtered, conv_gain)).astype(jnp.bfloat16)
    rec_share = HEADS * HEAD // N_TP
    conv_share = DC // N_TP
    mixed = jnp.zeros((seq_len, D), jnp.float32)
    for group in range(N_TP):
        term = jnp.dot(rec_out[:, group * rec_share:(group + 1) * rec_share], out_rec[group * rec_share:(group + 1) * rec_share], preferred_element_type=jnp.float32)
        term = term + jnp.dot(conv_out[:, group * conv_share:(group + 1) * conv_share], out_conv[group * conv_share:(group + 1) * conv_share], preferred_element_type=jnp.float32)
        mixed = mixed + lax.optimization_barrier(term.astype(jnp.bfloat16)).astype(jnp.float32)
    return mixed.astype(jnp.bfloat16)
```

```python
import functools

import jax
import jax.numpy as jnp
from jax import lax
from jax.experimental import pallas as pl
from jax.experimental.pallas import tpu as pltpu
from jax.sharding import PartitionSpec as P

CHUNK = 128
PAD = 16
SENDS = 4
RETURNS = 4
REACH = 32
TILE = 64
LANES = 128
SPAN = 512
MESH = pl.DeviceIdType.MESH
FORGET, VALUE, QUERY, GLU_VALUE, GLU_GATE, RGATE = range(6)

norm_epsilon = 1e-05
head_epsilon = 1e-06


def dot(a, b, dims=((1,), (0,))):
    return lax.dot_general(a, b, (dims, ((), ())), preferred_element_type=jnp.float32)


def exact(a, b, dims):
    return lax.dot_general(
        a, b, (dims, ((), ())), precision=lax.Precision.HIGHEST, preferred_element_type=jnp.float32
    )


def layer_norm(values, gain):
    widened = values.astype(jnp.float32)
    row_mean = jnp.mean(widened, axis=-1, keepdims=True)
    centred = widened - row_mean
    row_var = jnp.mean(centred * centred, axis=-1, keepdims=True)
    return centred * lax.rsqrt(row_var + norm_epsilon) * gain


def layer_kernel(
    head, tokens_ref, gain_ref, gap_ref, shift_ref, taps_ref, conv_gain_ref, head_gain_ref,
    w0, w1, w2, w3, w4, w5, rec_rows, conv_rows, out_ref,
    near_rows, far_rows, weight, merge, proj, intra, reach, local, closing, enter,
    own_state, own_log, pack, pack_in, group_state, group_log, chain_out, chain_in,
    rim, padded, filtered, own_stats, other_stats, moments,
    blend, held, to_pair, from_pair, to_cross, from_cross, mine, done,
    weight_sem, send_sem, recv_sem, pack_send, pack_recv, chain_send, chain_recv,
    rim_sem, stat_send, stat_recv, back_send, back_recv, out_sem,
):
    sources = (w0, w1, w2, w3, w4, w5)
    width = gap_ref.shape[1]
    fetched = [pltpu.make_async_copy(w, weight.at[i], weight_sem.at[i]) for i, w in enumerate(sources)]
    for i, w in enumerate((rec_rows, conv_rows)):
        fetched.append(
            pltpu.make_async_copy(w, merge.at[pl.ds(i * width, width), :], weight_sem.at[len(sources) + i])
        )
    for one in fetched:
        one.start()

    me, count = lax.axis_index("tp"), lax.axis_size("sp")
    pair = me + 1 - 2 * lax.rem(me, 2)
    cross, diag = lax.rem(me + 2, 4), lax.rem(pair + 2, 4)
    at = lax.axis_index("sp")
    side, team, teams = lax.rem(at, 2), at // 2, count // 2
    mate = at + 1 - 2 * side
    barrier = pltpu.get_barrier_semaphore()
    for other in (pair, cross, diag):
        pl.semaphore_signal(barrier, inc=1, device_id={"tp": other}, device_id_type=MESH)
    for hop in (1, 2, count - 1, count - 2):
        pl.semaphore_signal(barrier, inc=1, device_id={"sp": lax.rem(at + hop, count)}, device_id_type=MESH)
    pl.semaphore_wait(barrier, 7)

    block, depth = tokens_ref.shape
    rows_all = proj.shape[1]
    heads, chunks = width // head, rows_all // CHUNK
    piece = block // SENDS
    bigs = block // CHUNK
    per = CHUNK // piece
    lanes_of = [slice(g * LANES, (g + 1) * LANES) for g in range(width // LANES)]

    def remote(source, target, sends, recvs, axis, device):
        return pltpu.make_async_remote_copy(
            src_ref=source, dst_ref=target, send_sem=sends, recv_sem=recvs,
            device_id={axis: device}, device_id_type=MESH,
        )

    crossing, nearby, handed = [], [], []
    for p in range(SENDS):
        rows = pl.ds(p * piece, piece)
        near_rows[0, rows, :] = layer_norm(tokens_ref[rows, :], gain_ref[...]).astype(jnp.bfloat16)
        big, low = p // per, (p % per) * piece
        landing = far_rows.at[big, pl.ds(low, piece), :]
        crossing.append(remote(near_rows.at[0, rows, :], landing, send_sem.at[0, p], recv_sem.at[0, p], "tp", cross))
        nearby.append(
            remote(
                near_rows.at[0, rows, :], near_rows.at[1, rows, :], send_sem.at[1, p], recv_sem.at[1, p], "tp", pair
            )
        )
        handed.append(
            remote(
                landing, far_rows.at[big, pl.ds(CHUNK + low, piece), :],
                send_sem.at[2, p], recv_sem.at[2, p], "tp", pair,
            )
        )
        crossing[p].start()
        nearby[p].start()

    def project(values, first, last, places, ready=False):
        def step(i, carry):
            if ready:
                for k in range(first, last):
                    pl.when(i == k)(fetched[k].wait)
            result = dot(values[...], weight[i]).astype(jnp.bfloat16)
            for start, row, size in places:
                proj[i, pl.ds(pl.multiple_of(row, CHUNK), size), :] = result[start : start + size]
            return carry

        lax.fori_loop(first, last, step, 0)

    def pass_on(p):
        crossing[p].wait_recv()
        handed[p].start()

    row_at = lax.broadcasted_iota(jnp.int32, (CHUNK, CHUNK), 0)
    col_at = lax.broadcasted_iota(jnp.int32, (CHUNK, CHUNK), 1)
    causal = row_at >= col_at
    lower = jnp.where(causal, 1.0, 0.0).astype(jnp.bfloat16)
    lower = jnp.concatenate([lower, lower], axis=1)

    def chunk(c):
        rows = pl.ds(pl.multiple_of(c * CHUNK, CHUNK), CHUNK)
        for h in range(heads):
            part = slice(h * head, (h + 1) * head)
            query = proj[QUERY, rows, part].astype(jnp.float32)
            query = query * jax.nn.sigmoid(query)
            key = gap_ref[:, part] * jax.nn.sigmoid(-proj[FORGET, rows, part].astype(jnp.float32))
            shift = jnp.broadcast_to(shift_ref[h : h + 1, rows], (head, CHUNK)).T
            log = jnp.log1p(-key) + shift
            value = proj[VALUE, rows, part]
            high = log.astype(jnp.bfloat16)
            low = (log - high.astype(jnp.float32)).astype(jnp.bfloat16)
            total = dot(lower, jnp.concatenate([high, low], axis=0))
            last = total[CHUNK - 1 : CHUNK, :]
            middle = total[CHUNK // 2 - 1 : CHUNK // 2, :]
            query_mid = query * jnp.exp(total - middle)
            key_mid = key * jnp.exp(middle - total)
            scores = dot(query_mid.astype(jnp.bfloat16), key_mid.astype(jnp.bfloat16), ((1,), (1,)))
            scores = jnp.where(causal, scores, 0.0).astype(jnp.bfloat16)
            intra[rows, part] = dot(scores, value)
            reach[rows, part] = (query_mid * jnp.exp(middle)).astype(jnp.bfloat16)
            key_end = (key_mid * jnp.exp(last - middle)).astype(jnp.bfloat16)
            local[c, h] = dot(value, key_end, ((0,), (0,)))
            closing[c, :, part] = last

    def chunk_loop(first, number):
        def step(i, carry):
            chunk(first + i)
            return carry

        lax.fori_loop(0, number, step, 0)

    def mix(first, size):
        def step(i, carry):
            row = pl.multiple_of(first + i * TILE, TILE)
            for g, lanes in enumerate(lanes_of):
                gate = proj[GLU_GATE, pl.ds(row, TILE), lanes].astype(jnp.float32)
                value = proj[GLU_VALUE, pl.ds(row, TILE), lanes].astype(jnp.float32)
                mixed = (value * jax.nn.sigmoid(gate)).astype(jnp.bfloat16)
                padded[g, pl.ds(pl.multiple_of(row + REACH, 8), TILE), :] = mixed.astype(jnp.float32)
            return carry

        lax.fori_loop(0, size // TILE, step, 0)

    taps = taps_ref.shape[0]
    skip = REACH - taps + 1
    pick = lax.broadcasted_iota(jnp.int32, (8, LANES), 0)
    one_hot = [jnp.where(pick == k, 1.0, 0.0) for k in range(2)]

    def filter_tile(t):
        base = pl.multiple_of(t * LANES, LANES)

        def step(i, carry):
            g, row = i // (LANES // TILE), base + lax.rem(i, LANES // TILE) * TILE
            lanes = pl.ds(pl.multiple_of(g * LANES, LANES), LANES)
            total = jnp.zeros((TILE, LANES), jnp.float32)
            for j in range(taps):
                total = total + taps_ref[j : j + 1, lanes] * padded[g, pl.ds(row + (j + skip), TILE), :]
            filtered[pl.ds(pl.multiple_of(row, TILE), TILE), lanes] = total
            return carry

        lax.fori_loop(0, len(lanes_of) * (LANES // TILE), step, 0)
        sums = jnp.zeros((LANES, LANES), jnp.float32)
        squares = jnp.zeros((LANES, LANES), jnp.float32)
        for lanes in lanes_of:
            value = filtered[pl.ds(base, LANES), lanes]
            sums = sums + value
            squares = squares + value * value
        own_stats[:, pl.ds(base, LANES)] = exact(one_hot[0], sums, ((1,), (1,))) + exact(
            one_hot[1], squares, ((1,), (1,))
        )

    def filter_loop(first, number):
        def step(i, carry):
            filter_tile(first + i)
            return carry

        lax.fori_loop(0, number, step, 0)

    chip = 2 * block
    own_half = (me // 2) * chip
    far_half = chip - own_half if rows_all == 2 * chip else lax.rem(own_half + chip, rows_all)
    half_tiles = chip // LANES

    project(near_rows.at[0], 0, len(sources), [(0, me * block, block)], ready=True)
    for one in nearby:
        one.wait_recv()
    project(near_rows.at[1], 0, len(sources), [(0, pair * block, block)])
    pass_on(0)
    chunk_loop(own_half // CHUNK, chip // CHUNK)
    pass_on(1)
    mix(own_half, chip)
    filter_loop(own_half // LANES + 1, half_tiles - 1)

    def far_places(big):
        return [(0, cross * block + big * CHUNK, CHUNK), (CHUNK, diag * block + big * CHUNK, CHUNK)]

    def far_chunks(big):
        def step(i, carry):
            chunk(jnp.where(i == 0, cross, diag) * bigs + big)
            return carry

        lax.fori_loop(0, 2, step, 0)

    for big in range(bigs):
        final = big == bigs - 1
        for p in range(big * per, (big + 1) * per):
            if p > 1:
                pass_on(p)
        for p in range(big * per, (big + 1) * per):
            handed[p].wait_recv()
        if final:
            project(far_rows.at[big], 0, 3, far_places(big))
            far_chunks(big)
        else:
            project(far_rows.at[big], 0, len(sources), far_places(big))
            far_chunks(big)
            for _, row, size in far_places(big):
                mix(row, size)

    place = lax.broadcasted_iota(jnp.int32, (PAD, head), 0)
    packs = [remote(pack.at[h], pack_in.at[h], pack_send.at[h], pack_recv.at[h], "sp", mate) for h in range(heads)]
    for h in range(heads):
        part = slice(h * head, (h + 1) * head)
        state, log = local[0, h], closing[0, :, part]
        for c in range(1, chunks):
            state = state * jnp.exp(closing[c, :, part]) + local[c, h]
            log = log + closing[c, :, part]
        own_state[h] = state
        own_log[:, part] = log
        pack[h, 0:head, :] = state.astype(jnp.bfloat16)
        high = log.astype(jnp.bfloat16).astype(jnp.float32)
        rest = log - high
        mid = rest.astype(jnp.bfloat16).astype(jnp.float32)
        low = rest - mid
        tail = jnp.where(place == 0, high, jnp.where(place == 1, mid, jnp.where(place == 2, low, 0.0)))
        pack[h, head : head + PAD, :] = tail.astype(jnp.bfloat16)
        packs[h].start()

    project(far_rows.at[bigs - 1], 3, len(sources), far_places(bigs - 1))
    for _, row, size in far_places(bigs - 1):
        mix(row, size)
    for g, lanes in enumerate(lanes_of):
        rim[0, :, lanes] = padded[g, rows_all : rows_all + REACH, :].astype(jnp.bfloat16)
    edge = remote(rim.at[0], rim.at[1], rim_sem.at[0], rim_sem.at[1], "sp", lax.rem(at + 1, count))
    edge.start()

    links = [
        remote(chain_out.at[h], chain_in.at[h], chain_send.at[h], chain_recv.at[h], "sp", lax.rem(at + 2, count))
        for h in range(heads)
    ]

    def mate_log(h):
        tail = pack_in[h, head : head + PAD, :].astype(jnp.float32)
        return tail[0:1] + tail[1:2] + tail[2:3]

    for h in range(heads):
        part = slice(h * head, (h + 1) * head)
        packs[h].wait_recv()
        theirs, log = pack_in[h, 0:head, :].astype(jnp.float32), mate_log(h)
        ours, own = own_state[h], own_log[:, part]
        first = jnp.where(side == 0, ours, theirs)
        second = jnp.where(side == 0, theirs, ours)
        group_state[h] = first * jnp.exp(jnp.where(side == 0, log, own)) + second
        group_log[:, part] = log + own

        @pl.when(team == 0)
        def _():
            chain_in[h] = jnp.zeros((head, head), jnp.bfloat16)
            chain_out[h] = group_state[h].astype(jnp.bfloat16)
            links[h].start()

    def relay(k):
        @pl.when(team == k)
        def _():
            for h in range(heads):
                links[h].wait_recv()
                if k < teams - 1:
                    part = slice(h * head, (h + 1) * head)
                    step = chain_in[h].astype(jnp.float32) * jnp.exp(group_log[:, part]) + group_state[h]
                    chain_out[h] = step.astype(jnp.bfloat16)
                    links[h].start()

    far_tile = far_half // LANES

    def rim_in():
        edge.wait_recv()
        for g, lanes in enumerate(lanes_of):
            padded[g, 0:REACH, :] = jnp.where(at > 0, rim[1, :, lanes].astype(jnp.float32), 0.0)
        filter_tile(own_half // LANES)

    stats = [
        remote(own_stats, other_stats.at[k - 1], stat_send.at[k - 1], stat_recv.at[k - 1], "tp", lax.rem(me + k, 4))
        for k in range(1, 4)
    ]

    def send_stats():
        filter_tile(far_tile)
        for one in stats:
            one.start()

    work = [lambda: filter_loop(far_tile + 1, 2), lambda: filter_loop(far_tile + 3, 1), rim_in, send_stats]
    if half_tiles != 4:
        work[1] = lambda: filter_loop(far_tile + 3, half_tiles - 3)
    relays = [functools.partial(relay, k) for k in range(1, teams)]
    while work or relays:
        if work:
            work.pop(0)()
        if relays:
            relays.pop(0)()

    eye = jnp.where(pick == lax.broadcasted_iota(jnp.int32, (8, LANES), 1), 1.0, 0.0)
    for one in stats:
        one.wait_recv()

    def stats_tile(i, carry):
        row = pl.multiple_of(i * LANES, LANES)
        total = own_stats[:, pl.ds(row, LANES)]
        for k in range(3):
            total = total + other_stats[k, :, pl.ds(row, LANES)]
        moments[pl.ds(row, LANES), :] = exact(total, eye, ((0,), (0,)))
        return carry

    lax.fori_loop(0, rows_all // LANES, stats_tile, 0)

    for h in range(heads):
        part = slice(h * head, (h + 1) * head)
        state = chain_in[h].astype(jnp.float32)
        moved = state * jnp.exp(mate_log(h)) + pack_in[h, 0:head, :].astype(jnp.float32)
        state = jnp.where(side == 1, moved, state)
        for c in range(chunks):
            enter[c, h] = state.astype(jnp.bfloat16)
            if c < chunks - 1:
                state = state * jnp.exp(closing[c, :, part]) + local[c, h]

    channels = width * lax.axis_size("tp")

    def finish_rows(owner, low, size, slot):
        start = pl.multiple_of(owner * block + low, size)
        rows, c = pl.ds(start, size), owner * bigs + low // CHUNK
        target = pl.ds(slot, size)
        for h in range(heads):
            part = slice(h * head, (h + 1) * head)
            rec = intra[rows, part] + dot(reach[rows, part], enter[c, h], ((1,), (1,)))
            rec = rec * lax.rsqrt(jnp.mean(rec * rec, axis=-1, keepdims=True) + head_epsilon) * head_gain_ref[...]
            gate = proj[RGATE, rows, part].astype(jnp.float32)
            blend[target, part] = (rec * (gate * jax.nn.sigmoid(gate))).astype(jnp.bfloat16)
        row_mean = moments[rows, 0:1] / channels
        row_var = moments[rows, 1:2] / channels - row_mean * row_mean
        scale = lax.rsqrt(row_var + norm_epsilon)
        for g, lanes in enumerate(lanes_of):
            normed = (filtered[rows, lanes] - row_mean) * scale * conv_gain_ref[:, lanes]
            blend[target, width + g * LANES : width + (g + 1) * LANES] = (normed * jax.nn.sigmoid(normed)).astype(
                jnp.bfloat16
            )

    columns = merge.shape[1]

    def spread(size, put):
        def step(j, carry):
            cols = pl.ds(pl.multiple_of(j * SPAN, SPAN), SPAN)
            put(cols, dot(blend[0:size, :], merge[:, cols]))
            return carry

        lax.fori_loop(0, columns // SPAN, step, 0)

    for one in fetched[len(sources) :]:
        one.wait()
    turn = block // RETURNS
    lent, returned, close = [], [], []

    def settle(p):
        rows = pl.ds(p * turn, turn)
        lent[p].wait_recv()
        to_cross[rows, :] = (held[p % 2] + from_pair[0, rows, :].astype(jnp.float32)).astype(jnp.bfloat16)
        returned.append(
            remote(to_cross.at[rows, :], from_cross.at[rows, :], back_send.at[1, p], back_recv.at[1, p], "tp", cross)
        )
        returned[p].start()

    for p in range(RETURNS):
        rows = pl.ds(p * turn, turn)
        finish_rows(diag, p * turn, turn, 0)
        finish_rows(cross, p * turn, turn, turn)

        def put(cols, result, p=p, rows=rows):
            to_pair[0, rows, cols] = result[0:turn].astype(jnp.bfloat16)
            held[p % 2, :, cols] = result[turn : 2 * turn]

        spread(2 * turn, put)
        lent.append(
            remote(
                to_pair.at[0, rows, :], from_pair.at[0, rows, :], back_send.at[0, p], back_recv.at[0, p], "tp", pair
            )
        )
        lent[p].start()
        if p > 0:
            settle(p - 1)
    settle(RETURNS - 1)
    for big in range(bigs):
        rows = pl.ds(big * CHUNK, CHUNK)
        finish_rows(pair, big * CHUNK, CHUNK, 0)
        finish_rows(me, big * CHUNK, CHUNK, CHUNK)

        def put(cols, result, rows=rows):
            to_pair[1, rows, cols] = result[0:CHUNK].astype(jnp.bfloat16)
            mine[rows, cols] = result[CHUNK : 2 * CHUNK]

        spread(2 * CHUNK, put)
        close.append(
            remote(
                to_pair.at[1, rows, :], from_pair.at[1, rows, :], back_send.at[2, big], back_recv.at[2, big],
                "tp", pair,
            )
        )
        close[big].start()
    for big in range(bigs):
        rows = pl.ds(big * CHUNK, CHUNK)
        close[big].wait_recv()
        mine[rows, :] = mine[rows, :] + from_pair[1, rows, :].astype(jnp.float32)
    stores = []
    for p in range(RETURNS):
        rows = pl.ds(p * turn, turn)
        returned[p].wait_recv()
        done[rows, :] = (mine[rows, :] + from_cross[rows, :].astype(jnp.float32)).astype(jnp.bfloat16)
        stores.append(pltpu.make_async_copy(done.at[rows, :], out_ref.at[rows, :], out_sem.at[p]))
        stores[p].start()
    for one in crossing + nearby + handed + packs + [edge] + stats + lent + returned + close:
        one.wait_send()

    @pl.when(team < teams - 1)
    def _():
        for one in links:
            one.wait_send()

    for one in stores:
        one.wait()


def on_device(
    tokens, norm_gain, w_query, w_forget, w_value, w_rgate, w_glu_value, w_glu_gate, forget_gap,
    decay_shift, head_gain, conv_taps, conv_gain, out_rec, out_conv,
):
    weights = (w_forget, w_value, w_query, w_glu_value, w_glu_gate, w_rgate)
    block, depth = tokens.shape
    width, columns = out_rec.shape
    head = head_gain.shape[0]
    heads = width // head
    rows = block * lax.axis_size("tp")
    groups = width // LANES
    chunks = rows // CHUNK
    turn = block // RETURNS
    bf16, f32 = jnp.bfloat16, jnp.float32
    vmem = lambda shape, kind: pltpu.VMEM(shape, kind)
    sems = lambda *shape: pltpu.SemaphoreType.DMA(shape)
    return pl.pallas_call(
        functools.partial(layer_kernel, head),
        in_specs=[pl.BlockSpec(memory_space=pltpu.VMEM)] * 7 + [pl.BlockSpec(memory_space=pl.ANY)] * 8,
        out_specs=pl.BlockSpec(memory_space=pl.ANY),
        out_shape=jax.ShapeDtypeStruct((block, columns), bf16),
        scratch_shapes=[
            vmem((2, block, depth), bf16),
            vmem((block // CHUNK, 2 * CHUNK, depth), bf16),
            vmem((len(weights), depth, width), bf16),
            vmem((2 * width, columns), bf16),
            vmem((len(weights), rows, width), bf16),
            vmem((rows, width), f32),
            vmem((rows, width), bf16),
            vmem((chunks, heads, head, head), f32),
            vmem((chunks, 1, width), f32),
            vmem((chunks, heads, head, head), bf16),
            vmem((heads, head, head), f32),
            vmem((1, width), f32),
            vmem((heads, head + PAD, head), bf16),
            vmem((heads, head + PAD, head), bf16),
            vmem((heads, head, head), f32),
            vmem((1, width), f32),
            vmem((heads, head, head), bf16),
            vmem((heads, head, head), bf16),
            vmem((2, REACH, width), bf16),
            vmem((groups, REACH + rows, LANES), f32),
            vmem((rows, width), f32),
            vmem((8, rows), f32),
            vmem((3, 8, rows), f32),
            vmem((rows, LANES), f32),
            vmem((2 * CHUNK, 2 * width), bf16),
            vmem((2, turn, columns), f32),
            vmem((2, block, columns), bf16),
            vmem((2, block, columns), bf16),
            vmem((block, columns), bf16),
            vmem((block, columns), bf16),
            vmem((block, columns), f32),
            vmem((block, columns), bf16),
            sems(len(weights) + 2),
            sems(3, SENDS),
            sems(3, SENDS),
            sems(heads),
            sems(heads),
            sems(heads),
            sems(heads),
            sems(2),
            sems(3),
            sems(3),
            sems(3, RETURNS),
            sems(3, RETURNS),
            sems(RETURNS),
        ],
        compiler_params=pltpu.CompilerParams(
            collective_id=0, has_side_effects=True, vmem_limit_bytes=65000 * 1024
        ),
    )(
        tokens, norm_gain[None], forget_gap[None], decay_shift.T, conv_taps, conv_gain[None], head_gain[None],
        *weights, out_rec, out_conv,
    )


def solution(mesh):
    placed = (
        P(("sp", "tp"), None),
        P(),
        P(None, "tp"),
        P(None, "tp"),
        P(None, "tp"),
        P(None, "tp"),
        P(None, "tp"),
        P(None, "tp"),
        P("tp"),
        P("sp", "tp"),
        P(),
        P(None, "tp"),
        P("tp"),
        P("tp", None),
        P("tp", None),
    )
    return jax.shard_map(
        on_device, mesh=mesh, in_specs=placed, out_specs=P(("sp", "tp"), None), check_vma=False
    )
```

```python
import functools

import jax
import jax.numpy as jnp
from jax import lax
from jax.experimental import pallas as pl
from jax.experimental.pallas import tpu as pltpu
from jax.sharding import PartitionSpec as P

CHUNK = 128
PAD = 16
SENDS = 4
RETURNS = 4
REACH = 32
TILE = 64
LANES = 128
SPAN = 512
MESH = pl.DeviceIdType.MESH
FORGET, VALUE, QUERY, GLU_VALUE, GLU_GATE, RGATE = range(6)

norm_epsilon = 1e-05
head_epsilon = 1e-06


def dot(a, b, dims=((1,), (0,))):
    return lax.dot_general(a, b, (dims, ((), ())), preferred_element_type=jnp.float32)


def layer_norm(values, gain):
    widened = values.astype(jnp.float32)
    row_mean = jnp.mean(widened, axis=-1, keepdims=True)
    centred = widened - row_mean
    row_var = jnp.mean(centred * centred, axis=-1, keepdims=True)
    return centred * lax.rsqrt(row_var + norm_epsilon) * gain


def layer_kernel(
    head, gain_ref, gap_ref, shift_ref, taps_ref, conv_gain_ref, head_gain_ref,
    tokens_ref, w0, w1, w2, w3, w4, w5, rec_rows, conv_rows, out_ref,
    raw, near_rows, far_rows, weight, merge, proj, intra, reach, local, closing, centre, enter,
    own_state, own_log, pack, pack_in, group_state, group_log, chain_out, chain_in,
    rim, padded, filtered, own_stats, other_stats, moments,
    blend, held, to_pair, from_pair, to_cross, from_cross, mine, done,
    raw_sem, weight_sem, send_sem, recv_sem, pack_send, pack_recv, chain_send, chain_recv,
    rim_sem, stat_send, stat_recv, back_send, back_recv, out_sem,
):
    block, depth = tokens_ref.shape
    piece = block // SENDS
    raws = []
    for p in range(SENDS):
        rows = pl.ds(p * piece, piece)
        raws.append(pltpu.make_async_copy(tokens_ref.at[rows, :], raw.at[rows, :], raw_sem.at[p]))
        raws[p].start()
    sources = (w0, w1, w2, w3, w4, w5)
    width = gap_ref.shape[1]
    fetched = [pltpu.make_async_copy(w, weight.at[i], weight_sem.at[i]) for i, w in enumerate(sources)]
    for i, w in enumerate((rec_rows, conv_rows)):
        fetched.append(
            pltpu.make_async_copy(w, merge.at[pl.ds(i * width, width), :], weight_sem.at[len(sources) + i])
        )
    me, count = lax.axis_index("tp"), lax.axis_size("sp")
    pair = me + 1 - 2 * lax.rem(me, 2)
    cross, diag = lax.rem(me + 2, 4), lax.rem(pair + 2, 4)
    at = lax.axis_index("sp")
    side, team, teams = lax.rem(at, 2), at // 2, count // 2
    mate = at + 1 - 2 * side
    barrier = pltpu.get_barrier_semaphore()
    for other in (pair, cross, diag):
        pl.semaphore_signal(barrier, inc=1, device_id={"tp": other}, device_id_type=MESH)
    for hop in (1, 2, count - 1, count - 2):
        pl.semaphore_signal(barrier, inc=1, device_id={"sp": lax.rem(at + hop, count)}, device_id_type=MESH)
    pl.semaphore_wait(barrier, 7)

    rows_all = proj.shape[1]
    heads, chunks = width // head, rows_all // CHUNK
    bigs = block // CHUNK
    per = CHUNK // piece
    channels = width * lax.axis_size("tp")
    lanes_of = [slice(g * LANES, (g + 1) * LANES) for g in range(width // LANES)]

    def remote(source, target, sends, recvs, axis, device):
        return pltpu.make_async_remote_copy(
            src_ref=source, dst_ref=target, send_sem=sends, recv_sem=recvs,
            device_id={axis: device}, device_id_type=MESH,
        )

    for one in raws:
        one.wait()
    for one in fetched:
        one.start()

    crossing, nearby, handed = [], [], []
    for p in range(SENDS):
        rows = pl.ds(p * piece, piece)
        near_rows[0, rows, :] = layer_norm(raw[rows, :], gain_ref[...]).astype(jnp.bfloat16)
        big, low = p // per, (p % per) * piece
        landing = far_rows.at[big, pl.ds(low, piece), :]
        crossing.append(remote(near_rows.at[0, rows, :], landing, send_sem.at[0, p], recv_sem.at[0, p], "tp", cross))
        nearby.append(
            remote(
                near_rows.at[0, rows, :], near_rows.at[1, rows, :], send_sem.at[1, p], recv_sem.at[1, p], "tp", pair
            )
        )
        handed.append(
            remote(
                landing, far_rows.at[big, pl.ds(CHUNK + low, piece), :],
                send_sem.at[2, p], recv_sem.at[2, p], "tp", pair,
            )
        )
        crossing[p].start()
        nearby[p].start()

    def project(values, first, last, places, ready=False):
        def step(k, carry):
            for i in (first + 2 * k, first + 2 * k + 1):
                if ready:
                    for one in range(first, last):
                        pl.when(i == one)(fetched[one].wait)
            for i in (first + 2 * k, first + 2 * k + 1):
                result = dot(values[...], weight[i]).astype(jnp.bfloat16)
                for start, row, size in places:
                    proj[i, pl.ds(pl.multiple_of(row, CHUNK), size), :] = result[start : start + size]
            return carry

        lax.fori_loop(0, (last - first) // 2, step, 0)

    def pass_on(p):
        crossing[p].wait_recv()
        handed[p].start()

    row_at = lax.broadcasted_iota(jnp.int32, (CHUNK, CHUNK), 0)
    col_at = lax.broadcasted_iota(jnp.int32, (CHUNK, CHUNK), 1)
    causal = row_at >= col_at
    lower = jnp.where(causal, 1.0, 0.0).astype(jnp.bfloat16)
    lower = jnp.concatenate([lower, lower], axis=1)

    parts = [slice(h * head, (h + 1) * head) for h in range(heads)]

    def rows_of(c):
        return pl.ds(pl.multiple_of(c * CHUNK, CHUNK), CHUNK)

    def state_part(several):
        keys, totals = [], []
        for c in several:
            rows = rows_of(c)
            key = gap_ref[...] * jax.nn.sigmoid(-proj[FORGET, rows, :].astype(jnp.float32))
            shift = [jnp.broadcast_to(shift_ref[h : h + 1, rows], (head, CHUNK)).T for h in range(heads)]
            log = jnp.log1p(-key) + jnp.concatenate(shift, axis=1)
            high = log.astype(jnp.bfloat16)
            low = (log - high.astype(jnp.float32)).astype(jnp.bfloat16)
            keys.append(key)
            totals.append(dot(lower, jnp.concatenate([high, low], axis=0)))
        for c, key, total in zip(several, keys, totals):
            rows = rows_of(c)
            last = total[CHUNK - 1 : CHUNK, :]
            middle = total[CHUNK // 2 - 1 : CHUNK // 2, :]
            total = total - middle
            key_mid = key * jnp.exp(-total)
            intra[rows, :] = total
            reach[rows, :] = key_mid.astype(jnp.bfloat16)
            key_end = (key_mid * jnp.exp(last - middle)).astype(jnp.bfloat16)
            for h, part in enumerate(parts):
                local[c, h] = dot(proj[VALUE, rows, part], key_end[:, part], ((0,), (0,)))
            closing[c] = last
            centre[c] = middle

    def query_part(several):
        queries, scores = [], []
        for c in several:
            rows = rows_of(c)
            query = proj[QUERY, rows, :].astype(jnp.float32)
            query = query * jax.nn.sigmoid(query) * jnp.exp(intra[rows, :])
            queries.append(query)
            query = query.astype(jnp.bfloat16)
            scores.append([dot(query[:, part], reach[rows, part], ((1,), (1,))) for part in parts])
        for c, query, score in zip(several, queries, scores):
            rows = rows_of(c)
            for part, one in zip(parts, score):
                one = jnp.where(causal, one, 0.0).astype(jnp.bfloat16)
                intra[rows, part] = dot(one, proj[VALUE, rows, part])
            reach[rows, :] = (query * jnp.exp(centre[c])).astype(jnp.bfloat16)

    def chunk_loop(first, number):
        def step(i, carry):
            several = [first + 2 * i, first + 2 * i + 1]
            state_part(several)
            query_part(several)
            return carry

        lax.fori_loop(0, number // 2, step, 0)

    def mix(first, size):
        def step(i, carry):
            row = pl.multiple_of(first + i * TILE, TILE)
            for g, lanes in enumerate(lanes_of):
                gate = proj[GLU_GATE, pl.ds(row, TILE), lanes].astype(jnp.float32)
                value = proj[GLU_VALUE, pl.ds(row, TILE), lanes].astype(jnp.float32)
                mixed = (value * jax.nn.sigmoid(gate)).astype(jnp.bfloat16)
                padded[g, pl.ds(pl.multiple_of(row + REACH, 8), TILE), :] = mixed.astype(jnp.float32)
            return carry

        lax.fori_loop(0, size // TILE, step, 0)

    taps = taps_ref.shape[0]
    skip = REACH - taps + 1

    def filter_tile(t):
        base = pl.multiple_of(t * LANES, LANES)

        def step(i, carry):
            g, row = i // (LANES // TILE), base + lax.rem(i, LANES // TILE) * TILE
            lanes = pl.ds(pl.multiple_of(g * LANES, LANES), LANES)
            total = jnp.zeros((TILE, LANES), jnp.float32)
            for j in range(taps):
                total = total + taps_ref[j : j + 1, lanes] * padded[g, pl.ds(row + (j + skip), TILE), :]
            filtered[pl.ds(pl.multiple_of(row, TILE), TILE), lanes] = total
            return carry

        lax.fori_loop(0, len(lanes_of) * (LANES // TILE), step, 0)
        sums = jnp.zeros((LANES, LANES), jnp.float32)
        squares = jnp.zeros((LANES, LANES), jnp.float32)
        for lanes in lanes_of:
            value = filtered[pl.ds(base, LANES), lanes]
            sums = sums + value
            squares = squares + value * value
        own_stats[0:1, pl.ds(base, LANES)] = jnp.sum(sums.T, axis=0, keepdims=True)
        own_stats[1:2, pl.ds(base, LANES)] = jnp.sum(squares.T, axis=0, keepdims=True)

    def filter_loop(first, number):
        def step(i, carry):
            filter_tile(first + i)
            return carry

        lax.fori_loop(0, number, step, 0)

    chip = 2 * block
    own_half = (me // 2) * chip
    far_half = chip - own_half if rows_all == 2 * chip else lax.rem(own_half + chip, rows_all)
    half_tiles = chip // LANES

    project(near_rows.at[0], 0, len(sources), [(0, me * block, block)], ready=True)
    for one in nearby:
        one.wait_recv()
    project(near_rows.at[1], 0, len(sources), [(0, pair * block, block)])
    pass_on(0)
    chunk_loop(own_half // CHUNK, chip // CHUNK)
    pass_on(1)
    mix(own_half, chip)

    def far_places(big):
        return [(0, cross * block + big * CHUNK, CHUNK), (CHUNK, diag * block + big * CHUNK, CHUNK)]

    def far_chunks(big):
        return [owner * bigs + big for owner in (cross, diag)]

    for big in range(bigs):
        final = big == bigs - 1
        if final:
            filter_loop(own_half // LANES + 1, half_tiles - 1)
        for p in range(big * per, (big + 1) * per):
            if p > 1:
                pass_on(p)
        for p in range(big * per, (big + 1) * per):
            handed[p].wait_recv()
        if final:
            project(far_rows.at[big], 0, 2, far_places(big))
        else:
            project(far_rows.at[big], 0, len(sources), far_places(big))
        state_part(far_chunks(big))
        if not final:
            query_part(far_chunks(big))
            for _, row, size in far_places(big):
                mix(row, size)

    place = lax.broadcasted_iota(jnp.int32, (PAD, head), 0)
    packs = [remote(pack.at[h], pack_in.at[h], pack_send.at[h], pack_recv.at[h], "sp", mate) for h in range(heads)]
    for h in range(heads):
        part = slice(h * head, (h + 1) * head)
        state, log = local[0, h], closing[0, :, part]
        for c in range(1, chunks):
            state = state * jnp.exp(closing[c, :, part]) + local[c, h]
            log = log + closing[c, :, part]
        own_state[h] = state
        own_log[:, part] = log
        pack[h, 0:head, :] = state.astype(jnp.bfloat16)
        high = log.astype(jnp.bfloat16).astype(jnp.float32)
        rest = log - high
        mid = rest.astype(jnp.bfloat16).astype(jnp.float32)
        low = rest - mid
        tail = jnp.where(place == 0, high, jnp.where(place == 1, mid, jnp.where(place == 2, low, 0.0)))
        pack[h, head : head + PAD, :] = tail.astype(jnp.bfloat16)
        packs[h].start()

    project(far_rows.at[bigs - 1], 2, len(sources), far_places(bigs - 1))
    for _, row, size in far_places(bigs - 1):
        mix(row, size)
    for g, lanes in enumerate(lanes_of):
        rim[0, :, lanes] = padded[g, rows_all : rows_all + REACH, :].astype(jnp.bfloat16)
    edge = remote(rim.at[0], rim.at[1], rim_sem.at[0], rim_sem.at[1], "sp", lax.rem(at + 1, count))
    edge.start()
    query_part(far_chunks(bigs - 1))

    links = [
        remote(chain_out.at[h], chain_in.at[h], chain_send.at[h], chain_recv.at[h], "sp", lax.rem(at + 2, count))
        for h in range(heads)
    ]

    def mate_log(h):
        tail = pack_in[h, head : head + PAD, :].astype(jnp.float32)
        return tail[0:1] + tail[1:2] + tail[2:3]

    for h in range(heads):
        part = slice(h * head, (h + 1) * head)
        packs[h].wait_recv()
        theirs, log = pack_in[h, 0:head, :].astype(jnp.float32), mate_log(h)
        ours, own = own_state[h], own_log[:, part]
        first = jnp.where(side == 0, ours, theirs)
        second = jnp.where(side == 0, theirs, ours)
        group_state[h] = first * jnp.exp(jnp.where(side == 0, log, own)) + second
        group_log[:, part] = log + own

        @pl.when(team == 0)
        def _():
            chain_in[h] = jnp.zeros((head, head), jnp.bfloat16)
            chain_out[h] = group_state[h].astype(jnp.bfloat16)
            links[h].start()

    def relay(k):
        @pl.when(team == k)
        def _():
            for h in range(heads):
                links[h].wait_recv()
                if k < teams - 1:
                    part = slice(h * head, (h + 1) * head)
                    step = chain_in[h].astype(jnp.float32) * jnp.exp(group_log[:, part]) + group_state[h]
                    chain_out[h] = step.astype(jnp.bfloat16)
                    links[h].start()

    far_tile = far_half // LANES

    def rim_in():
        edge.wait_recv()
        for g, lanes in enumerate(lanes_of):
            padded[g, 0:REACH, :] = jnp.where(at > 0, rim[1, :, lanes].astype(jnp.float32), 0.0)
        filter_tile(own_half // LANES)

    stats = [
        remote(own_stats, other_stats.at[k - 1], stat_send.at[k - 1], stat_recv.at[k - 1], "tp", lax.rem(me + k, 4))
        for k in range(1, 4)
    ]

    def send_stats():
        filter_tile(far_tile)
        for one in stats:
            one.start()

    work = [lambda: filter_loop(far_tile + 1, 2), lambda: filter_loop(far_tile + 3, 1), rim_in, send_stats]
    if half_tiles != 4:
        work[1] = lambda: filter_loop(far_tile + 3, half_tiles - 3)
    relays = [functools.partial(relay, k) for k in range(1, teams)]
    while work or relays:
        if work:
            work.pop(0)()
        if relays:
            relays.pop(0)()

    for one in stats:
        one.wait_recv()

    def stats_tile(i, carry):
        row = pl.multiple_of(i * LANES, LANES)
        total = own_stats[:, pl.ds(row, LANES)]
        for k in range(3):
            total = total + other_stats[k, :, pl.ds(row, LANES)]
        mean = total[0:1] / channels
        scale = lax.rsqrt(total[1:2] / channels - mean * mean + norm_epsilon)
        for k, value in enumerate((mean, scale)):
            moments[k, pl.ds(row, LANES), :] = jnp.broadcast_to(value, (LANES, LANES)).T
        return carry

    lax.fori_loop(0, rows_all // LANES, stats_tile, 0)

    for h in range(heads):
        part = slice(h * head, (h + 1) * head)
        state = chain_in[h].astype(jnp.float32)
        moved = state * jnp.exp(mate_log(h)) + pack_in[h, 0:head, :].astype(jnp.float32)
        state = jnp.where(side == 1, moved, state)
        for c in range(chunks):
            enter[c, h] = state.astype(jnp.bfloat16)
            if c < chunks - 1:
                state = state * jnp.exp(closing[c, :, part]) + local[c, h]

    def finish_rows(owner, low, size, slot):
        start = pl.multiple_of(owner * block + low, size)
        rows, c = pl.ds(start, size), owner * bigs + low // CHUNK
        target = pl.ds(slot, size)
        for h in range(heads):
            part = slice(h * head, (h + 1) * head)
            rec = intra[rows, part] + dot(reach[rows, part], enter[c, h], ((1,), (1,)))
            rec = rec * lax.rsqrt(jnp.mean(rec * rec, axis=-1, keepdims=True) + head_epsilon) * head_gain_ref[...]
            gate = proj[RGATE, rows, part].astype(jnp.float32)
            blend[target, part] = (rec * (gate * jax.nn.sigmoid(gate))).astype(jnp.bfloat16)
        for g, lanes in enumerate(lanes_of):
            normed = (filtered[rows, lanes] - moments[0, rows, :]) * moments[1, rows, :] * conv_gain_ref[:, lanes]
            blend[target, width + g * LANES : width + (g + 1) * LANES] = (normed * jax.nn.sigmoid(normed)).astype(
                jnp.bfloat16
            )

    columns = merge.shape[1]

    def spread(size, put):
        def step(j, carry):
            cols = pl.ds(pl.multiple_of(j * SPAN, SPAN), SPAN)
            put(cols, dot(blend[0:size, :], merge[:, cols]))
            return carry

        lax.fori_loop(0, columns // SPAN, step, 0)

    for one in fetched[len(sources) :]:
        one.wait()
    turn = block // RETURNS
    lent, returned, close = [], [], []

    def settle(p):
        rows = pl.ds(p * turn, turn)
        lent[p].wait_recv()
        to_cross[rows, :] = (held[p % 2] + from_pair[0, rows, :].astype(jnp.float32)).astype(jnp.bfloat16)
        returned.append(
            remote(to_cross.at[rows, :], from_cross.at[rows, :], back_send.at[1, p], back_recv.at[1, p], "tp", cross)
        )
        returned[p].start()

    for p in range(RETURNS):
        rows = pl.ds(p * turn, turn)
        finish_rows(diag, p * turn, turn, 0)
        finish_rows(cross, p * turn, turn, turn)
        if p > 0:
            settle(p - 1)

        def put(cols, result, p=p, rows=rows):
            to_pair[0, rows, cols] = result[0:turn].astype(jnp.bfloat16)
            held[p % 2, :, cols] = result[turn : 2 * turn]

        spread(2 * turn, put)
        lent.append(
            remote(
                to_pair.at[0, rows, :], from_pair.at[0, rows, :], back_send.at[0, p], back_recv.at[0, p], "tp", pair
            )
        )
        lent[p].start()
    settle(RETURNS - 1)
    for big in range(bigs):
        rows = pl.ds(big * CHUNK, CHUNK)
        finish_rows(pair, big * CHUNK, CHUNK, 0)
        finish_rows(me, big * CHUNK, CHUNK, CHUNK)

        def put(cols, result, rows=rows):
            to_pair[1, rows, cols] = result[0:CHUNK].astype(jnp.bfloat16)
            mine[rows, cols] = result[CHUNK : 2 * CHUNK]

        spread(2 * CHUNK, put)
        close.append(
            remote(
                to_pair.at[1, rows, :], from_pair.at[1, rows, :], back_send.at[2, big], back_recv.at[2, big],
                "tp", pair,
            )
        )
        close[big].start()
    for big in range(bigs):
        rows = pl.ds(big * CHUNK, CHUNK)
        close[big].wait_recv()
        mine[rows, :] = mine[rows, :] + from_pair[1, rows, :].astype(jnp.float32)
    stores = []
    for p in range(RETURNS):
        rows = pl.ds(p * turn, turn)
        returned[p].wait_recv()
        done[rows, :] = (mine[rows, :] + from_cross[rows, :].astype(jnp.float32)).astype(jnp.bfloat16)
        stores.append(pltpu.make_async_copy(done.at[rows, :], out_ref.at[rows, :], out_sem.at[p]))
        stores[p].start()
    for one in crossing + nearby + handed + packs + [edge] + stats + lent + returned + close:
        one.wait_send()

    @pl.when(team < teams - 1)
    def _():
        for one in links:
            one.wait_send()

    for one in stores:
        one.wait()


def on_device(
    tokens, norm_gain, w_query, w_forget, w_value, w_rgate, w_glu_value, w_glu_gate, forget_gap,
    decay_shift, head_gain, conv_taps, conv_gain, out_rec, out_conv,
):
    weights = (w_forget, w_value, w_query, w_glu_value, w_glu_gate, w_rgate)
    block, depth = tokens.shape
    width, columns = out_rec.shape
    head = head_gain.shape[0]
    heads = width // head
    rows = block * lax.axis_size("tp")
    groups = width // LANES
    chunks = rows // CHUNK
    turn = block // RETURNS
    bf16, f32 = jnp.bfloat16, jnp.float32
    vmem = lambda shape, kind: pltpu.VMEM(shape, kind)
    sems = lambda *shape: pltpu.SemaphoreType.DMA(shape)
    return pl.pallas_call(
        functools.partial(layer_kernel, head),
        in_specs=[pl.BlockSpec(memory_space=pltpu.VMEM)] * 6 + [pl.BlockSpec(memory_space=pl.ANY)] * 9,
        out_specs=pl.BlockSpec(memory_space=pl.ANY),
        out_shape=jax.ShapeDtypeStruct((block, columns), bf16),
        scratch_shapes=[
            vmem((block, depth), bf16),
            vmem((2, block, depth), bf16),
            vmem((block // CHUNK, 2 * CHUNK, depth), bf16),
            vmem((len(weights), depth, width), bf16),
            vmem((2 * width, columns), bf16),
            vmem((len(weights), rows, width), bf16),
            vmem((rows, width), f32),
            vmem((rows, width), bf16),
            vmem((chunks, heads, head, head), f32),
            vmem((chunks, 1, width), f32),
            vmem((chunks, 1, width), f32),
            vmem((chunks, heads, head, head), bf16),
            vmem((heads, head, head), f32),
            vmem((1, width), f32),
            vmem((heads, head + PAD, head), bf16),
            vmem((heads, head + PAD, head), bf16),
            vmem((heads, head, head), f32),
            vmem((1, width), f32),
            vmem((heads, head, head), bf16),
            vmem((heads, head, head), bf16),
            vmem((2, REACH, width), bf16),
            vmem((groups, REACH + rows, LANES), f32),
            vmem((rows, width), f32),
            vmem((2, rows), f32),
            vmem((3, 2, rows), f32),
            vmem((2, rows, LANES), f32),
            vmem((2 * CHUNK, 2 * width), bf16),
            vmem((2, turn, columns), f32),
            vmem((2, block, columns), bf16),
            vmem((2, block, columns), bf16),
            vmem((block, columns), bf16),
            vmem((block, columns), bf16),
            vmem((block, columns), f32),
            vmem((block, columns), bf16),
            sems(SENDS),
            sems(len(weights) + 2),
            sems(3, SENDS),
            sems(3, SENDS),
            sems(heads),
            sems(heads),
            sems(heads),
            sems(heads),
            sems(2),
            sems(3),
            sems(3),
            sems(3, RETURNS),
            sems(3, RETURNS),
            sems(RETURNS),
        ],
        compiler_params=pltpu.CompilerParams(
            collective_id=0, has_side_effects=True, vmem_limit_bytes=65000 * 1024
        ),
    )(
        norm_gain[None], forget_gap[None], decay_shift.T, conv_taps, conv_gain[None], head_gain[None],
        tokens, *weights, out_rec, out_conv,
    )


def solution(mesh):
    placed = (
        P(("sp", "tp"), None),
        P(),
        P(None, "tp"),
        P(None, "tp"),
        P(None, "tp"),
        P(None, "tp"),
        P(None, "tp"),
        P(None, "tp"),
        P("tp"),
        P("sp", "tp"),
        P(),
        P(None, "tp"),
        P("tp"),
        P("tp", None),
        P("tp", None),
    )
    return jax.shard_map(
        on_device, mesh=mesh, in_specs=placed, out_specs=P(("sp", "tp"), None), check_vma=False
    )
```

```python
import functools

import jax
import jax.numpy as jnp
from jax import lax
from jax.experimental import pallas as pl
from jax.experimental.pallas import tpu as pltpu
from jax.sharding import PartitionSpec as P

CHUNK = 128
PAD = 16
SENDS = 8
RETURNS = 4
REACH = 32
TILE = 64
LANES = 128
SPAN = 512
MESH = pl.DeviceIdType.MESH
FORGET, VALUE, GLU_VALUE, GLU_GATE, QUERY, RGATE = range(6)

norm_epsilon = 1e-05
head_epsilon = 1e-06


def dot(a, b, dims=((1,), (0,))):
    return lax.dot_general(a, b, (dims, ((), ())), preferred_element_type=jnp.float32)


def layer_norm(values, gain):
    widened = values.astype(jnp.float32)
    row_mean = jnp.mean(widened, axis=-1, keepdims=True)
    centred = widened - row_mean
    row_var = jnp.mean(centred * centred, axis=-1, keepdims=True)
    return centred * lax.rsqrt(row_var + norm_epsilon) * gain


def layer_kernel(
    head, gain_in, gap_in, shift_in, taps_in, conv_gain_in, head_gain_in,
    tokens_ref, w0, w1, w2, w3, w4, w5, rec_rows, conv_rows, out_ref,
    gain_ref, gap_ref, shift_ref, taps_ref, conv_gain_ref, head_gain_ref,
    raw, near_rows, far_rows, weight, merge, proj, intra, reach, local, closing, centre, enter,
    own_state, own_log, pack, pack_in, group_state, group_log, chain_out, chain_in,
    rim, padded, filtered, own_stats, other_stats, moments,
    blend, early, held, to_pair, from_pair, to_cross, from_cross, mine, done,
    small_sem, raw_sem, weight_sem, send_sem, recv_sem, pack_send, pack_recv, chain_send, chain_recv,
    rim_sem, stat_send, stat_recv, back_send, back_recv, first_send, first_recv, out_sem,
):
    block, depth = tokens_ref.shape
    piece = block // SENDS
    raws = []
    for p in range(SENDS):
        rows = pl.ds(p * piece, piece)
        raws.append(pltpu.make_async_copy(tokens_ref.at[rows, :], raw.at[rows, :], raw_sem.at[p]))
        raws[p].start()
    smalls = []
    for i, (far, near) in enumerate((
        (gain_in, gain_ref), (gap_in, gap_ref), (shift_in, shift_ref), (taps_in, taps_ref),
        (conv_gain_in, conv_gain_ref), (head_gain_in, head_gain_ref),
    )):
        smalls.append(pltpu.make_async_copy(far, near, small_sem.at[i]))
        smalls[i].start()
    sources = (w0, w1, w2, w3, w4, w5)
    width = gap_ref.shape[1]
    fetched = [pltpu.make_async_copy(w, weight.at[i], weight_sem.at[i]) for i, w in enumerate(sources)]
    for i, w in enumerate((rec_rows, conv_rows)):
        fetched.append(
            pltpu.make_async_copy(w, merge.at[pl.ds(i * width, width), :], weight_sem.at[len(sources) + i])
        )
    me, count = lax.axis_index("tp"), lax.axis_size("sp")
    pair = me + 1 - 2 * lax.rem(me, 2)
    cross, diag = lax.rem(me + 2, 4), lax.rem(pair + 2, 4)
    at = lax.axis_index("sp")
    side, team, teams = lax.rem(at, 2), at // 2, count // 2
    mate = at + 1 - 2 * side
    barrier = pltpu.get_barrier_semaphore()
    for other in (pair, cross, diag):
        pl.semaphore_signal(barrier, inc=1, device_id={"tp": other}, device_id_type=MESH)
    pl.semaphore_signal(barrier, inc=1, device_id={"sp": mate}, device_id_type=MESH)

    @pl.when(team > 0)
    def _():
        pl.semaphore_signal(barrier, inc=1, device_id={"sp": at - 2}, device_id_type=MESH)

    @pl.when((team > 0) & (side == 0))
    def _():
        pl.semaphore_signal(barrier, inc=1, device_id={"sp": at - 1}, device_id_type=MESH)

    onward = team < teams - 1
    pl.semaphore_wait(barrier, jnp.where(onward, jnp.where(side == 1, 6, 5), 4))

    rows_all = proj.shape[1]
    heads, chunks = width // head, rows_all // CHUNK
    bigs = block // CHUNK
    per = CHUNK // piece
    channels = width * lax.axis_size("tp")
    lanes_of = [slice(g * LANES, (g + 1) * LANES) for g in range(width // LANES)]

    def remote(source, target, sends, recvs, axis, device):
        return pltpu.make_async_remote_copy(
            src_ref=source, dst_ref=target, send_sem=sends, recv_sem=recvs,
            device_id={axis: device}, device_id_type=MESH,
        )

    for one in raws + smalls:
        one.wait()
    for one in fetched:
        one.start()

    crossing, nearby, handed = [], [], []
    for p in range(SENDS):
        rows = pl.ds(p * piece, piece)
        near_rows[0, rows, :] = layer_norm(raw[rows, :], gain_ref[...]).astype(jnp.bfloat16)
        big, low = p // per, (p % per) * piece
        landing = far_rows.at[big, pl.ds(low, piece), :]
        crossing.append(remote(near_rows.at[0, rows, :], landing, send_sem.at[0, p], recv_sem.at[0, p], "tp", cross))
        nearby.append(
            remote(
                near_rows.at[0, rows, :], near_rows.at[1, rows, :], send_sem.at[1, p], recv_sem.at[1, p], "tp", pair
            )
        )
        handed.append(
            remote(
                landing, far_rows.at[big, pl.ds(CHUNK + low, piece), :],
                send_sem.at[2, p], recv_sem.at[2, p], "tp", pair,
            )
        )
        crossing[p].start()
        nearby[p].start()

    def project(values, first, last, places, ready=False):
        def step(k, carry):
            for i in (first + 2 * k, first + 2 * k + 1):
                if ready:
                    for one in range(first, last):
                        pl.when(i == one)(fetched[one].wait)
            for i in (first + 2 * k, first + 2 * k + 1):
                result = dot(values[...], weight[i]).astype(jnp.bfloat16)
                for start, row, size in places:
                    proj[i, pl.ds(pl.multiple_of(row, CHUNK), size), :] = result[start : start + size]
            return carry

        lax.fori_loop(0, (last - first) // 2, step, 0)

    def pass_on(p):
        crossing[p].wait_recv()
        handed[p].start()

    row_at = lax.broadcasted_iota(jnp.int32, (CHUNK, CHUNK), 0)
    col_at = lax.broadcasted_iota(jnp.int32, (CHUNK, CHUNK), 1)
    causal = row_at >= col_at
    lower = jnp.where(causal, 1.0, 0.0).astype(jnp.bfloat16)
    lower = jnp.concatenate([lower, lower], axis=1)

    parts = [slice(h * head, (h + 1) * head) for h in range(heads)]

    def rows_of(c):
        return pl.ds(pl.multiple_of(c * CHUNK, CHUNK), CHUNK)

    def state_part(several):
        keys, totals = [], []
        for c in several:
            rows = rows_of(c)
            key = gap_ref[...] * jax.nn.sigmoid(-proj[FORGET, rows, :].astype(jnp.float32))
            shift = [jnp.broadcast_to(shift_ref[h : h + 1, rows], (head, CHUNK)).T for h in range(heads)]
            log = jnp.log1p(-key) + jnp.concatenate(shift, axis=1)
            high = log.astype(jnp.bfloat16)
            low = (log - high.astype(jnp.float32)).astype(jnp.bfloat16)
            keys.append(key)
            totals.append(dot(lower, jnp.concatenate([high, low], axis=0)))
        for c, key, total in zip(several, keys, totals):
            rows = rows_of(c)
            last = total[CHUNK - 1 : CHUNK, :]
            middle = total[CHUNK // 2 - 1 : CHUNK // 2, :]
            total = total - middle
            key_mid = key * jnp.exp(-total)
            intra[rows, :] = total
            reach[rows, :] = key_mid.astype(jnp.bfloat16)
            key_end = (key_mid * jnp.exp(last - middle)).astype(jnp.bfloat16)
            for h, part in enumerate(parts):
                local[c, h] = dot(proj[VALUE, rows, part], key_end[:, part], ((0,), (0,)))
            closing[c] = last
            centre[c] = middle

    def query_part(several):
        queries, scores = [], []
        for c in several:
            rows = rows_of(c)
            query = proj[QUERY, rows, :].astype(jnp.float32)
            query = query * jax.nn.sigmoid(query) * jnp.exp(intra[rows, :])
            queries.append(query)
            query = query.astype(jnp.bfloat16)
            scores.append([dot(query[:, part], reach[rows, part], ((1,), (1,))) for part in parts])
        for c, query, score in zip(several, queries, scores):
            rows = rows_of(c)
            for part, one in zip(parts, score):
                one = jnp.where(causal, one, 0.0).astype(jnp.bfloat16)
                intra[rows, part] = dot(one, proj[VALUE, rows, part])
            reach[rows, :] = (query * jnp.exp(centre[c])).astype(jnp.bfloat16)

    def chunk_loop(first, number):
        def step(i, carry):
            several = [first + 2 * i, first + 2 * i + 1]
            state_part(several)
            query_part(several)
            return carry

        lax.fori_loop(0, number // 2, step, 0)

    def mix(first, size):
        def step(i, carry):
            row = pl.multiple_of(first + i * TILE, TILE)
            for g, lanes in enumerate(lanes_of):
                gate = proj[GLU_GATE, pl.ds(row, TILE), lanes].astype(jnp.float32)
                value = proj[GLU_VALUE, pl.ds(row, TILE), lanes].astype(jnp.float32)
                mixed = (value * jax.nn.sigmoid(gate)).astype(jnp.bfloat16)
                padded[g, pl.ds(pl.multiple_of(row + REACH, 8), TILE), :] = mixed.astype(jnp.float32)
            return carry

        lax.fori_loop(0, size // TILE, step, 0)

    taps = taps_ref.shape[0]
    skip = REACH - taps + 1

    def filter_rows(row0, number):
        def step(i, carry):
            g, row = i // number, row0 + lax.rem(i, number) * TILE
            lanes = pl.ds(pl.multiple_of(g * LANES, LANES), LANES)
            total = jnp.zeros((TILE, LANES), jnp.float32)
            for j in range(taps):
                total = total + taps_ref[j : j + 1, lanes] * padded[g, pl.ds(row + (j + skip), TILE), :]
            filtered[pl.ds(pl.multiple_of(row, TILE), TILE), lanes] = total
            return carry

        lax.fori_loop(0, len(lanes_of) * number, step, 0)

    def filter_tile(t, low=0):
        base = pl.multiple_of(t * LANES, LANES)
        filter_rows(base, (LANES - low) // TILE)
        sums = jnp.zeros((LANES, LANES), jnp.float32)
        squares = jnp.zeros((LANES, LANES), jnp.float32)
        for lanes in lanes_of:
            value = filtered[pl.ds(base, LANES), lanes]
            sums = sums + value
            squares = squares + value * value
        own_stats[0:1, pl.ds(base, LANES)] = jnp.sum(sums.T, axis=0, keepdims=True)
        own_stats[1:2, pl.ds(base, LANES)] = jnp.sum(squares.T, axis=0, keepdims=True)

    def filter_loop(first, number):
        def step(i, carry):
            filter_tile(first + i)
            return carry

        lax.fori_loop(0, number, step, 0)

    chip = 2 * block
    own_half = (me // 2) * chip
    far_half = chip - own_half if rows_all == 2 * chip else lax.rem(own_half + chip, rows_all)
    half_tiles = chip // LANES

    project(near_rows.at[0], 0, len(sources), [(0, me * block, block)], ready=True)
    for one in nearby:
        one.wait_recv()
    project(near_rows.at[1], 0, len(sources), [(0, pair * block, block)])
    pass_on(0)
    chunk_loop(own_half // CHUNK, chip // CHUNK)
    for p in range(1, per - 1):
        pass_on(p)
    mix(own_half, chip)
    filter_loop(own_half // LANES + 1, half_tiles - 2)
    pass_on(per - 1)

    def far_places(big):
        return [(0, cross * block + big * CHUNK, CHUNK), (CHUNK, diag * block + big * CHUNK, CHUNK)]

    def far_chunks(big):
        return [owner * bigs + big for owner in (cross, diag)]

    far_tile = far_half // LANES
    for big in range(bigs - 1):
        begin = big * per
        for p in range(begin, begin + per):
            handed[p].wait_recv()
        project(far_rows.at[big], 0, len(sources), far_places(big))
        pass_on(begin + per)
        state_part(far_chunks(big))
        query_part(far_chunks(big))
        for _, row, size in far_places(big):
            mix(row, size)
        for p in range(begin + per + 1, begin + 2 * per - 2):
            pass_on(p)
        if big == bigs - 2:
            filter_tile(own_half // LANES + half_tiles - 1)
            for tile in (own_half // LANES, far_tile, far_tile + bigs):
                filter_rows(pl.multiple_of(tile * LANES + TILE, TILE), 1)
        for p in range(begin + 2 * per - 2, begin + 2 * per):
            pass_on(p)
    for p in range(SENDS - per, SENDS):
        handed[p].wait_recv()
    project(far_rows.at[bigs - 1], 0, 2, far_places(bigs - 1))
    state_part(far_chunks(bigs - 1))

    place = lax.broadcasted_iota(jnp.int32, (PAD, head), 0)
    half = head // 2
    units = [(h, k) for h in range(heads) for k in range(2)]
    spans = (pl.ds(0, PAD + half), pl.ds(PAD + half, half))
    packs = [
        remote(pack.at[h, spans[k], :], pack_in.at[h, spans[k], :], pack_send.at[h, k], pack_recv.at[h, k], "sp", mate)
        for h, k in units
    ]
    for h in range(heads):
        part = slice(h * head, (h + 1) * head)
        state, log = local[0, h], closing[0, :, part]
        for c in range(1, chunks):
            state = state * jnp.exp(closing[c, :, part]) + local[c, h]
            log = log + closing[c, :, part]
        own_state[h] = state
        own_log[:, part] = log
        pack[h, PAD : PAD + head, :] = state.astype(jnp.bfloat16)
        high = log.astype(jnp.bfloat16).astype(jnp.float32)
        rest = log - high
        mid = rest.astype(jnp.bfloat16).astype(jnp.float32)
        low = rest - mid
        tail = jnp.where(place == 0, high, jnp.where(place == 1, mid, jnp.where(place == 2, low, 0.0)))
        pack[h, 0:PAD, :] = tail.astype(jnp.bfloat16)
        packs[2 * h].start()
        packs[2 * h + 1].start()

    project(far_rows.at[bigs - 1], 2, 4, far_places(bigs - 1))
    for _, row, size in far_places(bigs - 1):
        mix(row, size)
    for g, lanes in enumerate(lanes_of):
        rim[0, :, lanes] = padded[g, rows_all : rows_all + REACH, :].astype(jnp.bfloat16)
    edge = remote(rim.at[0], rim.at[1], rim_sem.at[0], rim_sem.at[1], "sp", lax.rem(at + 1, count))
    ahead = onward | (side == 0)
    pl.when(ahead)(edge.start)

    links = [
        remote(
            chain_out.at[h, pl.ds(k * half, half), :], chain_in.at[h, pl.ds(k * half, half), :],
            chain_send.at[h, k], chain_recv.at[h, k], "sp", lax.rem(at + 2, count),
        )
        for h, k in units
    ]

    def mate_log(h):
        tail = pack_in[h, 0:PAD, :].astype(jnp.float32)
        return tail[0:1] + tail[1:2] + tail[2:3]

    def meet(u):
        h, k = units[u]
        some = pl.ds(k * half, half)
        packs[u].wait_recv()
        theirs, log = pack_in[h, PAD + k * half : PAD + (k + 1) * half, :].astype(jnp.float32), mate_log(h)
        ours, own = own_state[h, some, :], own_log[:, parts[h]]
        first = jnp.where(side == 0, ours, theirs)
        second = jnp.where(side == 0, theirs, ours)
        group = first * jnp.exp(jnp.where(side == 0, log, own)) + second
        group_state[h, some, :] = group
        if k == 0:
            group_log[:, parts[h]] = log + own

        @pl.when(team == 0)
        def _():
            chain_in[h, some, :] = jnp.zeros((half, head), jnp.bfloat16)
            chain_out[h, some, :] = group.astype(jnp.bfloat16)
            links[u].start()

    def relay(k, first, last):
        @pl.when(team == k)
        def _():
            for u in range(first, last):
                h, some = units[u][0], pl.ds(units[u][1] * half, half)
                links[u].wait_recv()
                if k < teams - 1:
                    step = chain_in[h, some, :].astype(jnp.float32) * jnp.exp(group_log[:, parts[h]])
                    chain_out[h, some, :] = (step + group_state[h, some, :]).astype(jnp.bfloat16)
                    links[u].start()

    def rim_in():
        pl.when(at > 0)(edge.wait_recv)
        for g, lanes in enumerate(lanes_of):
            padded[g, 0:REACH, :] = jnp.where(at > 0, rim[1, :, lanes].astype(jnp.float32), 0.0)

    stats = [
        remote(own_stats, other_stats.at[k - 1], stat_send.at[k - 1], stat_recv.at[k - 1], "tp", lax.rem(me + k, 4))
        for k in range(1, 4)
    ]
    number = len(units)
    for u in range(0, 3):
        meet(u)
    filter_tile(far_tile + 1)
    for u in range(3, 6):
        meet(u)
    filter_tile(far_tile + bigs, TILE)
    for u in range(6, number):
        meet(u)
    relay(1, 0, 3)
    if bigs > 2:
        filter_loop(far_tile + 2, bigs - 2)
    filter_loop(far_tile + bigs + 1, bigs - 1)
    relay(1, 3, 6)
    rim_in()
    filter_tile(own_half // LANES, TILE)
    relay(1, 6, number)
    filter_tile(far_tile, TILE)
    for one in stats:
        one.start()
    if teams > 3:
        relay(2, 0, number)
    for one in stats:
        one.wait_recv()

    def stats_tile(i):
        row = pl.multiple_of(i * LANES, LANES)
        total = own_stats[:, pl.ds(row, LANES)]
        for k in range(3):
            total = total + other_stats[k, :, pl.ds(row, LANES)]
        mean = total[0:1] / channels
        scale = lax.rsqrt(total[1:2] / channels - mean * mean + norm_epsilon)
        for k, value in enumerate((mean, scale)):
            moments[k, pl.ds(row, LANES), :] = jnp.broadcast_to(value, (LANES, LANES)).T

    for owner in (diag, cross):
        stats_tile(owner * bigs)

    def conv_part(owner, low, size, slot):
        rows, target = pl.ds(pl.multiple_of(owner * block + low, size), size), pl.ds(slot, size)
        for g, lanes in enumerate(lanes_of):
            normed = (filtered[rows, lanes] - moments[0, rows, :]) * moments[1, rows, :] * conv_gain_ref[:, lanes]
            blend[target, width + g * LANES : width + (g + 1) * LANES] = (normed * jax.nn.sigmoid(normed)).astype(
                jnp.bfloat16
            )

    columns = merge.shape[1]
    turn = block // RETURNS

    def spread(size, put, first=0, last=2 * width):
        def step(j, carry):
            cols = pl.ds(pl.multiple_of(j * SPAN, SPAN), SPAN)
            put(cols, dot(blend[0:size, first:last], merge[first:last, cols]))
            return carry

        lax.fori_loop(0, columns // SPAN, step, 0)

    for one in fetched[len(sources) :]:
        one.wait()
    conv_part(diag, 0, turn, 0)
    conv_part(cross, 0, turn, turn)

    def put_early(cols, result):
        early[:, cols] = result

    spread(2 * turn, put_early, first=width)
    for k in range(3 if teams > 3 else 2, teams):
        relay(k, 0, number)

    for h in range(heads):
        part = slice(h * head, (h + 1) * head)
        state = chain_in[h].astype(jnp.float32)
        moved = state * jnp.exp(mate_log(h)) + pack_in[h, PAD : PAD + head, :].astype(jnp.float32)
        state = jnp.where(side == 1, moved, state)
        for c in range(chunks):
            enter[c, h] = state.astype(jnp.bfloat16)
            if c < chunks - 1:
                state = state * jnp.exp(closing[c, :, part]) + local[c, h]

    def rec_part(owner, low, size, slot):
        rows, target = pl.ds(pl.multiple_of(owner * block + low, size), size), pl.ds(slot, size)
        c = owner * bigs + low // CHUNK
        for h, part in enumerate(parts):
            rec = intra[rows, part] + dot(reach[rows, part], enter[c, h], ((1,), (1,)))
            rec = rec * lax.rsqrt(jnp.mean(rec * rec, axis=-1, keepdims=True) + head_epsilon) * head_gain_ref[...]
            gate = proj[RGATE, rows, part].astype(jnp.float32)
            blend[target, part] = (rec * (gate * jax.nn.sigmoid(gate))).astype(jnp.bfloat16)

    def finish_rows(owner, low, size, slot):
        rec_part(owner, low, size, slot)
        conv_part(owner, low, size, slot)

    lent, returned, close = {}, {}, []

    def settle(p):
        rows = pl.ds(p * turn, turn)
        lent[p].wait_recv()
        to_cross[rows, :] = (held[p % 2] + from_pair[0, rows, :].astype(jnp.float32)).astype(jnp.bfloat16)
        returned[p] = remote(
            to_cross.at[rows, :], from_cross.at[rows, :], back_send.at[1, p], back_recv.at[1, p], "tp", cross
        )
        returned[p].start()

    late = (bigs - 1) * CHUNK // turn
    head_rows = pl.ds(0, turn)
    first_lent, first_returned = [], []
    rec_part(diag, 0, turn, 0)
    rec_part(cross, 0, turn, turn)
    for j in range(columns // SPAN):
        cols = slice(j * SPAN, (j + 1) * SPAN)
        result = dot(blend[0 : 2 * turn, 0:width], merge[0:width, cols]) + early[:, cols]
        to_pair[0, head_rows, cols] = result[0:turn].astype(jnp.bfloat16)
        held[0, :, cols] = result[turn : 2 * turn]
        first_lent.append(
            remote(
                to_pair.at[0, head_rows, cols], from_pair.at[0, head_rows, cols],
                first_send.at[0, j], first_recv.at[0, j], "tp", pair,
            )
        )
        first_lent[j].start()
    for j in range(columns // SPAN):
        cols = slice(j * SPAN, (j + 1) * SPAN)
        first_lent[j].wait_recv()
        to_cross[head_rows, cols] = (held[0, :, cols] + from_pair[0, head_rows, cols].astype(jnp.float32)).astype(
            jnp.bfloat16
        )
        first_returned.append(
            remote(
                to_cross.at[head_rows, cols], from_cross.at[head_rows, cols],
                first_send.at[1, j], first_recv.at[1, j], "tp", cross,
            )
        )
        first_returned[j].start()
    for p in range(1, RETURNS):
        rows = pl.ds(p * turn, turn)
        if p == late:
            settle(p - 1)
            project(far_rows.at[bigs - 1], 4, len(sources), far_places(bigs - 1))
            query_part(far_chunks(bigs - 1))
            for owner in (diag, cross):
                for big in range(1, bigs):
                    stats_tile(owner * bigs + big)
        finish_rows(diag, p * turn, turn, 0)
        finish_rows(cross, p * turn, turn, turn)
        if p > 1 and p != late:
            settle(p - 1)

        def put(cols, result, p=p, rows=rows):
            to_pair[0, rows, cols] = result[0:turn].astype(jnp.bfloat16)
            held[p % 2, :, cols] = result[turn : 2 * turn]

        spread(2 * turn, put)
        lent[p] = remote(
            to_pair.at[0, rows, :], from_pair.at[0, rows, :], back_send.at[0, p], back_recv.at[0, p], "tp", pair
        )
        lent[p].start()
    settle(RETURNS - 1)
    for owner in (pair, me):
        for big in range(bigs):
            stats_tile(owner * bigs + big)
    for big in range(bigs):
        rows = pl.ds(big * CHUNK, CHUNK)
        finish_rows(pair, big * CHUNK, CHUNK, 0)
        finish_rows(me, big * CHUNK, CHUNK, CHUNK)

        def put(cols, result, rows=rows):
            to_pair[1, rows, cols] = result[0:CHUNK].astype(jnp.bfloat16)
            mine[rows, cols] = result[CHUNK : 2 * CHUNK]

        spread(2 * CHUNK, put)
        close.append(
            remote(
                to_pair.at[1, rows, :], from_pair.at[1, rows, :], back_send.at[2, big], back_recv.at[2, big],
                "tp", pair,
            )
        )
        close[big].start()
    for big in range(bigs):
        rows = pl.ds(big * CHUNK, CHUNK)
        close[big].wait_recv()
        mine[rows, :] = mine[rows, :] + from_pair[1, rows, :].astype(jnp.float32)
    stores = []
    for p in range(RETURNS):
        rows = pl.ds(p * turn, turn)
        for one in first_returned if p == 0 else [returned[p]]:
            one.wait_recv()
        done[rows, :] = (mine[rows, :] + from_cross[rows, :].astype(jnp.float32)).astype(jnp.bfloat16)
        stores.append(pltpu.make_async_copy(done.at[rows, :], out_ref.at[rows, :], out_sem.at[p]))
        stores[p].start()
    for one in crossing + nearby + handed + packs + stats + first_lent + first_returned + close:
        one.wait_send()
    for p in range(1, RETURNS):
        lent[p].wait_send()
        returned[p].wait_send()

    pl.when(ahead)(edge.wait_send)

    @pl.when(onward)
    def _():
        for one in links:
            one.wait_send()

    for one in stores:
        one.wait()


def on_device(
    tokens, norm_gain, w_query, w_forget, w_value, w_rgate, w_glu_value, w_glu_gate, forget_gap,
    decay_shift, head_gain, conv_taps, conv_gain, out_rec, out_conv,
):
    weights = (w_forget, w_value, w_glu_value, w_glu_gate, w_query, w_rgate)
    block, depth = tokens.shape
    width, columns = out_rec.shape
    head = head_gain.shape[0]
    heads = width // head
    rows = block * lax.axis_size("tp")
    groups = width // LANES
    chunks = rows // CHUNK
    turn = block // RETURNS
    bf16, f32 = jnp.bfloat16, jnp.float32
    vmem = lambda shape, kind: pltpu.VMEM(shape, kind)
    sems = lambda *shape: pltpu.SemaphoreType.DMA(shape)
    return pl.pallas_call(
        functools.partial(layer_kernel, head),
        in_specs=[pl.BlockSpec(memory_space=pl.ANY)] * 15,
        out_specs=pl.BlockSpec(memory_space=pl.ANY),
        out_shape=jax.ShapeDtypeStruct((block, columns), bf16),
        scratch_shapes=[
            vmem((1, depth), f32),
            vmem((1, width), f32),
            vmem((heads, rows), f32),
            vmem(conv_taps.shape, f32),
            vmem((1, width), f32),
            vmem((1, head), f32),
            vmem((block, depth), bf16),
            vmem((2, block, depth), bf16),
            vmem((block // CHUNK, 2 * CHUNK, depth), bf16),
            vmem((len(weights), depth, width), bf16),
            vmem((2 * width, columns), bf16),
            vmem((len(weights), rows, width), bf16),
            vmem((rows, width), f32),
            vmem((rows, width), bf16),
            vmem((chunks, heads, head, head), f32),
            vmem((chunks, 1, width), f32),
            vmem((chunks, 1, width), f32),
            vmem((chunks, heads, head, head), bf16),
            vmem((heads, head, head), f32),
            vmem((1, width), f32),
            vmem((heads, head + PAD, head), bf16),
            vmem((heads, head + PAD, head), bf16),
            vmem((heads, head, head), f32),
            vmem((1, width), f32),
            vmem((heads, head, head), bf16),
            vmem((heads, head, head), bf16),
            vmem((2, REACH, width), bf16),
            vmem((groups, REACH + rows, LANES), f32),
            vmem((rows, width), f32),
            vmem((2, rows), f32),
            vmem((3, 2, rows), f32),
            vmem((2, rows, LANES), f32),
            vmem((2 * CHUNK, 2 * width), bf16),
            vmem((2 * turn, columns), f32),
            vmem((2, turn, columns), f32),
            vmem((2, block, columns), bf16),
            vmem((2, block, columns), bf16),
            vmem((block, columns), bf16),
            vmem((block, columns), bf16),
            vmem((block, columns), f32),
            vmem((block, columns), bf16),
            sems(6),
            sems(SENDS),
            sems(len(weights) + 2),
            sems(3, SENDS),
            sems(3, SENDS),
            sems(heads, 2),
            sems(heads, 2),
            sems(heads, 2),
            sems(heads, 2),
            sems(2),
            sems(3),
            sems(3),
            sems(3, RETURNS),
            sems(3, RETURNS),
            sems(2, columns // SPAN),
            sems(2, columns // SPAN),
            sems(RETURNS),
        ],
        compiler_params=pltpu.CompilerParams(
            collective_id=0, has_side_effects=True, vmem_limit_bytes=65000 * 1024
        ),
    )(
        norm_gain[None], forget_gap[None], decay_shift.T, conv_taps, conv_gain[None], head_gain[None],
        tokens, *weights, out_rec, out_conv,
    )


def solution(mesh):
    placed = (
        P(("sp", "tp"), None),
        P(),
        P(None, "tp"),
        P(None, "tp"),
        P(None, "tp"),
        P(None, "tp"),
        P(None, "tp"),
        P(None, "tp"),
        P("tp"),
        P("sp", "tp"),
        P(),
        P(None, "tp"),
        P("tp"),
        P("tp", None),
        P("tp", None),
    )
    return jax.shard_map(
        on_device, mesh=mesh, in_specs=placed, out_specs=P(("sp", "tp"), None), check_vma=False
    )
```

```python
import functools

import jax
import jax.numpy as jnp
from jax import lax
from jax.experimental import pallas as pl
from jax.experimental.pallas import tpu as pltpu
from jax.sharding import PartitionSpec as P

CHUNK = 128
PAD = 16
SENDS = 8
RETURNS = 4
REACH = 32
TILE = 64
LANES = 128
SPAN = 512
MESH = pl.DeviceIdType.MESH
FORGET, VALUE, GLU_VALUE, GLU_GATE, QUERY, RGATE = range(6)

norm_epsilon = 1e-05
head_epsilon = 1e-06


def dot(a, b, dims=((1,), (0,))):
    return lax.dot_general(a, b, (dims, ((), ())), preferred_element_type=jnp.float32)


def layer_norm(values, gain):
    widened = values.astype(jnp.float32)
    row_mean = jnp.mean(widened, axis=-1, keepdims=True)
    centred = widened - row_mean
    row_var = jnp.mean(centred * centred, axis=-1, keepdims=True)
    return centred * lax.rsqrt(row_var + norm_epsilon) * gain


def layer_kernel(
    head, gain_in, gap_in, shift_in, taps_in, conv_gain_in, head_gain_in,
    tokens_ref, w0, w1, w2, w3, w4, w5, rec_rows, conv_rows, out_ref,
    gain_ref, gap_ref, shift_ref, taps_ref, conv_gain_ref, head_gain_ref,
    raw, near_rows, far_rows, weight, merge, proj, intra, reach, local, closing, centre, enter,
    own_state, own_log, pack, pack_in, group_state, group_log, chain_out, chain_in,
    rim, padded, filtered, own_stats, other_stats, moments,
    blend, early, held, to_pair, from_pair, to_cross, from_cross, mine,
    small_sem, raw_sem, weight_sem, send_sem, cross_sem, near_sem, hand_sem, pack_send, pack_recv, chain_send, chain_recv,
    rim_sem, stat_send, stat_recv, back_send, lent_sem, back_sem, close_sem, first_send, first_recv, first_done,
):
    block, depth = tokens_ref.shape
    piece = block // SENDS
    raws = []
    for i, rows in enumerate((pl.ds(0, piece), pl.ds(piece, block - piece))):
        raws.append(pltpu.make_async_copy(tokens_ref.at[rows, :], raw.at[rows, :], raw_sem.at[i]))
        raws[i].start()
    smalls = []
    for i, (far, near) in enumerate((
        (gain_in, gain_ref), (gap_in, gap_ref), (shift_in, shift_ref), (taps_in, taps_ref),
        (conv_gain_in, conv_gain_ref), (head_gain_in, head_gain_ref),
    )):
        smalls.append(pltpu.make_async_copy(far, near, small_sem.at[i]))
        smalls[i].start()
    sources = (w0, w1, w2, w3, w4, w5)
    width = gap_ref.shape[1]
    fetched = [pltpu.make_async_copy(w, weight.at[i], weight_sem.at[i]) for i, w in enumerate(sources)]
    for i, w in enumerate((rec_rows, conv_rows)):
        fetched.append(
            pltpu.make_async_copy(w, merge.at[pl.ds(i * width, width), :], weight_sem.at[len(sources) + i])
        )
    me, count = lax.axis_index("tp"), lax.axis_size("sp")
    pair = me + 1 - 2 * lax.rem(me, 2)
    cross, diag = lax.rem(me + 2, 4), lax.rem(pair + 2, 4)
    at = lax.axis_index("sp")
    side, team, teams = lax.rem(at, 2), at // 2, count // 2
    mate = at + 1 - 2 * side
    barrier = pltpu.get_barrier_semaphore()
    for other in (pair, cross, diag):
        pl.semaphore_signal(barrier, inc=1, device_id={"tp": other}, device_id_type=MESH)
    pl.semaphore_signal(barrier, inc=1, device_id={"sp": mate}, device_id_type=MESH)

    @pl.when(team > 0)
    def _():
        pl.semaphore_signal(barrier, inc=1, device_id={"sp": at - 2}, device_id_type=MESH)

    @pl.when((team > 0) & (side == 0))
    def _():
        pl.semaphore_signal(barrier, inc=1, device_id={"sp": at - 1}, device_id_type=MESH)

    onward = team < teams - 1
    pl.semaphore_wait(barrier, jnp.where(onward, jnp.where(side == 1, 6, 5), 4))

    rows_all = proj.shape[1]
    heads, chunks = width // head, rows_all // CHUNK
    bigs = block // CHUNK
    per = CHUNK // piece
    channels = width * lax.axis_size("tp")
    lanes_of = [slice(g * LANES, (g + 1) * LANES) for g in range(width // LANES)]

    def remote(source, target, sends, recvs, axis, device):
        return pltpu.make_async_remote_copy(
            src_ref=source, dst_ref=target, send_sem=sends, recv_sem=recvs,
            device_id={axis: device}, device_id_type=MESH,
        )

    smalls[0].wait()

    crossing, nearby, handed = [], [], []
    for p in range(SENDS):
        rows = pl.ds(p * piece, piece)
        if p < 2:
            raws[p].wait()
        if p == 1:
            for one in fetched:
                one.start()
        near_rows[0, rows, :] = layer_norm(raw[rows, :], gain_ref[...]).astype(jnp.bfloat16)
        big, low = p // per, (p % per) * piece
        landing = far_rows.at[big, pl.ds(low, piece), :]
        crossing.append(remote(near_rows.at[0, rows, :], landing, send_sem.at[0], cross_sem.at[p], "tp", cross))
        nearby.append(
            remote(
                near_rows.at[0, rows, :], near_rows.at[1, rows, :], send_sem.at[1], near_sem.at[0], "tp", pair
            )
        )
        handed.append(
            remote(
                landing, far_rows.at[big, pl.ds(CHUNK + low, piece), :],
                send_sem.at[2], hand_sem.at[big], "tp", pair,
            )
        )
        crossing[p].start()
        nearby[p].start()
    for one in smalls[1:]:
        one.wait()

    def project(values, first, last, places, ready=False):
        def step(k, carry):
            for i in (first + 2 * k, first + 2 * k + 1):
                if ready:
                    for one in range(first, last):
                        pl.when(i == one)(fetched[one].wait)
            for i in (first + 2 * k, first + 2 * k + 1):
                result = dot(values[...], weight[i]).astype(jnp.bfloat16)
                for start, row, size in places:
                    proj[i, pl.ds(pl.multiple_of(row, CHUNK), size), :] = result[start : start + size]
            return carry

        lax.fori_loop(0, (last - first) // 2, step, 0)

    def pass_on(p):
        crossing[p].wait_recv()
        handed[p].start()

    def handed_in(big):
        part = far_rows.at[big, pl.ds(CHUNK, CHUNK), :]
        remote(part, part, send_sem.at[2], hand_sem.at[big], "tp", pair).wait_recv()

    row_at = lax.broadcasted_iota(jnp.int32, (CHUNK, CHUNK), 0)
    col_at = lax.broadcasted_iota(jnp.int32, (CHUNK, CHUNK), 1)
    causal = row_at >= col_at
    lower = jnp.where(causal, 1.0, 0.0).astype(jnp.bfloat16)
    lower = jnp.concatenate([lower, lower], axis=1)

    parts = [slice(h * head, (h + 1) * head) for h in range(heads)]

    def rows_of(c):
        return pl.ds(pl.multiple_of(c * CHUNK, CHUNK), CHUNK)

    def state_part(several, group=None):
        group = list(range(heads)) if group is None else group
        wide = slice(group[0] * head, (group[-1] + 1) * head)
        keys, totals = [], []
        for c in several:
            rows = rows_of(c)
            key = gap_ref[:, wide] * jax.nn.sigmoid(-proj[FORGET, rows, wide].astype(jnp.float32))
            shift = [jnp.broadcast_to(shift_ref[h : h + 1, rows], (head, CHUNK)).T for h in group]
            log = jnp.log1p(-key) + jnp.concatenate(shift, axis=1)
            high = log.astype(jnp.bfloat16)
            low = (log - high.astype(jnp.float32)).astype(jnp.bfloat16)
            keys.append(key)
            totals.append(dot(lower, jnp.concatenate([high, low], axis=0)))
        for c, key, total in zip(several, keys, totals):
            rows = rows_of(c)
            last = total[CHUNK - 1 : CHUNK, :]
            middle = total[CHUNK // 2 - 1 : CHUNK // 2, :]
            total = total - middle
            key_mid = key * jnp.exp(-total)
            intra[rows, wide] = total
            reach[rows, wide] = key_mid.astype(jnp.bfloat16)
            key_end = (key_mid * jnp.exp(last - middle)).astype(jnp.bfloat16)
            for i, h in enumerate(group):
                local[c, h] = dot(proj[VALUE, rows, parts[h]], key_end[:, parts[i]], ((0,), (0,)))
            closing[c, :, wide] = last
            centre[c, :, wide] = middle

    def query_part(several):
        queries, scores = [], []
        for c in several:
            rows = rows_of(c)
            query = proj[QUERY, rows, :].astype(jnp.float32)
            query = query * jax.nn.sigmoid(query) * jnp.exp(intra[rows, :])
            queries.append(query)
            query = query.astype(jnp.bfloat16)
            scores.append([dot(query[:, part], reach[rows, part], ((1,), (1,))) for part in parts])
        for c, query, score in zip(several, queries, scores):
            rows = rows_of(c)
            for part, one in zip(parts, score):
                one = jnp.where(causal, one, 0.0).astype(jnp.bfloat16)
                intra[rows, part] = dot(one, proj[VALUE, rows, part])
            reach[rows, :] = (query * jnp.exp(centre[c])).astype(jnp.bfloat16)

    def chunk_loop(first, number):
        def step(i, carry):
            several = [first + 2 * i, first + 2 * i + 1]
            state_part(several)
            query_part(several)
            return carry

        lax.fori_loop(0, number // 2, step, 0)

    def mix(first, size):
        def step(i, carry):
            row = pl.multiple_of(first + i * TILE, TILE)
            for g, lanes in enumerate(lanes_of):
                gate = proj[GLU_GATE, pl.ds(row, TILE), lanes].astype(jnp.float32)
                value = proj[GLU_VALUE, pl.ds(row, TILE), lanes].astype(jnp.float32)
                mixed = (value * jax.nn.sigmoid(gate)).astype(jnp.bfloat16)
                padded[g, pl.ds(pl.multiple_of(row + REACH, 8), TILE), :] = mixed.astype(jnp.float32)
            return carry

        lax.fori_loop(0, size // TILE, step, 0)

    taps = taps_ref.shape[0]
    skip = REACH - taps + 1

    def filter_rows(row0, number):
        def step(i, carry):
            g, row = i // number, row0 + lax.rem(i, number) * TILE
            lanes = pl.ds(pl.multiple_of(g * LANES, LANES), LANES)
            total = jnp.zeros((TILE, LANES), jnp.float32)
            for j in range(taps):
                total = total + taps_ref[j : j + 1, lanes] * padded[g, pl.ds(row + (j + skip), TILE), :]
            filtered[pl.ds(pl.multiple_of(row, TILE), TILE), lanes] = total
            return carry

        lax.fori_loop(0, len(lanes_of) * number, step, 0)

    def tally(t):
        base = pl.multiple_of(t * LANES, LANES)
        sums = jnp.zeros((LANES, LANES), jnp.float32)
        squares = jnp.zeros((LANES, LANES), jnp.float32)
        for lanes in lanes_of:
            value = filtered[pl.ds(base, LANES), lanes]
            sums = sums + value
            squares = squares + value * value
        own_stats[0:1, pl.ds(base, LANES)] = jnp.sum(sums.T, axis=0, keepdims=True)
        own_stats[1:2, pl.ds(base, LANES)] = jnp.sum(squares.T, axis=0, keepdims=True)

    def filter_tile(t):
        filter_rows(pl.multiple_of(t * LANES, LANES), LANES // TILE)
        tally(t)

    def filter_loop(first, number):
        def step(i, carry):
            filter_tile(first + i)
            return carry

        lax.fori_loop(0, number, step, 0)

    chip = 2 * block
    own_half = (me // 2) * chip
    far_half = chip - own_half if rows_all == 2 * chip else lax.rem(own_half + chip, rows_all)
    half_tiles = chip // LANES

    project(near_rows.at[0], 0, len(sources), [(0, me * block, block)], ready=True)
    remote(near_rows.at[0], near_rows.at[1], send_sem.at[1], near_sem.at[0], "tp", pair).wait_recv()
    project(near_rows.at[1], 0, len(sources), [(0, pair * block, block)])
    pass_on(0)
    chunk_loop(own_half // CHUNK, chip // CHUNK)
    for p in range(1, per - 1):
        pass_on(p)
    mix(own_half, chip)
    filter_loop(own_half // LANES + 1, half_tiles - 2)
    pass_on(per - 1)

    def far_places(big):
        return [(0, cross * block + big * CHUNK, CHUNK), (CHUNK, diag * block + big * CHUNK, CHUNK)]

    def far_chunks(big):
        return [owner * bigs + big for owner in (cross, diag)]

    far_tile = far_half // LANES
    for big in range(bigs - 1):
        begin = big * per
        handed_in(big)
        project(far_rows.at[big], 0, len(sources), far_places(big))
        pass_on(begin + per)
        state_part(far_chunks(big))
        query_part(far_chunks(big))
        for _, row, size in far_places(big):
            mix(row, size)
        for p in range(begin + per + 1, begin + 2 * per - 2):
            pass_on(p)
        if big == bigs - 2:
            filter_tile(own_half // LANES + half_tiles - 1)
            for tile in (own_half // LANES, far_tile, far_tile + bigs):
                filter_rows(pl.multiple_of(tile * LANES + TILE, TILE), 1)
        for p in range(begin + 2 * per - 2, begin + 2 * per):
            pass_on(p)
    handed_in(bigs - 1)
    project(far_rows.at[bigs - 1], 0, 2, far_places(bigs - 1))

    place = lax.broadcasted_iota(jnp.int32, (PAD, head), 0)
    half = head // 2
    units = [(h, k) for h in range(heads) for k in range(2)]
    spans = (pl.ds(0, PAD + half), pl.ds(PAD + half, half))
    packs = [
        remote(pack.at[h, spans[k], :], pack_in.at[h, spans[k], :], pack_send.at[0], pack_recv.at[h, k], "sp", mate)
        for h, k in units
    ]
    def send_state(h):
        part = slice(h * head, (h + 1) * head)
        state, log = local[0, h], closing[0, :, part]
        for c in range(1, chunks):
            state = state * jnp.exp(closing[c, :, part]) + local[c, h]
            log = log + closing[c, :, part]
        own_state[h] = state
        own_log[:, part] = log
        pack[h, PAD : PAD + head, :] = state.astype(jnp.bfloat16)
        high = log.astype(jnp.bfloat16).astype(jnp.float32)
        rest = log - high
        mid = rest.astype(jnp.bfloat16).astype(jnp.float32)
        low = rest - mid
        tail = jnp.where(place == 0, high, jnp.where(place == 1, mid, jnp.where(place == 2, low, 0.0)))
        pack[h, 0:PAD, :] = tail.astype(jnp.bfloat16)
        packs[2 * h].start()
        packs[2 * h + 1].start()

    state_part(far_chunks(bigs - 1))
    for h in range(heads):
        send_state(h)
    project(far_rows.at[bigs - 1], 2, 4, far_places(bigs - 1))
    for _, row, size in far_places(bigs - 1):
        mix(row, size)
    for g, lanes in enumerate(lanes_of):
        rim[0, :, lanes] = padded[g, rows_all : rows_all + REACH, :].astype(jnp.bfloat16)
    edge = remote(rim.at[0], rim.at[1], rim_sem.at[0], rim_sem.at[1], "sp", lax.rem(at + 1, count))
    ahead = onward | (side == 0)
    pl.when(ahead)(edge.start)

    links = [
        remote(
            chain_out.at[h, pl.ds(k * half, half), :], chain_in.at[h, pl.ds(k * half, half), :],
            chain_send.at[0], chain_recv.at[h, k], "sp", lax.rem(at + 2, count),
        )
        for h, k in units
    ]

    def mate_log(h):
        tail = pack_in[h, 0:PAD, :].astype(jnp.float32)
        return tail[0:1] + tail[1:2] + tail[2:3]

    def meet(u):
        h, k = units[u]
        some = pl.ds(k * half, half)
        packs[u].wait_recv()
        theirs, log = pack_in[h, PAD + k * half : PAD + (k + 1) * half, :].astype(jnp.float32), mate_log(h)
        ours, own = own_state[h, some, :], own_log[:, parts[h]]
        first = jnp.where(side == 0, ours, theirs)
        second = jnp.where(side == 0, theirs, ours)
        group = first * jnp.exp(jnp.where(side == 0, log, own)) + second
        group_state[h, some, :] = group
        if k == 0:
            group_log[:, parts[h]] = log + own

        @pl.when(team == 0)
        def _():
            chain_in[h, some, :] = jnp.zeros((half, head), jnp.bfloat16)
            chain_out[h, some, :] = group.astype(jnp.bfloat16)
            links[u].start()

    def relay(k, first, last):
        @pl.when(team == k)
        def _():
            for u in range(first, last):
                h, some = units[u][0], pl.ds(units[u][1] * half, half)
                links[u].wait_recv()
                if k < teams - 1:
                    step = chain_in[h, some, :].astype(jnp.float32) * jnp.exp(group_log[:, parts[h]])
                    chain_out[h, some, :] = (step + group_state[h, some, :]).astype(jnp.bfloat16)
                    links[u].start()

    def rim_in():
        pl.when(at > 0)(edge.wait_recv)
        for g, lanes in enumerate(lanes_of):
            padded[g, 0:REACH, :] = jnp.where(at > 0, rim[1, :, lanes].astype(jnp.float32), 0.0)

    stats = [
        remote(own_stats, other_stats.at[k - 1], stat_send.at[0], stat_recv.at[0], "tp", lax.rem(me + k, 4))
        for k in range(1, 4)
    ]
    number = len(units)
    def low_half(t):
        filter_rows(pl.multiple_of(t * LANES, LANES), 1)

    def high_half(t):
        filter_rows(pl.multiple_of(t * LANES + TILE, TILE), 1)
        tally(t)

    def low_rest(t):
        low_half(t)
        tally(t)

    whole_tiles = [far_tile + b * bigs + j for b in range(2) for j in range(1, bigs)]
    work = []
    for t in whole_tiles:
        work += [functools.partial(low_half, t), functools.partial(high_half, t)]
    work.insert(2, functools.partial(low_rest, far_tile + bigs))
    last_work = [rim_in, functools.partial(low_rest, own_half // LANES), functools.partial(low_rest, far_tile)]
    for _ in range(3):
        work.pop(0)()
    work += last_work
    for u in range(number):
        meet(u)
        if work and u != 3:
            work.pop(0)()
    for one in work:
        one()
    for one in stats:
        one.start()
    relay(1, 0, number)
    if teams > 3:
        relay(2, 0, number)
    all_stats = remote(other_stats, other_stats, stat_send.at[0], stat_recv.at[0], "tp", pair)
    all_stats.wait_recv()

    def stats_tile(i):
        row = pl.multiple_of(i * LANES, LANES)
        total = own_stats[:, pl.ds(row, LANES)]
        for k in range(3):
            total = total + other_stats[k, :, pl.ds(row, LANES)]
        mean = total[0:1] / channels
        scale = lax.rsqrt(total[1:2] / channels - mean * mean + norm_epsilon)
        for k, value in enumerate((mean, scale)):
            moments[k, pl.ds(row, LANES), :] = jnp.broadcast_to(value, (LANES, LANES)).T

    for owner in (diag, cross):
        stats_tile(owner * bigs)

    def conv_part(owner, low, size, slot):
        rows, target = pl.ds(pl.multiple_of(owner * block + low, size), size), pl.ds(slot, size)
        for g, lanes in enumerate(lanes_of):
            normed = (filtered[rows, lanes] - moments[0, rows, :]) * moments[1, rows, :] * conv_gain_ref[:, lanes]
            blend[target, width + g * LANES : width + (g + 1) * LANES] = (normed * jax.nn.sigmoid(normed)).astype(
                jnp.bfloat16
            )

    columns = merge.shape[1]
    turn = block // RETURNS

    def spread(size, put, first=0, last=2 * width):
        def step(j, carry):
            cols = pl.ds(pl.multiple_of(j * SPAN, SPAN), SPAN)
            put(cols, dot(blend[0:size, first:last], merge[first:last, cols]))
            return carry

        lax.fori_loop(0, columns // SPAN, step, 0)

    for one in fetched[len(sources) :]:
        one.wait()
    conv_part(diag, 0, turn, 0)
    conv_part(cross, 0, turn, turn)

    def put_early(cols, result):
        early[:, cols] = result

    spread(2 * turn, put_early, first=width)
    for k in range(3 if teams > 3 else 2, teams):
        relay(k, 0, number)

    for h in range(heads):
        part = slice(h * head, (h + 1) * head)
        state = chain_in[h].astype(jnp.float32)
        moved = state * jnp.exp(mate_log(h)) + pack_in[h, PAD : PAD + head, :].astype(jnp.float32)
        state = jnp.where(side == 1, moved, state)
        for c in range(chunks):
            enter[c, h] = state.astype(jnp.bfloat16)
            if c < chunks - 1:
                state = state * jnp.exp(closing[c, :, part]) + local[c, h]

    def rec_part(owner, low, size, slot):
        rows, target = pl.ds(pl.multiple_of(owner * block + low, size), size), pl.ds(slot, size)
        c = owner * bigs + low // CHUNK
        for h, part in enumerate(parts):
            rec = intra[rows, part] + dot(reach[rows, part], enter[c, h], ((1,), (1,)))
            rec = rec * lax.rsqrt(jnp.mean(rec * rec, axis=-1, keepdims=True) + head_epsilon) * head_gain_ref[...]
            gate = proj[RGATE, rows, part].astype(jnp.float32)
            blend[target, part] = (rec * (gate * jax.nn.sigmoid(gate))).astype(jnp.bfloat16)

    def finish_rows(owner, low, size, slot):
        rec_part(owner, low, size, slot)
        conv_part(owner, low, size, slot)

    lent, returned, close = {}, {}, []

    def settle(p):
        rows = pl.ds(p * turn, turn)
        lent[p].wait_recv()
        to_cross[rows, :] = (held[p % 2] + from_pair[0, rows, :].astype(jnp.float32)).astype(jnp.bfloat16)
        returned[p] = remote(
            to_cross.at[rows, :], from_cross.at[rows, :], back_send.at[1], back_sem.at[p - 1], "tp", cross
        )
        returned[p].start()

    late = (bigs - 1) * CHUNK // turn
    head_rows = pl.ds(0, turn)
    first_lent, first_returned = [], []
    rec_part(diag, 0, turn, 0)
    rec_part(cross, 0, turn, turn)
    for j in range(columns // SPAN):
        cols = slice(j * SPAN, (j + 1) * SPAN)
        result = dot(blend[0 : 2 * turn, 0:width], merge[0:width, cols]) + early[:, cols]
        to_pair[0, head_rows, cols] = result[0:turn].astype(jnp.bfloat16)
        held[0, :, cols] = result[turn : 2 * turn]
        first_lent.append(
            remote(
                to_pair.at[0, head_rows, cols], from_pair.at[0, head_rows, cols],
                first_send.at[0], first_recv.at[j], "tp", pair,
            )
        )
        first_lent[j].start()
    for j in range(columns // SPAN):
        cols = slice(j * SPAN, (j + 1) * SPAN)
        first_lent[j].wait_recv()
        to_cross[head_rows, cols] = (held[0, :, cols] + from_pair[0, head_rows, cols].astype(jnp.float32)).astype(
            jnp.bfloat16
        )
        first_returned.append(
            remote(
                to_cross.at[head_rows, cols], from_cross.at[head_rows, cols],
                first_send.at[1], first_done.at[0], "tp", cross,
            )
        )
        first_returned[j].start()
    for p in range(1, RETURNS):
        rows = pl.ds(p * turn, turn)
        if p == late:
            settle(p - 1)
            project(far_rows.at[bigs - 1], 4, len(sources), far_places(bigs - 1))
            query_part(far_chunks(bigs - 1))
            for owner in (diag, cross):
                for big in range(1, bigs):
                    stats_tile(owner * bigs + big)
        finish_rows(diag, p * turn, turn, 0)
        finish_rows(cross, p * turn, turn, turn)
        if p > 1 and p != late:
            settle(p - 1)

        def put(cols, result, p=p, rows=rows):
            to_pair[0, rows, cols] = result[0:turn].astype(jnp.bfloat16)
            held[p % 2, :, cols] = result[turn : 2 * turn]

        spread(2 * turn, put)
        lent[p] = remote(
            to_pair.at[0, rows, :], from_pair.at[0, rows, :], back_send.at[0], lent_sem.at[p - 1], "tp", pair
        )
        lent[p].start()
    settle(RETURNS - 1)
    for owner in (pair, me):
        for big in range(bigs):
            stats_tile(owner * bigs + big)
    for big in range(bigs):
        rows = pl.ds(big * CHUNK, CHUNK)
        finish_rows(pair, big * CHUNK, CHUNK, 0)
        finish_rows(me, big * CHUNK, CHUNK, CHUNK)

        def put(cols, result, rows=rows):
            to_pair[1, rows, cols] = result[0:CHUNK].astype(jnp.bfloat16)
            mine[rows, cols] = result[CHUNK : 2 * CHUNK]

        spread(2 * CHUNK, put)
        close.append(
            remote(
                to_pair.at[1, rows, :], from_pair.at[1, rows, :], back_send.at[2], close_sem.at[big],
                "tp", pair,
            )
        )
        close[big].start()
    for big in range(bigs):
        rows = pl.ds(big * CHUNK, CHUNK)
        close[big].wait_recv()
        mine[rows, :] = mine[rows, :] + from_pair[1, rows, :].astype(jnp.float32)
    first_whole = remote(
        to_cross.at[head_rows, :], from_cross.at[head_rows, :], first_send.at[1], first_done.at[0], "tp", cross
    )
    for p in range(RETURNS):
        rows = pl.ds(p * turn, turn)
        (first_whole if p == 0 else returned[p]).wait_recv()
        out_ref[rows, :] = (mine[rows, :] + from_cross[rows, :].astype(jnp.float32)).astype(jnp.bfloat16)

    def sent(ref, sem):
        remote(ref, ref, sem, near_sem.at[0], "tp", pair).wait_send()

    rest = pl.ds(turn, block - turn)
    for k in range(3):
        sent(near_rows.at[0], send_sem.at[k])
    sent(pack, pack_send.at[0])
    sent(other_stats, stat_send.at[0])
    sent(to_pair.at[0, head_rows, :], first_send.at[0])
    sent(to_cross.at[head_rows, :], first_send.at[1])
    sent(to_pair.at[0, rest, :], back_send.at[0])
    sent(to_cross.at[rest, :], back_send.at[1])
    sent(to_pair.at[1], back_send.at[2])
    pl.when(ahead)(edge.wait_send)

    @pl.when(onward)
    def _():
        sent(chain_out, chain_send.at[0])


def on_device(
    tokens, norm_gain, w_query, w_forget, w_value, w_rgate, w_glu_value, w_glu_gate, forget_gap,
    decay_shift, head_gain, conv_taps, conv_gain, out_rec, out_conv,
):
    weights = (w_forget, w_value, w_glu_value, w_glu_gate, w_query, w_rgate)
    block, depth = tokens.shape
    width, columns = out_rec.shape
    head = head_gain.shape[0]
    heads = width // head
    rows = block * lax.axis_size("tp")
    groups = width // LANES
    chunks = rows // CHUNK
    turn = block // RETURNS
    bf16, f32 = jnp.bfloat16, jnp.float32
    vmem = lambda shape, kind: pltpu.VMEM(shape, kind)
    sems = lambda *shape: pltpu.SemaphoreType.DMA(shape)
    return pl.pallas_call(
        functools.partial(layer_kernel, head),
        in_specs=[pl.BlockSpec(memory_space=pl.ANY)] * 15,
        out_specs=pl.BlockSpec(memory_space=pltpu.VMEM),
        out_shape=pltpu.VMEM((block, columns), bf16),
        scratch_shapes=[
            vmem((1, depth), f32),
            vmem((1, width), f32),
            vmem((heads, rows), f32),
            vmem(conv_taps.shape, f32),
            vmem((1, width), f32),
            vmem((1, head), f32),
            vmem((block, depth), bf16),
            vmem((2, block, depth), bf16),
            vmem((block // CHUNK, 2 * CHUNK, depth), bf16),
            vmem((len(weights), depth, width), bf16),
            vmem((2 * width, columns), bf16),
            vmem((len(weights), rows, width), bf16),
            vmem((rows, width), f32),
            vmem((rows, width), bf16),
            vmem((chunks, heads, head, head), f32),
            vmem((chunks, 1, width), f32),
            vmem((chunks, 1, width), f32),
            vmem((chunks, heads, head, head), bf16),
            vmem((heads, head, head), f32),
            vmem((1, width), f32),
            vmem((heads, head + PAD, head), bf16),
            vmem((heads, head + PAD, head), bf16),
            vmem((heads, head, head), f32),
            vmem((1, width), f32),
            vmem((heads, head, head), bf16),
            vmem((heads, head, head), bf16),
            vmem((2, REACH, width), bf16),
            vmem((groups, REACH + rows, LANES), f32),
            vmem((rows, width), f32),
            vmem((2, rows), f32),
            vmem((3, 2, rows), f32),
            vmem((2, rows, LANES), f32),
            vmem((2 * CHUNK, 2 * width), bf16),
            vmem((2 * turn, columns), f32),
            vmem((2, turn, columns), f32),
            vmem((2, block, columns), bf16),
            vmem((2, block, columns), bf16),
            vmem((block, columns), bf16),
            vmem((block, columns), bf16),
            vmem((block, columns), f32),
            sems(6),
            sems(2),
            sems(len(weights) + 2),
            sems(3),
            sems(SENDS),
            sems(1),
            sems(block // CHUNK),
            sems(1),
            sems(heads, 2),
            sems(1),
            sems(heads, 2),
            sems(2),
            sems(1),
            sems(1),
            sems(3),
            sems(RETURNS - 1),
            sems(RETURNS - 1),
            sems(block // CHUNK),
            sems(2),
            sems(columns // SPAN),
            sems(1),
        ],
        compiler_params=pltpu.CompilerParams(
            collective_id=0, has_side_effects=True, vmem_limit_bytes=58000 * 1024
        ),
    )(
        norm_gain[None], forget_gap[None], decay_shift.T, conv_taps, conv_gain[None], head_gain[None],
        tokens, *weights, out_rec, out_conv,
    )


def solution(mesh):
    placed = (
        P(("sp", "tp"), None),
        P(),
        P(None, "tp"),
        P(None, "tp"),
        P(None, "tp"),
        P(None, "tp"),
        P(None, "tp"),
        P(None, "tp"),
        P("tp"),
        P("sp", "tp"),
        P(),
        P(None, "tp"),
        P("tp"),
        P("tp", None),
        P("tp", None),
    )
    return jax.shard_map(
        on_device, mesh=mesh, in_specs=placed, out_specs=P(("sp", "tp"), None), check_vma=False
    )
```

```python
import functools

import jax
import jax.numpy as jnp
from jax import lax
from jax.experimental import pallas as pl
from jax.experimental.pallas import tpu as pltpu
from jax.sharding import PartitionSpec as P

CHUNK = 128
SENDS = 8
RETURNS = 4
REACH = 32
TILE = 64
LANES = 128
SPAN = 512
MESH = pl.DeviceIdType.MESH
FORGET, VALUE, GLU_VALUE, GLU_GATE, QUERY, RGATE = range(6)

norm_epsilon = 1e-05
head_epsilon = 1e-06


def dot(a, b, dims=((1,), (0,))):
    return lax.dot_general(a, b, (dims, ((), ())), preferred_element_type=jnp.float32)


def layer_norm(values, gain):
    widened = values.astype(jnp.float32)
    row_mean = jnp.mean(widened, axis=-1, keepdims=True)
    centred = widened - row_mean
    row_var = jnp.mean(centred * centred, axis=-1, keepdims=True)
    return centred * lax.rsqrt(row_var + norm_epsilon) * gain


def layer_kernel(
    head, gain_in, gap_in, shift_in, taps_in, conv_gain_in, head_gain_in,
    tokens_ref, w0, w1, w2, w3, w4, w5, rec_rows, conv_rows, out_ref,
    gain_ref, gap_ref, shift_ref, taps_ref, conv_gain_ref, head_gain_ref,
    raw, near_rows, far_rows, weight, merge, proj, intra, reach, local, closing, centre, enter,
    own_state, own_log, pack, pack_in, log_in, decay, prefix, group_state, group_log, chain_out, chain_in,
    rim, padded, filtered, own_stats, other_stats, moments,
    blend, early, held, to_pair, from_pair, to_cross, from_cross, mine,
    small_sem, raw_sem, weight_sem, log_sem, send_sem, cross_sem, near_sem, hand_sem, pack_send, pack_recv, chain_send, chain_recv,
    rim_sem, stat_send, stat_recv, back_send, lent_sem, back_sem, close_sem, first_send, first_recv, first_done,
):
    block, depth = tokens_ref.shape
    piece = block // SENDS
    raws = []
    for i, rows in enumerate((pl.ds(0, piece), pl.ds(piece, block - piece))):
        raws.append(pltpu.make_async_copy(tokens_ref.at[rows, :], raw.at[rows, :], raw_sem.at[i]))
        raws[i].start()
    smalls = []
    for i, (far, near) in enumerate((
        (gain_in, gain_ref), (gap_in, gap_ref), (shift_in, shift_ref), (taps_in, taps_ref),
        (conv_gain_in, conv_gain_ref), (head_gain_in, head_gain_ref),
    )):
        smalls.append(pltpu.make_async_copy(far, near, small_sem.at[i]))
        smalls[i].start()
    sources = (w0, w1, w2, w3, w4, w5)
    width = gap_ref.shape[1]
    fetched = [pltpu.make_async_copy(w, weight.at[i], weight_sem.at[i]) for i, w in enumerate(sources)]
    for i, w in enumerate((rec_rows, conv_rows)):
        fetched.append(
            pltpu.make_async_copy(w, merge.at[pl.ds(i * width, width), :], weight_sem.at[len(sources) + i])
        )
    me, count = lax.axis_index("tp"), lax.axis_size("sp")
    pair = me + 1 - 2 * lax.rem(me, 2)
    cross, diag = lax.rem(me + 2, 4), lax.rem(pair + 2, 4)
    at = lax.axis_index("sp")
    side, team, teams = lax.rem(at, 2), at // 2, count // 2
    mate = at + 1 - 2 * side
    barrier = pltpu.get_barrier_semaphore()
    for other in (pair, cross, diag):
        pl.semaphore_signal(barrier, inc=1, device_id={"tp": other}, device_id_type=MESH)
    pl.semaphore_signal(barrier, inc=1, device_id={"sp": mate}, device_id_type=MESH)

    @pl.when(team > 0)
    def _():
        pl.semaphore_signal(barrier, inc=1, device_id={"sp": at - 2}, device_id_type=MESH)

    @pl.when((team > 0) & (side == 0))
    def _():
        pl.semaphore_signal(barrier, inc=1, device_id={"sp": at - 1}, device_id_type=MESH)

    onward = team < teams - 1
    pl.semaphore_wait(barrier, jnp.where(onward, jnp.where(side == 1, 6, 5), 4))

    rows_all = proj.shape[1]
    heads, chunks = width // head, rows_all // CHUNK
    bigs = block // CHUNK
    per = CHUNK // piece
    channels = width * lax.axis_size("tp")
    lanes_of = [slice(g * LANES, (g + 1) * LANES) for g in range(width // LANES)]

    def remote(source, target, sends, recvs, axis, device):
        return pltpu.make_async_remote_copy(
            src_ref=source, dst_ref=target, send_sem=sends, recv_sem=recvs,
            device_id={axis: device}, device_id_type=MESH,
        )

    smalls[0].wait()

    crossing, nearby, handed = [], [], []
    for p in range(SENDS):
        rows = pl.ds(p * piece, piece)
        if p < 2:
            raws[p].wait()
        if p == 1:
            for one in fetched:
                one.start()
        near_rows[0, rows, :] = layer_norm(raw[rows, :], gain_ref[...]).astype(jnp.bfloat16)
        big, low = p // per, (p % per) * piece
        landing = far_rows.at[big, pl.ds(low, piece), :]
        crossing.append(remote(near_rows.at[0, rows, :], landing, send_sem.at[0], cross_sem.at[p], "tp", cross))
        nearby.append(
            remote(
                near_rows.at[0, rows, :], near_rows.at[1, rows, :], send_sem.at[1], near_sem.at[0], "tp", pair
            )
        )
        handed.append(
            remote(
                landing, far_rows.at[big, pl.ds(CHUNK + low, piece), :],
                send_sem.at[2], hand_sem.at[big], "tp", pair,
            )
        )
        crossing[p].start()
        nearby[p].start()
    for one in smalls[1:]:
        one.wait()

    def project(values, first, last, places, ready=False):
        def step(k, carry):
            for i in (first + 2 * k, first + 2 * k + 1):
                if ready:
                    for one in range(first, last):
                        pl.when(i == one)(fetched[one].wait)
            for i in (first + 2 * k, first + 2 * k + 1):
                result = dot(values[...], weight[i]).astype(jnp.bfloat16)
                for start, row, size in places:
                    proj[i, pl.ds(pl.multiple_of(row, CHUNK), size), :] = result[start : start + size]
            return carry

        lax.fori_loop(0, (last - first) // 2, step, 0)

    def pass_on(p):
        crossing[p].wait_recv()
        handed[p].start()

    def handed_in(big):
        part = far_rows.at[big, pl.ds(CHUNK, CHUNK), :]
        remote(part, part, send_sem.at[2], hand_sem.at[big], "tp", pair).wait_recv()

    row_at = lax.broadcasted_iota(jnp.int32, (CHUNK, CHUNK), 0)
    col_at = lax.broadcasted_iota(jnp.int32, (CHUNK, CHUNK), 1)
    causal = row_at >= col_at
    lower = jnp.where(causal, 1.0, 0.0).astype(jnp.bfloat16)
    lower = jnp.concatenate([lower, lower], axis=1)

    parts = [slice(h * head, (h + 1) * head) for h in range(heads)]

    def rows_of(c):
        return pl.ds(pl.multiple_of(c * CHUNK, CHUNK), CHUNK)

    def state_part(several, ready=None):
        keys, totals, values = [], [], []
        for k, c in enumerate(several):
            rows = rows_of(c)
            forget = proj[FORGET, rows, :] if ready is None else ready[0][k * CHUNK : (k + 1) * CHUNK]
            values.append(proj[VALUE, rows, :] if ready is None else ready[1][k * CHUNK : (k + 1) * CHUNK])
            key = gap_ref[...] * jax.nn.sigmoid(-forget.astype(jnp.float32))
            shift = [jnp.broadcast_to(shift_ref[h : h + 1, rows], (head, CHUNK)).T for h in range(heads)]
            log = jnp.log1p(-key) + jnp.concatenate(shift, axis=1)
            high = log.astype(jnp.bfloat16)
            low = (log - high.astype(jnp.float32)).astype(jnp.bfloat16)
            keys.append(key)
            totals.append(dot(lower, jnp.concatenate([high, low], axis=0)))
        for c, key, total, value in zip(several, keys, totals, values):
            rows = rows_of(c)
            last = total[CHUNK - 1 : CHUNK, :]
            middle = total[CHUNK // 2 - 1 : CHUNK // 2, :]
            total = total - middle
            key_mid = key * jnp.exp(-total)
            intra[rows, :] = total
            reach[rows, :] = key_mid.astype(jnp.bfloat16)
            key_end = (key_mid * jnp.exp(last - middle)).astype(jnp.bfloat16)
            for h, part in enumerate(parts):
                local[c, h] = dot(value[:, part], key_end[:, part], ((0,), (0,)))
            closing[c] = last
            centre[c] = middle

    def query_part(several):
        queries, scores = [], []
        for c in several:
            rows = rows_of(c)
            query = proj[QUERY, rows, :].astype(jnp.float32)
            query = query * jax.nn.sigmoid(query) * jnp.exp(intra[rows, :])
            queries.append(query)
            query = query.astype(jnp.bfloat16)
            scores.append([dot(query[:, part], reach[rows, part], ((1,), (1,))) for part in parts])
        for c, query, score in zip(several, queries, scores):
            rows = rows_of(c)
            for part, one in zip(parts, score):
                one = jnp.where(causal, one, 0.0).astype(jnp.bfloat16)
                intra[rows, part] = dot(one, proj[VALUE, rows, part])
            reach[rows, :] = (query * jnp.exp(centre[c])).astype(jnp.bfloat16)

    def chunk_loop(first, number):
        def step(i, carry):
            several = [first + 2 * i, first + 2 * i + 1]
            state_part(several)
            query_part(several)
            return carry

        lax.fori_loop(0, number // 2, step, 0)

    def mix(first, size):
        def step(i, carry):
            row = pl.multiple_of(first + i * TILE, TILE)
            for g, lanes in enumerate(lanes_of):
                gate = proj[GLU_GATE, pl.ds(row, TILE), lanes].astype(jnp.float32)
                value = proj[GLU_VALUE, pl.ds(row, TILE), lanes].astype(jnp.float32)
                mixed = (value * jax.nn.sigmoid(gate)).astype(jnp.bfloat16)
                padded[g, pl.ds(pl.multiple_of(row + REACH, 8), TILE), :] = mixed.astype(jnp.float32)
            return carry

        lax.fori_loop(0, size // TILE, step, 0)

    taps = taps_ref.shape[0]
    skip = REACH - taps + 1

    def filter_rows(row0, number):
        def step(i, carry):
            g, row = i // number, row0 + lax.rem(i, number) * TILE
            lanes = pl.ds(pl.multiple_of(g * LANES, LANES), LANES)
            total = jnp.zeros((TILE, LANES), jnp.float32)
            for j in range(taps):
                total = total + taps_ref[j : j + 1, lanes] * padded[g, pl.ds(row + (j + skip), TILE), :]
            filtered[pl.ds(pl.multiple_of(row, TILE), TILE), lanes] = total
            return carry

        lax.fori_loop(0, len(lanes_of) * number, step, 0)

    def tally(t):
        base = pl.multiple_of(t * LANES, LANES)
        sums = jnp.zeros((LANES, LANES), jnp.float32)
        squares = jnp.zeros((LANES, LANES), jnp.float32)
        for lanes in lanes_of:
            value = filtered[pl.ds(base, LANES), lanes]
            sums = sums + value
            squares = squares + value * value
        own_stats[0:1, pl.ds(base, LANES)] = jnp.sum(sums.T, axis=0, keepdims=True)
        own_stats[1:2, pl.ds(base, LANES)] = jnp.sum(squares.T, axis=0, keepdims=True)

    def filter_tile(t):
        filter_rows(pl.multiple_of(t * LANES, LANES), LANES // TILE)
        tally(t)

    def filter_loop(first, number):
        def step(i, carry):
            filter_tile(first + i)
            return carry

        lax.fori_loop(0, number, step, 0)

    chip = 2 * block
    own_half = (me // 2) * chip
    far_half = chip - own_half if rows_all == 2 * chip else lax.rem(own_half + chip, rows_all)
    half_tiles = chip // LANES

    project(near_rows.at[0], 0, len(sources), [(0, me * block, block)], ready=True)
    remote(near_rows.at[0], near_rows.at[1], send_sem.at[1], near_sem.at[0], "tp", pair).wait_recv()
    project(near_rows.at[1], 0, len(sources), [(0, pair * block, block)])
    pass_on(0)
    chunk_loop(own_half // CHUNK, chip // CHUNK)
    for p in range(1, per - 1):
        pass_on(p)
    mix(own_half, chip)
    filter_loop(own_half // LANES + 1, half_tiles - 2)
    pass_on(per - 1)

    def far_places(big):
        return [(0, cross * block + big * CHUNK, CHUNK), (CHUNK, diag * block + big * CHUNK, CHUNK)]

    def far_chunks(big):
        return [owner * bigs + big for owner in (cross, diag)]

    far_tile = far_half // LANES
    for big in range(bigs - 1):
        begin = big * per
        handed_in(big)
        project(far_rows.at[big], 0, len(sources), far_places(big))
        pass_on(begin + per)
        state_part(far_chunks(big))
        query_part(far_chunks(big))
        for _, row, size in far_places(big):
            mix(row, size)
        for p in range(begin + per + 1, begin + 2 * per - 2):
            pass_on(p)
        if big == bigs - 2:
            filter_tile(own_half // LANES + half_tiles - 1)
            for tile in (own_half // LANES, far_tile, far_tile + bigs):
                filter_rows(pl.multiple_of(tile * LANES + TILE, TILE), 1)
        for p in range(begin + 2 * per - 2, begin + 2 * per):
            pass_on(p)
    handed_in(bigs - 1)

    half = head // 2
    units = [(h, k) for h in range(heads) for k in range(2)]
    spans = (pl.ds(0, half), pl.ds(half, half))
    packs = [
        remote(pack.at[h, spans[k], :], pack_in.at[h, spans[k], :], pack_send.at[0], pack_recv.at[h, k], "sp", mate)
        for h, k in units
    ]
    def send_state(h):
        state = local[0, h]
        prefix[0, h] = jnp.zeros_like(state)
        for c in range(1, chunks):
            prefix[c, h] = state
            state = state * jnp.exp(closing[c, :, parts[h]]) + local[c, h]
        own_state[h] = state
        pack[h] = state.astype(jnp.bfloat16)
        packs[2 * h].start()
        packs[2 * h + 1].start()

    gates, inputs = [dot(far_rows[bigs - 1], weight[i]).astype(jnp.bfloat16) for i in (FORGET, VALUE)]
    for start, row, size in far_places(bigs - 1):
        proj[VALUE, pl.ds(pl.multiple_of(row, CHUNK), size), :] = inputs[start : start + size]
    state_part(far_chunks(bigs - 1), (gates, inputs))
    log = closing[0]
    for c in range(1, chunks):
        log = log + closing[c]
    own_log[...] = log
    logs = remote(own_log, log_in, log_sem.at[0], log_sem.at[1], "sp", mate)
    logs.start()
    for h in range(heads):
        send_state(h)
    log = jnp.zeros_like(log)
    for c in range(chunks):
        decay[c] = jnp.exp(log)
        log = log + closing[c]
    project(far_rows.at[bigs - 1], 2, 4, far_places(bigs - 1))
    for _, row, size in far_places(bigs - 1):
        mix(row, size)
    for g, lanes in enumerate(lanes_of):
        rim[0, :, lanes] = padded[g, rows_all : rows_all + REACH, :].astype(jnp.bfloat16)
    edge = remote(rim.at[0], rim.at[1], rim_sem.at[0], rim_sem.at[1], "sp", lax.rem(at + 1, count))
    ahead = onward | (side == 0)
    pl.when(ahead)(edge.start)

    links = [
        remote(
            chain_out.at[h, pl.ds(k * half, half), :], chain_in.at[h, pl.ds(k * half, half), :],
            chain_send.at[0], chain_recv.at[h, k], "sp", lax.rem(at + 2, count),
        )
        for h, k in units
    ]

    def mate_log(h):
        return log_in[:, parts[h]]

    def meet(u):
        h, k = units[u]
        some = pl.ds(k * half, half)
        if u == 0:
            logs.wait_recv()
        packs[u].wait_recv()
        theirs, log = pack_in[h, some, :].astype(jnp.float32), mate_log(h)
        ours, own = own_state[h, some, :], own_log[:, parts[h]]
        first = jnp.where(side == 0, ours, theirs)
        second = jnp.where(side == 0, theirs, ours)
        group = first * jnp.exp(jnp.where(side == 0, log, own)) + second
        group_state[h, some, :] = group
        if k == 0:
            group_log[:, parts[h]] = log + own

        @pl.when(team == 0)
        def _():
            chain_in[h, some, :] = jnp.zeros((half, head), jnp.bfloat16)
            chain_out[h, some, :] = group.astype(jnp.bfloat16)
            links[u].start()

    def relay(k, first, last):
        @pl.when(team == k)
        def _():
            for u in range(first, last):
                h, some = units[u][0], pl.ds(units[u][1] * half, half)
                links[u].wait_recv()
                if k < teams - 1:
                    step = chain_in[h, some, :].astype(jnp.float32) * jnp.exp(group_log[:, parts[h]])
                    chain_out[h, some, :] = (step + group_state[h, some, :]).astype(jnp.bfloat16)
                    links[u].start()

    def rim_in():
        pl.when(at > 0)(edge.wait_recv)
        for g, lanes in enumerate(lanes_of):
            padded[g, 0:REACH, :] = jnp.where(at > 0, rim[1, :, lanes].astype(jnp.float32), 0.0)

    stats = [
        remote(own_stats, other_stats.at[k - 1], stat_send.at[0], stat_recv.at[0], "tp", lax.rem(me + k, 4))
        for k in range(1, 4)
    ]
    number = len(units)
    def low_half(t):
        filter_rows(pl.multiple_of(t * LANES, LANES), 1)

    def high_half(t):
        filter_rows(pl.multiple_of(t * LANES + TILE, TILE), 1)
        tally(t)

    def low_rest(t):
        low_half(t)
        tally(t)

    whole_tiles = [far_tile + b * bigs + j for b in range(2) for j in range(1, bigs)]
    work = []
    for t in whole_tiles:
        work += [functools.partial(low_half, t), functools.partial(high_half, t)]
    work.insert(2, functools.partial(low_rest, far_tile + bigs))
    last_work = [rim_in, functools.partial(low_rest, own_half // LANES), functools.partial(low_rest, far_tile)]
    for _ in range(3):
        work.pop(0)()
    work += last_work
    for u in range(number):
        meet(u)
        if work and u != 3:
            work.pop(0)()
        if u >= 5:
            relay(1, u - 5, u - 4)
    for one in work:
        one()
    for one in stats:
        one.start()
    relay(1, number - 5, number)
    if teams > 3:
        relay(2, 0, number)
    all_stats = remote(other_stats, other_stats, stat_send.at[0], stat_recv.at[0], "tp", pair)
    all_stats.wait_recv()

    def stats_tile(i):
        row = pl.multiple_of(i * LANES, LANES)
        total = own_stats[:, pl.ds(row, LANES)]
        for k in range(3):
            total = total + other_stats[k, :, pl.ds(row, LANES)]
        mean = total[0:1] / channels
        scale = lax.rsqrt(total[1:2] / channels - mean * mean + norm_epsilon)
        for k, value in enumerate((mean, scale)):
            moments[k, pl.ds(row, LANES), :] = jnp.broadcast_to(value, (LANES, LANES)).T

    for owner in (diag, cross):
        stats_tile(owner * bigs)

    def conv_part(owner, low, size, slot):
        rows, target = pl.ds(pl.multiple_of(owner * block + low, size), size), pl.ds(slot, size)
        for g, lanes in enumerate(lanes_of):
            normed = (filtered[rows, lanes] - moments[0, rows, :]) * moments[1, rows, :] * conv_gain_ref[:, lanes]
            blend[target, width + g * LANES : width + (g + 1) * LANES] = (normed * jax.nn.sigmoid(normed)).astype(
                jnp.bfloat16
            )

    columns = merge.shape[1]
    turn = block // RETURNS

    def spread(size, put, first=0, last=2 * width):
        def step(j, carry):
            cols = pl.ds(pl.multiple_of(j * SPAN, SPAN), SPAN)
            put(cols, dot(blend[0:size, first:last], merge[first:last, cols]))
            return carry

        lax.fori_loop(0, columns // SPAN, step, 0)

    for one in fetched[len(sources) :]:
        one.wait()
    conv_part(diag, 0, turn, 0)
    conv_part(cross, 0, turn, turn)

    def put_early(cols, result):
        early[:, cols] = result

    spread(2 * turn, put_early, first=width)
    for k in range(3 if teams > 3 else 2, teams):
        relay(k, 0, number)

    for h in range(heads):
        state = chain_in[h].astype(jnp.float32)
        moved = state * jnp.exp(mate_log(h)) + pack_in[h].astype(jnp.float32)
        own_state[h] = jnp.where(side == 1, moved, state)

    def enter_chunk(c):
        for h in range(heads):
            enter[c, h] = (own_state[h] * decay[c, :, parts[h]] + prefix[c, h]).astype(jnp.bfloat16)

    for owner in (diag, cross):
        enter_chunk(owner * bigs)

    def rec_part(owner, low, size, slot):
        rows, target = pl.ds(pl.multiple_of(owner * block + low, size), size), pl.ds(slot, size)
        c = owner * bigs + low // CHUNK
        for h, part in enumerate(parts):
            rec = intra[rows, part] + dot(reach[rows, part], enter[c, h], ((1,), (1,)))
            rec = rec * lax.rsqrt(jnp.mean(rec * rec, axis=-1, keepdims=True) + head_epsilon) * head_gain_ref[...]
            gate = proj[RGATE, rows, part].astype(jnp.float32)
            blend[target, part] = (rec * (gate * jax.nn.sigmoid(gate))).astype(jnp.bfloat16)

    def finish_rows(owner, low, size, slot):
        rec_part(owner, low, size, slot)
        conv_part(owner, low, size, slot)

    lent, returned, close = {}, {}, []

    def settle(p):
        rows = pl.ds(p * turn, turn)
        lent[p].wait_recv()
        to_cross[rows, :] = (held[p % 2] + from_pair[0, rows, :].astype(jnp.float32)).astype(jnp.bfloat16)
        returned[p] = remote(
            to_cross.at[rows, :], from_cross.at[rows, :], back_send.at[1], back_sem.at[p - 1], "tp", cross
        )
        returned[p].start()

    late = (bigs - 1) * CHUNK // turn
    head_rows = pl.ds(0, turn)
    first_lent, first_returned = [], []
    rec_part(diag, 0, turn, 0)
    rec_part(cross, 0, turn, turn)
    for j in range(columns // SPAN):
        cols = slice(j * SPAN, (j + 1) * SPAN)
        result = dot(blend[0 : 2 * turn, 0:width], merge[0:width, cols]) + early[:, cols]
        to_pair[0, head_rows, cols] = result[0:turn].astype(jnp.bfloat16)
        held[0, :, cols] = result[turn : 2 * turn]
        first_lent.append(
            remote(
                to_pair.at[0, head_rows, cols], from_pair.at[0, head_rows, cols],
                first_send.at[0], first_recv.at[j], "tp", pair,
            )
        )
        first_lent[j].start()
    for j in range(columns // SPAN):
        cols = slice(j * SPAN, (j + 1) * SPAN)
        first_lent[j].wait_recv()
        to_cross[head_rows, cols] = (held[0, :, cols] + from_pair[0, head_rows, cols].astype(jnp.float32)).astype(
            jnp.bfloat16
        )
        first_returned.append(
            remote(
                to_cross.at[head_rows, cols], from_cross.at[head_rows, cols],
                first_send.at[1], first_done.at[0], "tp", cross,
            )
        )
        first_returned[j].start()
    for p in range(1, RETURNS):
        rows = pl.ds(p * turn, turn)
        if p == late:
            settle(p - 1)
            project(far_rows.at[bigs - 1], 4, len(sources), far_places(bigs - 1))
            query_part(far_chunks(bigs - 1))
            for owner in (diag, cross):
                for big in range(1, bigs):
                    stats_tile(owner * bigs + big)
                    enter_chunk(owner * bigs + big)
        finish_rows(diag, p * turn, turn, 0)
        finish_rows(cross, p * turn, turn, turn)
        if p > 1 and p != late:
            settle(p - 1)

        def put(cols, result, p=p, rows=rows):
            to_pair[0, rows, cols] = result[0:turn].astype(jnp.bfloat16)
            held[p % 2, :, cols] = result[turn : 2 * turn]

        spread(2 * turn, put)
        lent[p] = remote(
            to_pair.at[0, rows, :], from_pair.at[0, rows, :], back_send.at[0], lent_sem.at[p - 1], "tp", pair
        )
        lent[p].start()
    settle(RETURNS - 1)
    for owner in (pair, me):
        for big in range(bigs):
            stats_tile(owner * bigs + big)
            enter_chunk(owner * bigs + big)
    for big in range(bigs):
        rows = pl.ds(big * CHUNK, CHUNK)
        finish_rows(pair, big * CHUNK, CHUNK, 0)
        finish_rows(me, big * CHUNK, CHUNK, CHUNK)

        def put(cols, result, rows=rows):
            to_pair[1, rows, cols] = result[0:CHUNK].astype(jnp.bfloat16)
            mine[rows, cols] = result[CHUNK : 2 * CHUNK]

        spread(2 * CHUNK, put)
        close.append(
            remote(
                to_pair.at[1, rows, :], from_pair.at[1, rows, :], back_send.at[2], close_sem.at[big],
                "tp", pair,
            )
        )
        close[big].start()
    for big in range(bigs):
        rows = pl.ds(big * CHUNK, CHUNK)
        close[big].wait_recv()
        mine[rows, :] = mine[rows, :] + from_pair[1, rows, :].astype(jnp.float32)
    first_whole = remote(
        to_cross.at[head_rows, :], from_cross.at[head_rows, :], first_send.at[1], first_done.at[0], "tp", cross
    )
    for p in range(RETURNS):
        rows = pl.ds(p * turn, turn)
        (first_whole if p == 0 else returned[p]).wait_recv()
        out_ref[rows, :] = (mine[rows, :] + from_cross[rows, :].astype(jnp.float32)).astype(jnp.bfloat16)

    def sent(ref, sem):
        remote(ref, ref, sem, near_sem.at[0], "tp", pair).wait_send()

    rest = pl.ds(turn, block - turn)
    for k in range(3):
        sent(near_rows.at[0], send_sem.at[k])
    sent(pack, pack_send.at[0])
    logs.wait_send()
    sent(other_stats, stat_send.at[0])
    sent(to_pair.at[0, head_rows, :], first_send.at[0])
    sent(to_cross.at[head_rows, :], first_send.at[1])
    sent(to_pair.at[0, rest, :], back_send.at[0])
    sent(to_cross.at[rest, :], back_send.at[1])
    sent(to_pair.at[1], back_send.at[2])
    pl.when(ahead)(edge.wait_send)

    @pl.when(onward)
    def _():
        sent(chain_out, chain_send.at[0])


def on_device(
    tokens, norm_gain, w_query, w_forget, w_value, w_rgate, w_glu_value, w_glu_gate, forget_gap,
    decay_shift, head_gain, conv_taps, conv_gain, out_rec, out_conv,
):
    weights = (w_forget, w_value, w_glu_value, w_glu_gate, w_query, w_rgate)
    block, depth = tokens.shape
    width, columns = out_rec.shape
    head = head_gain.shape[0]
    heads = width // head
    rows = block * lax.axis_size("tp")
    groups = width // LANES
    chunks = rows // CHUNK
    turn = block // RETURNS
    bf16, f32 = jnp.bfloat16, jnp.float32
    vmem = lambda shape, kind: pltpu.VMEM(shape, kind)
    sems = lambda *shape: pltpu.SemaphoreType.DMA(shape)
    return pl.pallas_call(
        functools.partial(layer_kernel, head),
        in_specs=[pl.BlockSpec(memory_space=pl.ANY)] * 15,
        out_specs=pl.BlockSpec(memory_space=pltpu.VMEM),
        out_shape=pltpu.VMEM((block, columns), bf16),
        scratch_shapes=[
            vmem((1, depth), f32),
            vmem((1, width), f32),
            vmem((heads, rows), f32),
            vmem(conv_taps.shape, f32),
            vmem((1, width), f32),
            vmem((1, head), f32),
            vmem((block, depth), bf16),
            vmem((2, block, depth), bf16),
            vmem((block // CHUNK, 2 * CHUNK, depth), bf16),
            vmem((len(weights), depth, width), bf16),
            vmem((2 * width, columns), bf16),
            vmem((len(weights), rows, width), bf16),
            vmem((rows, width), f32),
            vmem((rows, width), bf16),
            vmem((chunks, heads, head, head), f32),
            vmem((chunks, 1, width), f32),
            vmem((chunks, 1, width), f32),
            vmem((chunks, heads, head, head), bf16),
            vmem((heads, head, head), f32),
            vmem((1, width), f32),
            vmem((heads, head, head), bf16),
            vmem((heads, head, head), bf16),
            vmem((1, width), f32),
            vmem((chunks, 1, width), f32),
            vmem((chunks, heads, head, head), f32),
            vmem((heads, head, head), f32),
            vmem((1, width), f32),
            vmem((heads, head, head), bf16),
            vmem((heads, head, head), bf16),
            vmem((2, REACH, width), bf16),
            vmem((groups, REACH + rows, LANES), f32),
            vmem((rows, width), f32),
            vmem((2, rows), f32),
            vmem((3, 2, rows), f32),
            vmem((2, rows, LANES), f32),
            vmem((2 * CHUNK, 2 * width), bf16),
            vmem((2 * turn, columns), f32),
            vmem((2, turn, columns), f32),
            vmem((2, block, columns), bf16),
            vmem((2, block, columns), bf16),
            vmem((block, columns), bf16),
            vmem((block, columns), bf16),
            vmem((block, columns), f32),
            sems(6),
            sems(2),
            sems(len(weights) + 2),
            sems(2),
            sems(3),
            sems(SENDS),
            sems(1),
            sems(block // CHUNK),
            sems(1),
            sems(heads, 2),
            sems(1),
            sems(heads, 2),
            sems(2),
            sems(1),
            sems(1),
            sems(3),
            sems(RETURNS - 1),
            sems(RETURNS - 1),
            sems(block // CHUNK),
            sems(2),
            sems(columns // SPAN),
            sems(1),
        ],
        compiler_params=pltpu.CompilerParams(
            collective_id=0, has_side_effects=True, vmem_limit_bytes=58000 * 1024
        ),
    )(
        norm_gain[None], forget_gap[None], decay_shift.T, conv_taps, conv_gain[None], head_gain[None],
        tokens, *weights, out_rec, out_conv,
    )


def solution(mesh):
    placed = (
        P(("sp", "tp"), None),
        P(),
        P(None, "tp"),
        P(None, "tp"),
        P(None, "tp"),
        P(None, "tp"),
        P(None, "tp"),
        P(None, "tp"),
        P("tp"),
        P("sp", "tp"),
        P(),
        P(None, "tp"),
        P("tp"),
        P("tp", None),
        P("tp", None),
    )
    return jax.shard_map(
        on_device, mesh=mesh, in_specs=placed, out_specs=P(("sp", "tp"), None), check_vma=False
    )
```

```python
import functools

import jax
import jax.numpy as jnp
from jax import lax
from jax.experimental import pallas as pl
from jax.experimental.pallas import tpu as pltpu
from jax.sharding import PartitionSpec as P

CHUNK = 128
SENDS = 8
RETURNS = 4
REACH = 32
TILE = 64
LANES = 128
SPAN = 512
STRAIGHT = 256
MESH = pl.DeviceIdType.MESH
FORGET, VALUE, GLU_VALUE, GLU_GATE, QUERY, RGATE = range(6)

norm_epsilon = 1e-05
head_epsilon = 1e-06


def dot(a, b, dims=((1,), (0,))):
    return lax.dot_general(a, b, (dims, ((), ())), preferred_element_type=jnp.float32)


def layer_norm(values, gain):
    widened = values.astype(jnp.float32)
    row_mean = jnp.mean(widened, axis=-1, keepdims=True)
    centred = widened - row_mean
    row_var = jnp.mean(centred * centred, axis=-1, keepdims=True)
    return centred * lax.rsqrt(row_var + norm_epsilon) * gain


def layer_kernel(
    head, gain_in, gap_in, shift_in, taps_in, conv_gain_in, head_gain_in,
    tokens_ref, w0, w1, w2, w3, w4, w5, rec_rows, conv_rows, out_ref,
    gain_ref, gap_ref, shift_ref, taps_ref, conv_gain_ref, head_gain_ref,
    raw, near_rows, far_rows, weight, merge, proj, intra, reach, local, closing, centre, enter,
    own_state, own_log, pack, pack_in, log_in, decay, prefix, group_state, group_log, chain_out, chain_in,
    rim, padded, filtered, own_stats, other_stats, moments,
    blend, early, straight_out, straight_in, held, to_pair, from_pair, to_cross, from_cross, mine,
    small_sem, raw_sem, weight_sem, log_sem, send_sem, cross_sem, near_sem, hand_sem, pack_send, pack_recv, chain_send, chain_recv,
    rim_sem, stat_send, stat_recv, back_send, lent_sem, back_sem, close_sem, first_send, first_recv, first_done, straight_sem,
):
    block, depth = tokens_ref.shape
    piece = block // SENDS
    raws = []
    for i, rows in enumerate((pl.ds(0, piece), pl.ds(piece, block - piece))):
        raws.append(pltpu.make_async_copy(tokens_ref.at[rows, :], raw.at[rows, :], raw_sem.at[i]))
        raws[i].start()
    smalls = []
    for i, (far, near) in enumerate((
        (gain_in, gain_ref), (gap_in, gap_ref), (shift_in, shift_ref), (taps_in, taps_ref),
        (conv_gain_in, conv_gain_ref), (head_gain_in, head_gain_ref),
    )):
        smalls.append(pltpu.make_async_copy(far, near, small_sem.at[i]))
        smalls[i].start()
    sources = (w0, w1, w2, w3, w4, w5)
    width = gap_ref.shape[1]
    fetched = [pltpu.make_async_copy(w, weight.at[i], weight_sem.at[i]) for i, w in enumerate(sources)]
    for i, w in enumerate((rec_rows, conv_rows)):
        fetched.append(
            pltpu.make_async_copy(w, merge.at[pl.ds(i * width, width), :], weight_sem.at[len(sources) + i])
        )
    me, count = lax.axis_index("tp"), lax.axis_size("sp")
    pair = me + 1 - 2 * lax.rem(me, 2)
    cross, diag = lax.rem(me + 2, 4), lax.rem(pair + 2, 4)
    at = lax.axis_index("sp")
    side, team, teams = lax.rem(at, 2), at // 2, count // 2
    mate = at + 1 - 2 * side
    barrier = pltpu.get_barrier_semaphore()
    for other in (pair, cross, diag):
        pl.semaphore_signal(barrier, inc=1, device_id={"tp": other}, device_id_type=MESH)
    pl.semaphore_signal(barrier, inc=1, device_id={"sp": mate}, device_id_type=MESH)

    @pl.when(team > 0)
    def _():
        pl.semaphore_signal(barrier, inc=1, device_id={"sp": at - 2}, device_id_type=MESH)

    @pl.when((team > 0) & (side == 0))
    def _():
        pl.semaphore_signal(barrier, inc=1, device_id={"sp": at - 1}, device_id_type=MESH)

    onward = team < teams - 1
    pl.semaphore_wait(barrier, jnp.where(onward, jnp.where(side == 1, 6, 5), 4))

    rows_all = proj.shape[1]
    heads, chunks = width // head, rows_all // CHUNK
    bigs = block // CHUNK
    per = CHUNK // piece
    channels = width * lax.axis_size("tp")
    lanes_of = [slice(g * LANES, (g + 1) * LANES) for g in range(width // LANES)]

    def remote(source, target, sends, recvs, axis, device):
        return pltpu.make_async_remote_copy(
            src_ref=source, dst_ref=target, send_sem=sends, recv_sem=recvs,
            device_id={axis: device}, device_id_type=MESH,
        )

    smalls[0].wait()

    crossing, nearby, handed = [], [], []
    for p in range(SENDS):
        rows = pl.ds(p * piece, piece)
        if p < 2:
            raws[p].wait()
        if p == 1:
            for one in fetched:
                one.start()
        near_rows[0, rows, :] = layer_norm(raw[rows, :], gain_ref[...]).astype(jnp.bfloat16)
        big, low = p // per, (p % per) * piece
        landing = far_rows.at[big, pl.ds(low, piece), :]
        crossing.append(remote(near_rows.at[0, rows, :], landing, send_sem.at[0], cross_sem.at[p], "tp", cross))
        nearby.append(
            remote(
                near_rows.at[0, rows, :], near_rows.at[1, rows, :], send_sem.at[1], near_sem.at[0], "tp", pair
            )
        )
        handed.append(
            remote(
                landing, far_rows.at[big, pl.ds(CHUNK + low, piece), :],
                send_sem.at[2], hand_sem.at[big], "tp", pair,
            )
        )
        crossing[p].start()
        nearby[p].start()
    for one in smalls[1:]:
        one.wait()

    def project(values, first, last, places, ready=False):
        def step(k, carry):
            for i in (first + 2 * k, first + 2 * k + 1):
                if ready:
                    for one in range(first, last):
                        pl.when(i == one)(fetched[one].wait)
            for i in (first + 2 * k, first + 2 * k + 1):
                result = dot(values[...], weight[i]).astype(jnp.bfloat16)
                for start, row, size in places:
                    proj[i, pl.ds(pl.multiple_of(row, CHUNK), size), :] = result[start : start + size]
            return carry

        lax.fori_loop(0, (last - first) // 2, step, 0)

    def pass_on(p):
        crossing[p].wait_recv()
        handed[p].start()

    def handed_in(big):
        part = far_rows.at[big, pl.ds(CHUNK, CHUNK), :]
        remote(part, part, send_sem.at[2], hand_sem.at[big], "tp", pair).wait_recv()

    row_at = lax.broadcasted_iota(jnp.int32, (CHUNK, CHUNK), 0)
    col_at = lax.broadcasted_iota(jnp.int32, (CHUNK, CHUNK), 1)
    causal = row_at >= col_at
    lower = jnp.where(causal, 1.0, 0.0).astype(jnp.bfloat16)
    lower = jnp.concatenate([lower, lower], axis=1)

    parts = [slice(h * head, (h + 1) * head) for h in range(heads)]

    def rows_of(c):
        return pl.ds(pl.multiple_of(c * CHUNK, CHUNK), CHUNK)

    def state_part(several, ready=None):
        keys, totals, values = [], [], []
        for k, c in enumerate(several):
            rows = rows_of(c)
            forget = proj[FORGET, rows, :] if ready is None else ready[0][k * CHUNK : (k + 1) * CHUNK]
            values.append(proj[VALUE, rows, :] if ready is None else ready[1][k * CHUNK : (k + 1) * CHUNK])
            key = gap_ref[...] * jax.nn.sigmoid(-forget.astype(jnp.float32))
            shift = [jnp.broadcast_to(shift_ref[h : h + 1, rows], (head, CHUNK)).T for h in range(heads)]
            log = jnp.log1p(-key) + jnp.concatenate(shift, axis=1)
            high = log.astype(jnp.bfloat16)
            low = (log - high.astype(jnp.float32)).astype(jnp.bfloat16)
            keys.append(key)
            totals.append(dot(lower, jnp.concatenate([high, low], axis=0)))
        for c, key, total, value in zip(several, keys, totals, values):
            rows = rows_of(c)
            last = total[CHUNK - 1 : CHUNK, :]
            middle = total[CHUNK // 2 - 1 : CHUNK // 2, :]
            total = total - middle
            key_mid = key * jnp.exp(-total)
            intra[rows, :] = total
            reach[rows, :] = key_mid.astype(jnp.bfloat16)
            key_end = (key_mid * jnp.exp(last - middle)).astype(jnp.bfloat16)
            for h, part in enumerate(parts):
                local[c, h] = dot(value[:, part], key_end[:, part], ((0,), (0,)))
            closing[c] = last
            centre[c] = middle

    def query_part(several):
        queries, scores = [], []
        for c in several:
            rows = rows_of(c)
            query = proj[QUERY, rows, :].astype(jnp.float32)
            query = query * jax.nn.sigmoid(query) * jnp.exp(intra[rows, :])
            queries.append(query)
            query = query.astype(jnp.bfloat16)
            scores.append([dot(query[:, part], reach[rows, part], ((1,), (1,))) for part in parts])
        for c, query, score in zip(several, queries, scores):
            rows = rows_of(c)
            for part, one in zip(parts, score):
                one = jnp.where(causal, one, 0.0).astype(jnp.bfloat16)
                intra[rows, part] = dot(one, proj[VALUE, rows, part])
            reach[rows, :] = (query * jnp.exp(centre[c])).astype(jnp.bfloat16)

    def chunk_loop(first, number):
        def step(i, carry):
            several = [first + 2 * i, first + 2 * i + 1]
            state_part(several)
            query_part(several)
            return carry

        lax.fori_loop(0, number // 2, step, 0)

    def mix(first, size):
        def step(i, carry):
            row = pl.multiple_of(first + i * TILE, TILE)
            for g, lanes in enumerate(lanes_of):
                gate = proj[GLU_GATE, pl.ds(row, TILE), lanes].astype(jnp.float32)
                value = proj[GLU_VALUE, pl.ds(row, TILE), lanes].astype(jnp.float32)
                mixed = (value * jax.nn.sigmoid(gate)).astype(jnp.bfloat16)
                padded[g, pl.ds(pl.multiple_of(row + REACH, 8), TILE), :] = mixed.astype(jnp.float32)
            return carry

        lax.fori_loop(0, size // TILE, step, 0)

    taps = taps_ref.shape[0]
    skip = REACH - taps + 1

    def filter_rows(row0, number):
        def step(i, carry):
            g, row = i // number, row0 + lax.rem(i, number) * TILE
            lanes = pl.ds(pl.multiple_of(g * LANES, LANES), LANES)
            total = jnp.zeros((TILE, LANES), jnp.float32)
            for j in range(taps):
                total = total + taps_ref[j : j + 1, lanes] * padded[g, pl.ds(row + (j + skip), TILE), :]
            filtered[pl.ds(pl.multiple_of(row, TILE), TILE), lanes] = total
            return carry

        lax.fori_loop(0, len(lanes_of) * number, step, 0)

    def tally(t):
        base = pl.multiple_of(t * LANES, LANES)
        sums = jnp.zeros((LANES, LANES), jnp.float32)
        squares = jnp.zeros((LANES, LANES), jnp.float32)
        for lanes in lanes_of:
            value = filtered[pl.ds(base, LANES), lanes]
            sums = sums + value
            squares = squares + value * value
        own_stats[0:1, pl.ds(base, LANES)] = jnp.sum(sums.T, axis=0, keepdims=True)
        own_stats[1:2, pl.ds(base, LANES)] = jnp.sum(squares.T, axis=0, keepdims=True)

    def filter_tile(t):
        filter_rows(pl.multiple_of(t * LANES, LANES), LANES // TILE)
        tally(t)

    def filter_loop(first, number):
        def step(i, carry):
            filter_tile(first + i)
            return carry

        lax.fori_loop(0, number, step, 0)

    chip = 2 * block
    own_half = (me // 2) * chip
    far_half = chip - own_half if rows_all == 2 * chip else lax.rem(own_half + chip, rows_all)
    half_tiles = chip // LANES

    project(near_rows.at[0], 0, len(sources), [(0, me * block, block)], ready=True)
    remote(near_rows.at[0], near_rows.at[1], send_sem.at[1], near_sem.at[0], "tp", pair).wait_recv()
    project(near_rows.at[1], 0, len(sources), [(0, pair * block, block)])
    pass_on(0)
    chunk_loop(own_half // CHUNK, chip // CHUNK)
    for p in range(1, per - 1):
        pass_on(p)
    mix(own_half, chip)
    filter_loop(own_half // LANES + 1, half_tiles - 2)
    pass_on(per - 1)

    def far_places(big):
        return [(0, cross * block + big * CHUNK, CHUNK), (CHUNK, diag * block + big * CHUNK, CHUNK)]

    def far_chunks(big):
        return [owner * bigs + big for owner in (cross, diag)]

    far_tile = far_half // LANES
    for big in range(bigs - 1):
        begin = big * per
        handed_in(big)
        project(far_rows.at[big], 0, len(sources), far_places(big))
        pass_on(begin + per)
        state_part(far_chunks(big))
        query_part(far_chunks(big))
        for _, row, size in far_places(big):
            mix(row, size)
        for p in range(begin + per + 1, begin + 2 * per - 2):
            pass_on(p)
        if big == bigs - 2:
            filter_tile(own_half // LANES + half_tiles - 1)
            for tile in (own_half // LANES, far_tile, far_tile + bigs):
                filter_rows(pl.multiple_of(tile * LANES + TILE, TILE), 1)
        for p in range(begin + 2 * per - 2, begin + 2 * per):
            pass_on(p)
    handed_in(bigs - 1)

    half = head // 2
    units = [(h, k) for h in range(heads) for k in range(2)]
    spans = (pl.ds(0, half), pl.ds(half, half))
    packs = [
        remote(pack.at[h, spans[k], :], pack_in.at[h, spans[k], :], pack_send.at[0], pack_recv.at[h, k], "sp", mate)
        for h, k in units
    ]
    def send_state(h):
        state = local[0, h]
        prefix[0, h] = jnp.zeros_like(state)
        for c in range(1, chunks):
            prefix[c, h] = state
            state = state * jnp.exp(closing[c, :, parts[h]]) + local[c, h]
        own_state[h] = state
        pack[h] = state.astype(jnp.bfloat16)
        packs[2 * h].start()
        packs[2 * h + 1].start()

    gates, inputs = [dot(far_rows[bigs - 1], weight[i]).astype(jnp.bfloat16) for i in (FORGET, VALUE)]
    for start, row, size in far_places(bigs - 1):
        proj[VALUE, pl.ds(pl.multiple_of(row, CHUNK), size), :] = inputs[start : start + size]
    state_part(far_chunks(bigs - 1), (gates, inputs))
    log = closing[0]
    for c in range(1, chunks):
        log = log + closing[c]
    own_log[...] = log
    logs = remote(own_log, log_in, log_sem.at[0], log_sem.at[1], "sp", mate)
    logs.start()
    for h in range(heads):
        send_state(h)
    log = jnp.zeros_like(log)
    for c in range(chunks):
        decay[c] = jnp.exp(log)
        log = log + closing[c]
    project(far_rows.at[bigs - 1], 2, 4, far_places(bigs - 1))
    for _, row, size in far_places(bigs - 1):
        mix(row, size)
    for g, lanes in enumerate(lanes_of):
        rim[0, :, lanes] = padded[g, rows_all : rows_all + REACH, :].astype(jnp.bfloat16)
    edge = remote(rim.at[0], rim.at[1], rim_sem.at[0], rim_sem.at[1], "sp", lax.rem(at + 1, count))
    ahead = onward | (side == 0)
    pl.when(ahead)(edge.start)

    links = [
        remote(
            chain_out.at[h, pl.ds(k * half, half), :], chain_in.at[h, pl.ds(k * half, half), :],
            chain_send.at[0], chain_recv.at[h, k], "sp", lax.rem(at + 2, count),
        )
        for h, k in units
    ]

    def mate_log(h):
        return log_in[:, parts[h]]

    def meet(u):
        h, k = units[u]
        some = pl.ds(k * half, half)
        if u == 0:
            logs.wait_recv()
        packs[u].wait_recv()
        theirs, log = pack_in[h, some, :].astype(jnp.float32), mate_log(h)
        ours, own = own_state[h, some, :], own_log[:, parts[h]]
        first = jnp.where(side == 0, ours, theirs)
        second = jnp.where(side == 0, theirs, ours)
        group = first * jnp.exp(jnp.where(side == 0, log, own)) + second
        group_state[h, some, :] = group
        if k == 0:
            group_log[:, parts[h]] = log + own

        @pl.when(team == 0)
        def _():
            chain_in[h, some, :] = jnp.zeros((half, head), jnp.bfloat16)
            chain_out[h, some, :] = group.astype(jnp.bfloat16)
            links[u].start()

    def relay(k, first, last):
        @pl.when(team == k)
        def _():
            for u in range(first, last):
                h, some = units[u][0], pl.ds(units[u][1] * half, half)
                links[u].wait_recv()
                if k < teams - 1:
                    step = chain_in[h, some, :].astype(jnp.float32) * jnp.exp(group_log[:, parts[h]])
                    chain_out[h, some, :] = (step + group_state[h, some, :]).astype(jnp.bfloat16)
                    links[u].start()

    def rim_in():
        pl.when(at > 0)(edge.wait_recv)
        for g, lanes in enumerate(lanes_of):
            padded[g, 0:REACH, :] = jnp.where(at > 0, rim[1, :, lanes].astype(jnp.float32), 0.0)

    stats = [
        remote(own_stats, other_stats.at[k - 1], stat_send.at[0], stat_recv.at[0], "tp", lax.rem(me + k, 4))
        for k in range(1, 4)
    ]
    number = len(units)
    def low_half(t):
        filter_rows(pl.multiple_of(t * LANES, LANES), 1)

    def high_half(t):
        filter_rows(pl.multiple_of(t * LANES + TILE, TILE), 1)
        tally(t)

    def low_rest(t):
        low_half(t)
        tally(t)

    whole_tiles = [far_tile + b * bigs + j for b in range(2) for j in range(1, bigs)]
    work = []
    for t in whole_tiles:
        work += [functools.partial(low_half, t), functools.partial(high_half, t)]
    work.insert(2, functools.partial(low_rest, far_tile + bigs))
    last_work = [rim_in, functools.partial(low_rest, own_half // LANES), functools.partial(low_rest, far_tile)]
    for _ in range(3):
        work.pop(0)()
    work += last_work
    for u in range(number):
        meet(u)
        if work and u != 3:
            work.pop(0)()
        if u >= 5:
            relay(1, u - 5, u - 4)
    for one in work:
        one()
    for one in stats:
        one.start()
    relay(1, number - 5, number)
    if teams > 3:
        relay(2, 0, number)
    all_stats = remote(other_stats, other_stats, stat_send.at[0], stat_recv.at[0], "tp", pair)
    all_stats.wait_recv()

    def stats_tile(i):
        row = pl.multiple_of(i * LANES, LANES)
        total = own_stats[:, pl.ds(row, LANES)]
        for k in range(3):
            total = total + other_stats[k, :, pl.ds(row, LANES)]
        mean = total[0:1] / channels
        scale = lax.rsqrt(total[1:2] / channels - mean * mean + norm_epsilon)
        for k, value in enumerate((mean, scale)):
            moments[k, pl.ds(row, LANES), :] = jnp.broadcast_to(value, (LANES, LANES)).T

    for owner in (diag, cross):
        stats_tile(owner * bigs)

    def conv_part(owner, low, size, slot):
        rows, target = pl.ds(pl.multiple_of(owner * block + low, size), size), pl.ds(slot, size)
        for g, lanes in enumerate(lanes_of):
            normed = (filtered[rows, lanes] - moments[0, rows, :]) * moments[1, rows, :] * conv_gain_ref[:, lanes]
            blend[target, width + g * LANES : width + (g + 1) * LANES] = (normed * jax.nn.sigmoid(normed)).astype(
                jnp.bfloat16
            )

    columns = merge.shape[1]
    turn = block // RETURNS

    def spread(size, put, first=0, last=2 * width):
        def step(j, carry):
            cols = pl.ds(pl.multiple_of(j * SPAN, SPAN), SPAN)
            put(cols, dot(blend[0:size, first:last], merge[first:last, cols]))
            return carry

        lax.fori_loop(0, columns // SPAN, step, 0)

    for one in fetched[len(sources) :]:
        one.wait()
    conv_part(diag, 0, turn, 0)
    conv_part(cross, 0, turn, turn)

    def put_early(cols, result):
        early[:, cols] = result

    spread(2 * turn, put_early, first=width)
    for k in range(3 if teams > 3 else 2, teams):
        relay(k, 0, number)

    for h in range(heads):
        state = chain_in[h].astype(jnp.float32)
        moved = state * jnp.exp(mate_log(h)) + pack_in[h].astype(jnp.float32)
        own_state[h] = jnp.where(side == 1, moved, state)

    def enter_chunk(c):
        for h in range(heads):
            enter[c, h] = (own_state[h] * decay[c, :, parts[h]] + prefix[c, h]).astype(jnp.bfloat16)

    for owner in (diag, cross):
        enter_chunk(owner * bigs)

    def rec_part(owner, low, size, slot):
        rows, target = pl.ds(pl.multiple_of(owner * block + low, size), size), pl.ds(slot, size)
        c = owner * bigs + low // CHUNK
        for h, part in enumerate(parts):
            rec = intra[rows, part] + dot(reach[rows, part], enter[c, h], ((1,), (1,)))
            rec = rec * lax.rsqrt(jnp.mean(rec * rec, axis=-1, keepdims=True) + head_epsilon) * head_gain_ref[...]
            gate = proj[RGATE, rows, part].astype(jnp.float32)
            blend[target, part] = (rec * (gate * jax.nn.sigmoid(gate))).astype(jnp.bfloat16)

    def finish_rows(owner, low, size, slot):
        rec_part(owner, low, size, slot)
        conv_part(owner, low, size, slot)

    lent, returned, close = {}, {}, []

    def settle(p):
        rows = pl.ds(p * turn, turn)
        lent[p].wait_recv()
        to_cross[rows, :] = (held[p % 2] + from_pair[0, rows, :].astype(jnp.float32)).astype(jnp.bfloat16)
        returned[p] = remote(
            to_cross.at[rows, :], from_cross.at[rows, :], back_send.at[1], back_sem.at[p - 1], "tp", cross
        )
        returned[p].start()

    late = (bigs - 1) * CHUNK // turn
    head_rows = pl.ds(0, turn)
    first_lent, first_returned = [], []
    rec_part(diag, 0, turn, 0)
    rec_part(cross, 0, turn, turn)
    straight = [
        remote(straight_out.at[k], straight_in.at[k], straight_sem.at[0], straight_sem.at[1], "tp", device)
        for k, device in enumerate((cross, diag))
    ]
    splits = [slice(max(j * SPAN, STRAIGHT), (j + 1) * SPAN) for j in range(columns // SPAN)]
    for j, cols in enumerate(splits):
        wide = slice(j * SPAN, (j + 1) * SPAN)
        result = dot(blend[0 : 2 * turn, 0:width], merge[0:width, wide]) + early[:, wide]
        if j == 0:
            straight_out[0] = result[turn : 2 * turn, 0:STRAIGHT].astype(jnp.bfloat16)
            straight_out[1] = result[0:turn, 0:STRAIGHT].astype(jnp.bfloat16)
            for one in straight:
                one.start()
            result = result[:, STRAIGHT:]
        to_pair[0, head_rows, cols] = result[0:turn].astype(jnp.bfloat16)
        held[0, :, cols] = result[turn : 2 * turn]
        first_lent.append(
            remote(
                to_pair.at[0, head_rows, cols], from_pair.at[0, head_rows, cols],
                first_send.at[0], first_recv.at[j], "tp", pair,
            )
        )
        first_lent[j].start()
    for j, cols in enumerate(splits):
        first_lent[j].wait_recv()
        to_cross[head_rows, cols] = (held[0, :, cols] + from_pair[0, head_rows, cols].astype(jnp.float32)).astype(
            jnp.bfloat16
        )
        first_returned.append(
            remote(
                to_cross.at[head_rows, cols], from_cross.at[head_rows, cols],
                first_send.at[1], first_done.at[0], "tp", cross,
            )
        )
        first_returned[j].start()
    for p in range(1, RETURNS):
        rows = pl.ds(p * turn, turn)
        if p == late:
            settle(p - 1)
            project(far_rows.at[bigs - 1], 4, len(sources), far_places(bigs - 1))
            query_part(far_chunks(bigs - 1))
            for owner in (diag, cross):
                for big in range(1, bigs):
                    stats_tile(owner * bigs + big)
                    enter_chunk(owner * bigs + big)
        finish_rows(diag, p * turn, turn, 0)
        finish_rows(cross, p * turn, turn, turn)
        if p > 1 and p != late:
            settle(p - 1)

        def put(cols, result, p=p, rows=rows):
            to_pair[0, rows, cols] = result[0:turn].astype(jnp.bfloat16)
            held[p % 2, :, cols] = result[turn : 2 * turn]

        spread(2 * turn, put)
        lent[p] = remote(
            to_pair.at[0, rows, :], from_pair.at[0, rows, :], back_send.at[0], lent_sem.at[p - 1], "tp", pair
        )
        lent[p].start()
    settle(RETURNS - 1)
    for owner in (pair, me):
        for big in range(bigs):
            stats_tile(owner * bigs + big)
            enter_chunk(owner * bigs + big)
    for big in range(bigs):
        rows = pl.ds(big * CHUNK, CHUNK)
        finish_rows(pair, big * CHUNK, CHUNK, 0)
        finish_rows(me, big * CHUNK, CHUNK, CHUNK)

        def put(cols, result, rows=rows):
            to_pair[1, rows, cols] = result[0:CHUNK].astype(jnp.bfloat16)
            mine[rows, cols] = result[CHUNK : 2 * CHUNK]

        spread(2 * CHUNK, put)
        close.append(
            remote(
                to_pair.at[1, rows, :], from_pair.at[1, rows, :], back_send.at[2], close_sem.at[big],
                "tp", pair,
            )
        )
        close[big].start()
    for big in range(bigs):
        rows = pl.ds(big * CHUNK, CHUNK)
        close[big].wait_recv()
        mine[rows, :] = mine[rows, :] + from_pair[1, rows, :].astype(jnp.float32)
    summed = pl.ds(STRAIGHT, columns - STRAIGHT)
    first_whole = remote(
        to_cross.at[head_rows, summed], from_cross.at[head_rows, summed], first_send.at[1], first_done.at[0],
        "tp", cross,
    )
    remote(straight_in, straight_in, straight_sem.at[0], straight_sem.at[1], "tp", cross).wait_recv()
    across = straight_in[0].astype(jnp.float32) + straight_in[1].astype(jnp.float32)
    out_ref[head_rows, 0:STRAIGHT] = (mine[head_rows, 0:STRAIGHT] + across).astype(jnp.bfloat16)
    for p in range(RETURNS):
        rows = pl.ds(p * turn, turn)
        (first_whole if p == 0 else returned[p]).wait_recv()
        cols = summed if p == 0 else pl.ds(0, columns)
        out_ref[rows, cols] = (mine[rows, cols] + from_cross[rows, cols].astype(jnp.float32)).astype(jnp.bfloat16)

    def sent(ref, sem):
        remote(ref, ref, sem, near_sem.at[0], "tp", pair).wait_send()

    rest = pl.ds(turn, block - turn)
    for k in range(3):
        sent(near_rows.at[0], send_sem.at[k])
    sent(pack, pack_send.at[0])
    logs.wait_send()
    sent(other_stats, stat_send.at[0])
    sent(to_pair.at[0, head_rows, summed], first_send.at[0])
    sent(to_cross.at[head_rows, summed], first_send.at[1])
    sent(straight_in, straight_sem.at[0])
    sent(to_pair.at[0, rest, :], back_send.at[0])
    sent(to_cross.at[rest, :], back_send.at[1])
    sent(to_pair.at[1], back_send.at[2])
    pl.when(ahead)(edge.wait_send)

    @pl.when(onward)
    def _():
        sent(chain_out, chain_send.at[0])


def on_device(
    tokens, norm_gain, w_query, w_forget, w_value, w_rgate, w_glu_value, w_glu_gate, forget_gap,
    decay_shift, head_gain, conv_taps, conv_gain, out_rec, out_conv,
):
    weights = (w_forget, w_value, w_glu_value, w_glu_gate, w_query, w_rgate)
    block, depth = tokens.shape
    width, columns = out_rec.shape
    head = head_gain.shape[0]
    heads = width // head
    rows = block * lax.axis_size("tp")
    groups = width // LANES
    chunks = rows // CHUNK
    turn = block // RETURNS
    bf16, f32 = jnp.bfloat16, jnp.float32
    vmem = lambda shape, kind: pltpu.VMEM(shape, kind)
    sems = lambda *shape: pltpu.SemaphoreType.DMA(shape)
    return pl.pallas_call(
        functools.partial(layer_kernel, head),
        in_specs=[pl.BlockSpec(memory_space=pl.ANY)] * 15,
        out_specs=pl.BlockSpec(memory_space=pltpu.VMEM),
        out_shape=pltpu.VMEM((block, columns), bf16),
        scratch_shapes=[
            vmem((1, depth), f32),
            vmem((1, width), f32),
            vmem((heads, rows), f32),
            vmem(conv_taps.shape, f32),
            vmem((1, width), f32),
            vmem((1, head), f32),
            vmem((block, depth), bf16),
            vmem((2, block, depth), bf16),
            vmem((block // CHUNK, 2 * CHUNK, depth), bf16),
            vmem((len(weights), depth, width), bf16),
            vmem((2 * width, columns), bf16),
            vmem((len(weights), rows, width), bf16),
            vmem((rows, width), f32),
            vmem((rows, width), bf16),
            vmem((chunks, heads, head, head), f32),
            vmem((chunks, 1, width), f32),
            vmem((chunks, 1, width), f32),
            vmem((chunks, heads, head, head), bf16),
            vmem((heads, head, head), f32),
            vmem((1, width), f32),
            vmem((heads, head, head), bf16),
            vmem((heads, head, head), bf16),
            vmem((1, width), f32),
            vmem((chunks, 1, width), f32),
            vmem((chunks, heads, head, head), f32),
            vmem((heads, head, head), f32),
            vmem((1, width), f32),
            vmem((heads, head, head), bf16),
            vmem((heads, head, head), bf16),
            vmem((2, REACH, width), bf16),
            vmem((groups, REACH + rows, LANES), f32),
            vmem((rows, width), f32),
            vmem((2, rows), f32),
            vmem((3, 2, rows), f32),
            vmem((2, rows, LANES), f32),
            vmem((2 * CHUNK, 2 * width), bf16),
            vmem((2 * turn, columns), f32),
            vmem((2, turn, STRAIGHT), bf16),
            vmem((2, turn, STRAIGHT), bf16),
            vmem((2, turn, columns), f32),
            vmem((2, block, columns), bf16),
            vmem((2, block, columns), bf16),
            vmem((block, columns), bf16),
            vmem((block, columns), bf16),
            vmem((block, columns), f32),
            sems(6),
            sems(2),
            sems(len(weights) + 2),
            sems(2),
            sems(3),
            sems(SENDS),
            sems(1),
            sems(block // CHUNK),
            sems(1),
            sems(heads, 2),
            sems(1),
            sems(heads, 2),
            sems(2),
            sems(1),
            sems(1),
            sems(3),
            sems(RETURNS - 1),
            sems(RETURNS - 1),
            sems(block // CHUNK),
            sems(2),
            sems(columns // SPAN),
            sems(1),
            sems(2),
        ],
        compiler_params=pltpu.CompilerParams(
            collective_id=0, has_side_effects=True, vmem_limit_bytes=58000 * 1024
        ),
    )(
        norm_gain[None], forget_gap[None], decay_shift.T, conv_taps, conv_gain[None], head_gain[None],
        tokens, *weights, out_rec, out_conv,
    )


def solution(mesh):
    placed = (
        P(("sp", "tp"), None),
        P(),
        P(None, "tp"),
        P(None, "tp"),
        P(None, "tp"),
        P(None, "tp"),
        P(None, "tp"),
        P(None, "tp"),
        P("tp"),
        P("sp", "tp"),
        P(),
        P(None, "tp"),
        P("tp"),
        P("tp", None),
        P("tp", None),
    )
    return jax.shard_map(
        on_device, mesh=mesh, in_specs=placed, out_specs=P(("sp", "tp"), None), check_vma=False
    )
```

```python
import functools

import jax
import jax.numpy as jnp
from jax import lax
from jax.experimental import pallas as pl
from jax.experimental.pallas import tpu as pltpu
from jax.sharding import PartitionSpec as P

CHUNK = 128
SENDS = 8
RETURNS = 4
REACH = 32
TILE = 64
LANES = 128
SPAN = 512
STRAIGHT = 256
MESH = pl.DeviceIdType.MESH
FORGET, VALUE, GLU_VALUE, GLU_GATE, QUERY, RGATE = range(6)

norm_epsilon = 1e-05
head_epsilon = 1e-06


def dot(a, b, dims=((1,), (0,))):
    return lax.dot_general(a, b, (dims, ((), ())), preferred_element_type=jnp.float32)


def layer_norm(values, gain):
    widened = values.astype(jnp.float32)
    row_mean = jnp.mean(widened, axis=-1, keepdims=True)
    centred = widened - row_mean
    row_var = jnp.mean(centred * centred, axis=-1, keepdims=True)
    return centred * lax.rsqrt(row_var + norm_epsilon) * gain


def layer_kernel(
    head, gain_in, gap_in, shift_in, taps_in, conv_gain_in, head_gain_in,
    tokens_ref, w0, w1, w2, w3, w4, w5, rec_rows, conv_rows, out_ref,
    gain_ref, gap_ref, shift_ref, taps_ref, conv_gain_ref, head_gain_ref,
    raw, near_rows, far_rows, weight, merge, proj, intra, reach, local, closing, centre, enter,
    own_state, own_log, pack, pack_in, log_in, decay, prefix, group_state, group_log, chain_out, chain_in,
    rim, padded, filtered, own_stats, other_stats, moments,
    blend, early, straight_out, straight_in, held, to_pair, from_pair, to_cross, from_cross, mine,
    small_sem, raw_sem, weight_sem, log_sem, send_sem, cross_sem, near_sem, hand_sem, pack_send, pack_recv, chain_send, chain_recv,
    rim_sem, stat_send, stat_recv, back_send, lent_sem, back_sem, close_sem, first_send, first_recv, first_done, straight_sem,
):
    block, depth = tokens_ref.shape
    piece = block // SENDS
    raws = []
    for i, rows in enumerate((pl.ds(0, piece), pl.ds(piece, block - piece))):
        raws.append(pltpu.make_async_copy(tokens_ref.at[rows, :], raw.at[rows, :], raw_sem.at[i]))
        raws[i].start()
    smalls = []
    for i, (far, near) in enumerate((
        (gain_in, gain_ref), (gap_in, gap_ref), (shift_in, shift_ref), (taps_in, taps_ref),
        (conv_gain_in, conv_gain_ref), (head_gain_in, head_gain_ref),
    )):
        smalls.append(pltpu.make_async_copy(far, near, small_sem.at[i]))
        smalls[i].start()
    sources = (w0, w1, w2, w3, w4, w5)
    width = gap_ref.shape[1]
    fetched = [pltpu.make_async_copy(w, weight.at[i], weight_sem.at[i]) for i, w in enumerate(sources)]
    for i, w in enumerate((rec_rows, conv_rows)):
        fetched.append(
            pltpu.make_async_copy(w, merge.at[pl.ds(i * width, width), :], weight_sem.at[len(sources) + i])
        )
    me, count = lax.axis_index("tp"), lax.axis_size("sp")
    pair = me + 1 - 2 * lax.rem(me, 2)
    cross, diag = lax.rem(me + 2, 4), lax.rem(pair + 2, 4)
    at = lax.axis_index("sp")
    side, team, teams = lax.rem(at, 2), at // 2, count // 2
    mate = at + 1 - 2 * side
    barrier = pltpu.get_barrier_semaphore()
    for other in (pair, cross, diag):
        pl.semaphore_signal(barrier, inc=1, device_id={"tp": other}, device_id_type=MESH)
    pl.semaphore_signal(barrier, inc=1, device_id={"sp": mate}, device_id_type=MESH)

    @pl.when(team > 0)
    def _():
        pl.semaphore_signal(barrier, inc=1, device_id={"sp": at - 2}, device_id_type=MESH)

    @pl.when((team > 0) & (side == 0))
    def _():
        pl.semaphore_signal(barrier, inc=1, device_id={"sp": at - 1}, device_id_type=MESH)

    onward = team < teams - 1

    rows_all = proj.shape[1]
    heads, chunks = width // head, rows_all // CHUNK
    bigs = block // CHUNK
    per = CHUNK // piece
    channels = width * lax.axis_size("tp")
    lanes_of = [slice(g * LANES, (g + 1) * LANES) for g in range(width // LANES)]

    def remote(source, target, sends, recvs, axis, device):
        return pltpu.make_async_remote_copy(
            src_ref=source, dst_ref=target, send_sem=sends, recv_sem=recvs,
            device_id={axis: device}, device_id_type=MESH,
        )


    def norm_rows(p):
        rows = pl.ds(p * piece, piece)
        if p < 2:
            raws[p].wait()
        if p == 1:
            for one in fetched:
                one.start()
        near_rows[0, rows, :] = layer_norm(raw[rows, :], gain_ref[...]).astype(jnp.bfloat16)

    smalls[0].wait()
    norm_rows(0)
    pl.semaphore_wait(barrier, jnp.where(onward, jnp.where(side == 1, 6, 5), 4))

    crossing, nearby, handed = [], [], []
    for p in range(SENDS):
        rows = pl.ds(p * piece, piece)
        if p > 0:
            norm_rows(p)
        big, low = p // per, (p % per) * piece
        landing = far_rows.at[big, pl.ds(low, piece), :]
        crossing.append(remote(near_rows.at[0, rows, :], landing, send_sem.at[0], cross_sem.at[p], "tp", cross))
        nearby.append(
            remote(
                near_rows.at[0, rows, :], near_rows.at[1, rows, :], send_sem.at[1], near_sem.at[0], "tp", pair
            )
        )
        handed.append(
            remote(
                landing, far_rows.at[big, pl.ds(CHUNK + low, piece), :],
                send_sem.at[2], hand_sem.at[big], "tp", pair,
            )
        )
        if p < SENDS - 1:
            crossing[p].start()
        else:
            pl.when(lax.rem(me, 2) == 0)(crossing[p].start)
        nearby[p].start()
    for one in smalls[1:]:
        one.wait()

    def project(values, first, last, places, ready=False):
        def step(k, carry):
            for i in (first + 2 * k, first + 2 * k + 1):
                if ready:
                    for one in range(first, last):
                        pl.when(i == one)(fetched[one].wait)
            for i in (first + 2 * k, first + 2 * k + 1):
                result = dot(values[...], weight[i]).astype(jnp.bfloat16)
                for start, row, size in places:
                    proj[i, pl.ds(pl.multiple_of(row, CHUNK), size), :] = result[start : start + size]
            return carry

        lax.fori_loop(0, (last - first) // 2, step, 0)

    def pass_on(p):
        crossing[p].wait_recv()
        handed[p].start()

    def handed_in(big):
        part = far_rows.at[big, pl.ds(CHUNK, CHUNK), :]
        remote(part, part, send_sem.at[2], hand_sem.at[big], "tp", pair).wait_recv()

    row_at = lax.broadcasted_iota(jnp.int32, (CHUNK, CHUNK), 0)
    col_at = lax.broadcasted_iota(jnp.int32, (CHUNK, CHUNK), 1)
    causal = row_at >= col_at
    lower = jnp.where(causal, 1.0, 0.0).astype(jnp.bfloat16)
    lower = jnp.concatenate([lower, lower], axis=1)

    parts = [slice(h * head, (h + 1) * head) for h in range(heads)]

    def rows_of(c):
        return pl.ds(pl.multiple_of(c * CHUNK, CHUNK), CHUNK)

    def state_part(several, ready=None):
        keys, totals, values = [], [], []
        for k, c in enumerate(several):
            rows = rows_of(c)
            forget = proj[FORGET, rows, :] if ready is None else ready[0][k * CHUNK : (k + 1) * CHUNK]
            values.append(proj[VALUE, rows, :] if ready is None else ready[1][k * CHUNK : (k + 1) * CHUNK])
            key = gap_ref[...] * jax.nn.sigmoid(-forget.astype(jnp.float32))
            shift = [jnp.broadcast_to(shift_ref[h : h + 1, rows], (head, CHUNK)).T for h in range(heads)]
            log = jnp.log1p(-key) + jnp.concatenate(shift, axis=1)
            high = log.astype(jnp.bfloat16)
            low = (log - high.astype(jnp.float32)).astype(jnp.bfloat16)
            keys.append(key)
            totals.append(dot(lower, jnp.concatenate([high, low], axis=0)))
        for c, key, total, value in zip(several, keys, totals, values):
            rows = rows_of(c)
            last = total[CHUNK - 1 : CHUNK, :]
            middle = total[CHUNK // 2 - 1 : CHUNK // 2, :]
            total = total - middle
            key_mid = key * jnp.exp(-total)
            intra[rows, :] = total
            reach[rows, :] = key_mid.astype(jnp.bfloat16)
            key_end = (key_mid * jnp.exp(last - middle)).astype(jnp.bfloat16)
            for h, part in enumerate(parts):
                local[c, h] = dot(value[:, part], key_end[:, part], ((0,), (0,)))
            closing[c] = last
            centre[c] = middle

    def query_part(several):
        queries, scores = [], []
        for c in several:
            rows = rows_of(c)
            query = proj[QUERY, rows, :].astype(jnp.float32)
            query = query * jax.nn.sigmoid(query) * jnp.exp(intra[rows, :])
            queries.append(query)
            query = query.astype(jnp.bfloat16)
            scores.append([dot(query[:, part], reach[rows, part], ((1,), (1,))) for part in parts])
        for c, query, score in zip(several, queries, scores):
            rows = rows_of(c)
            for part, one in zip(parts, score):
                one = jnp.where(causal, one, 0.0).astype(jnp.bfloat16)
                intra[rows, part] = dot(one, proj[VALUE, rows, part])
            reach[rows, :] = (query * jnp.exp(centre[c])).astype(jnp.bfloat16)

    def chunk_loop(first, number):
        def step(i, carry):
            several = [first + 2 * i, first + 2 * i + 1]
            state_part(several)
            query_part(several)
            return carry

        lax.fori_loop(0, number // 2, step, 0)

    def mix(first, size):
        def step(i, carry):
            row = pl.multiple_of(first + i * TILE, TILE)
            for g, lanes in enumerate(lanes_of):
                gate = proj[GLU_GATE, pl.ds(row, TILE), lanes].astype(jnp.float32)
                value = proj[GLU_VALUE, pl.ds(row, TILE), lanes].astype(jnp.float32)
                mixed = (value * jax.nn.sigmoid(gate)).astype(jnp.bfloat16)
                padded[g, pl.ds(pl.multiple_of(row + REACH, 8), TILE), :] = mixed.astype(jnp.float32)
            return carry

        lax.fori_loop(0, size // TILE, step, 0)

    taps = taps_ref.shape[0]
    skip = REACH - taps + 1

    def filter_rows(row0, number):
        def step(i, carry):
            g, row = i // number, row0 + lax.rem(i, number) * TILE
            lanes = pl.ds(pl.multiple_of(g * LANES, LANES), LANES)
            total = jnp.zeros((TILE, LANES), jnp.float32)
            for j in range(taps):
                total = total + taps_ref[j : j + 1, lanes] * padded[g, pl.ds(row + (j + skip), TILE), :]
            filtered[pl.ds(pl.multiple_of(row, TILE), TILE), lanes] = total
            return carry

        lax.fori_loop(0, len(lanes_of) * number, step, 0)

    def tally(t):
        base = pl.multiple_of(t * LANES, LANES)
        sums = jnp.zeros((LANES, LANES), jnp.float32)
        squares = jnp.zeros((LANES, LANES), jnp.float32)
        for lanes in lanes_of:
            value = filtered[pl.ds(base, LANES), lanes]
            sums = sums + value
            squares = squares + value * value
        own_stats[0:1, pl.ds(base, LANES)] = jnp.sum(sums.T, axis=0, keepdims=True)
        own_stats[1:2, pl.ds(base, LANES)] = jnp.sum(squares.T, axis=0, keepdims=True)

    def filter_tile(t):
        filter_rows(pl.multiple_of(t * LANES, LANES), LANES // TILE)
        tally(t)

    def filter_loop(first, number):
        def step(i, carry):
            filter_tile(first + i)
            return carry

        lax.fori_loop(0, number, step, 0)

    chip = 2 * block
    own_half = (me // 2) * chip
    far_half = chip - own_half if rows_all == 2 * chip else lax.rem(own_half + chip, rows_all)
    half_tiles = chip // LANES

    project(near_rows.at[0], 0, len(sources), [(0, me * block, block)], ready=True)
    remote(near_rows.at[0], near_rows.at[1], send_sem.at[1], near_sem.at[0], "tp", pair).wait_recv()
    project(near_rows.at[1], 0, len(sources), [(0, pair * block, block)])
    pass_on(0)
    chunk_loop(own_half // CHUNK, chip // CHUNK)
    for p in range(1, per - 1):
        pass_on(p)
    mix(own_half, chip)
    filter_loop(own_half // LANES + 1, half_tiles - 2)
    pass_on(per - 1)

    def far_places(big):
        return [(0, cross * block + big * CHUNK, CHUNK), (CHUNK, diag * block + big * CHUNK, CHUNK)]

    def far_chunks(big):
        return [owner * bigs + big for owner in (cross, diag)]

    far_tile = far_half // LANES
    for big in range(bigs - 1):
        begin = big * per
        handed_in(big)
        project(far_rows.at[big], 0, len(sources), far_places(big))
        pass_on(begin + per)
        state_part(far_chunks(big))
        query_part(far_chunks(big))
        for _, row, size in far_places(big):
            mix(row, size)
        for p in range(begin + per + 1, begin + 2 * per - 2):
            pass_on(p)
        if big == bigs - 2:
            pl.when(lax.rem(me, 2) == 1)(crossing[SENDS - 1].start)
            filter_tile(own_half // LANES + half_tiles - 1)
            for tile in (own_half // LANES, far_tile, far_tile + bigs):
                filter_rows(pl.multiple_of(tile * LANES + TILE, TILE), 1)
        for p in range(begin + 2 * per - 2, begin + 2 * per):
            pass_on(p)
    handed_in(bigs - 1)

    half = head // 2
    units = [(h, k) for h in range(heads) for k in range(2)]
    spans = (pl.ds(0, half), pl.ds(half, half))
    packs = [
        remote(pack.at[h, spans[k], :], pack_in.at[h, spans[k], :], pack_send.at[0], pack_recv.at[h, k], "sp", mate)
        for h, k in units
    ]
    def send_state(h):
        state = local[0, h]
        prefix[0, h] = jnp.zeros_like(state)
        for c in range(1, chunks):
            prefix[c, h] = state
            state = state * jnp.exp(closing[c, :, parts[h]]) + local[c, h]
        own_state[h] = state
        pack[h] = state.astype(jnp.bfloat16)
        packs[2 * h].start()
        packs[2 * h + 1].start()

    gates, inputs = [dot(far_rows[bigs - 1], weight[i]).astype(jnp.bfloat16) for i in (FORGET, VALUE)]
    for start, row, size in far_places(bigs - 1):
        proj[VALUE, pl.ds(pl.multiple_of(row, CHUNK), size), :] = inputs[start : start + size]
    state_part(far_chunks(bigs - 1), (gates, inputs))
    log = closing[0]
    for c in range(1, chunks):
        log = log + closing[c]
    own_log[...] = log
    logs = remote(own_log, log_in, log_sem.at[0], log_sem.at[1], "sp", mate)
    logs.start()
    for h in range(heads):
        send_state(h)
    log = jnp.zeros_like(log)
    for c in range(chunks):
        decay[c] = jnp.exp(log)
        log = log + closing[c]
    project(far_rows.at[bigs - 1], 2, 4, far_places(bigs - 1))
    for _, row, size in far_places(bigs - 1):
        mix(row, size)
    for g, lanes in enumerate(lanes_of):
        rim[0, :, lanes] = padded[g, rows_all : rows_all + REACH, :].astype(jnp.bfloat16)
    edge = remote(rim.at[0], rim.at[1], rim_sem.at[0], rim_sem.at[1], "sp", lax.rem(at + 1, count))
    ahead = onward | (side == 0)
    pl.when(ahead)(edge.start)

    links = [
        remote(
            chain_out.at[h, pl.ds(k * half, half), :], chain_in.at[h, pl.ds(k * half, half), :],
            chain_send.at[0], chain_recv.at[h, k], "sp", lax.rem(at + 2, count),
        )
        for h, k in units
    ]

    def mate_log(h):
        return log_in[:, parts[h]]

    def meet(u):
        h, k = units[u]
        some = pl.ds(k * half, half)
        if u == 0:
            logs.wait_recv()
        packs[u].wait_recv()
        theirs, log = pack_in[h, some, :].astype(jnp.float32), mate_log(h)
        ours, own = own_state[h, some, :], own_log[:, parts[h]]
        first = jnp.where(side == 0, ours, theirs)
        second = jnp.where(side == 0, theirs, ours)
        group = first * jnp.exp(jnp.where(side == 0, log, own)) + second
        group_state[h, some, :] = group
        if k == 0:
            group_log[:, parts[h]] = log + own

        @pl.when(team == 0)
        def _():
            chain_in[h, some, :] = jnp.zeros((half, head), jnp.bfloat16)
            chain_out[h, some, :] = group.astype(jnp.bfloat16)
            links[u].start()

    def relay(k, first, last):
        @pl.when(team == k)
        def _():
            for u in range(first, last):
                h, some = units[u][0], pl.ds(units[u][1] * half, half)
                links[u].wait_recv()
                if k < teams - 1:
                    step = chain_in[h, some, :].astype(jnp.float32) * jnp.exp(group_log[:, parts[h]])
                    chain_out[h, some, :] = (step + group_state[h, some, :]).astype(jnp.bfloat16)
                    links[u].start()

    def rim_in():
        pl.when(at > 0)(edge.wait_recv)
        for g, lanes in enumerate(lanes_of):
            padded[g, 0:REACH, :] = jnp.where(at > 0, rim[1, :, lanes].astype(jnp.float32), 0.0)

    stats = [
        remote(own_stats, other_stats.at[k - 1], stat_send.at[0], stat_recv.at[0], "tp", lax.rem(me + k, 4))
        for k in range(1, 4)
    ]
    number = len(units)
    def low_half(t):
        filter_rows(pl.multiple_of(t * LANES, LANES), 1)

    def high_half(t):
        filter_rows(pl.multiple_of(t * LANES + TILE, TILE), 1)
        tally(t)

    def low_rest(t):
        low_half(t)
        tally(t)

    whole_tiles = [far_tile + b * bigs + j for b in range(2) for j in range(1, bigs)]
    work = []
    for t in whole_tiles:
        work += [functools.partial(low_half, t), functools.partial(high_half, t)]
    work.insert(2, functools.partial(low_rest, far_tile + bigs))
    last_work = [rim_in, functools.partial(low_rest, own_half // LANES), functools.partial(low_rest, far_tile)]
    for _ in range(3):
        work.pop(0)()
    work += last_work
    for u in range(number):
        meet(u)
        if work and u != 3:
            work.pop(0)()
        if u >= 5:
            relay(1, u - 5, u - 4)
    for one in work:
        one()
    for one in stats:
        one.start()
    relay(1, number - 5, number)
    if teams > 3:
        relay(2, 0, number)
    all_stats = remote(other_stats, other_stats, stat_send.at[0], stat_recv.at[0], "tp", pair)
    all_stats.wait_recv()

    def stats_tile(i):
        row = pl.multiple_of(i * LANES, LANES)
        total = own_stats[:, pl.ds(row, LANES)]
        for k in range(3):
            total = total + other_stats[k, :, pl.ds(row, LANES)]
        mean = total[0:1] / channels
        scale = lax.rsqrt(total[1:2] / channels - mean * mean + norm_epsilon)
        for k, value in enumerate((mean, scale)):
            moments[k, pl.ds(row, LANES), :] = jnp.broadcast_to(value, (LANES, LANES)).T

    for owner in (diag, cross):
        stats_tile(owner * bigs)

    def conv_part(owner, low, size, slot):
        rows, target = pl.ds(pl.multiple_of(owner * block + low, size), size), pl.ds(slot, size)
        for g, lanes in enumerate(lanes_of):
            normed = (filtered[rows, lanes] - moments[0, rows, :]) * moments[1, rows, :] * conv_gain_ref[:, lanes]
            blend[target, width + g * LANES : width + (g + 1) * LANES] = (normed * jax.nn.sigmoid(normed)).astype(
                jnp.bfloat16
            )

    columns = merge.shape[1]
    turn = block // RETURNS

    def spread(size, put, first=0, last=2 * width):
        def step(j, carry):
            cols = pl.ds(pl.multiple_of(j * SPAN, SPAN), SPAN)
            put(cols, dot(blend[0:size, first:last], merge[first:last, cols]))
            return carry

        lax.fori_loop(0, columns // SPAN, step, 0)

    for one in fetched[len(sources) :]:
        one.wait()
    conv_part(diag, 0, turn, 0)
    conv_part(cross, 0, turn, turn)

    def put_early(cols, result):
        early[:, cols] = result

    spread(2 * turn, put_early, first=width)
    for k in range(3 if teams > 3 else 2, teams):
        relay(k, 0, number)

    for h in range(heads):
        state = chain_in[h].astype(jnp.float32)
        moved = state * jnp.exp(mate_log(h)) + pack_in[h].astype(jnp.float32)
        own_state[h] = jnp.where(side == 1, moved, state)

    def enter_chunk(c):
        for h in range(heads):
            enter[c, h] = (own_state[h] * decay[c, :, parts[h]] + prefix[c, h]).astype(jnp.bfloat16)

    for owner in (diag, cross):
        enter_chunk(owner * bigs)

    def rec_part(owner, low, size, slot):
        rows, target = pl.ds(pl.multiple_of(owner * block + low, size), size), pl.ds(slot, size)
        c = owner * bigs + low // CHUNK
        for h, part in enumerate(parts):
            rec = intra[rows, part] + dot(reach[rows, part], enter[c, h], ((1,), (1,)))
            rec = rec * lax.rsqrt(jnp.mean(rec * rec, axis=-1, keepdims=True) + head_epsilon) * head_gain_ref[...]
            gate = proj[RGATE, rows, part].astype(jnp.float32)
            blend[target, part] = (rec * (gate * jax.nn.sigmoid(gate))).astype(jnp.bfloat16)

    def finish_rows(owner, low, size, slot):
        rec_part(owner, low, size, slot)
        conv_part(owner, low, size, slot)

    lent, returned, close = {}, {}, []

    def settle(p):
        rows = pl.ds(p * turn, turn)
        lent[p].wait_recv()
        to_cross[rows, :] = (held[p % 2] + from_pair[0, rows, :].astype(jnp.float32)).astype(jnp.bfloat16)
        returned[p] = remote(
            to_cross.at[rows, :], from_cross.at[rows, :], back_send.at[1], back_sem.at[p - 1], "tp", cross
        )
        returned[p].start()

    late = (bigs - 1) * CHUNK // turn
    head_rows = pl.ds(0, turn)
    first_lent, first_returned = [], []
    rec_part(diag, 0, turn, 0)
    rec_part(cross, 0, turn, turn)
    straight = [
        remote(straight_out.at[k], straight_in.at[k], straight_sem.at[0], straight_sem.at[1], "tp", device)
        for k, device in enumerate((cross, diag))
    ]
    splits = [slice(max(j * SPAN, STRAIGHT), (j + 1) * SPAN) for j in range(columns // SPAN)]
    for j, cols in enumerate(splits):
        wide = slice(j * SPAN, (j + 1) * SPAN)
        result = dot(blend[0 : 2 * turn, 0:width], merge[0:width, wide]) + early[:, wide]
        if j == 0:
            straight_out[0] = result[turn : 2 * turn, 0:STRAIGHT].astype(jnp.bfloat16)
            straight_out[1] = result[0:turn, 0:STRAIGHT].astype(jnp.bfloat16)
            for one in straight:
                one.start()
            result = result[:, STRAIGHT:]
        to_pair[0, head_rows, cols] = result[0:turn].astype(jnp.bfloat16)
        held[0, :, cols] = result[turn : 2 * turn]
        first_lent.append(
            remote(
                to_pair.at[0, head_rows, cols], from_pair.at[0, head_rows, cols],
                first_send.at[0], first_recv.at[j], "tp", pair,
            )
        )
        first_lent[j].start()
    for j, cols in enumerate(splits):
        first_lent[j].wait_recv()
        to_cross[head_rows, cols] = (held[0, :, cols] + from_pair[0, head_rows, cols].astype(jnp.float32)).astype(
            jnp.bfloat16
        )
        first_returned.append(
            remote(
                to_cross.at[head_rows, cols], from_cross.at[head_rows, cols],
                first_send.at[1], first_done.at[0], "tp", cross,
            )
        )
        first_returned[j].start()
    for p in range(1, RETURNS):
        rows = pl.ds(p * turn, turn)
        if p == late:
            settle(p - 1)
            project(far_rows.at[bigs - 1], 4, len(sources), far_places(bigs - 1))
            query_part(far_chunks(bigs - 1))
            for owner in (diag, cross):
                for big in range(1, bigs):
                    stats_tile(owner * bigs + big)
                    enter_chunk(owner * bigs + big)
        finish_rows(diag, p * turn, turn, 0)
        finish_rows(cross, p * turn, turn, turn)
        if p > 1 and p != late:
            settle(p - 1)

        def put(cols, result, p=p, rows=rows):
            to_pair[0, rows, cols] = result[0:turn].astype(jnp.bfloat16)
            held[p % 2, :, cols] = result[turn : 2 * turn]

        spread(2 * turn, put)
        lent[p] = remote(
            to_pair.at[0, rows, :], from_pair.at[0, rows, :], back_send.at[0], lent_sem.at[p - 1], "tp", pair
        )
        lent[p].start()
    settle(RETURNS - 1)
    for owner in (pair, me):
        for big in range(bigs):
            stats_tile(owner * bigs + big)
            enter_chunk(owner * bigs + big)
    for big in range(bigs):
        rows = pl.ds(big * CHUNK, CHUNK)
        finish_rows(pair, big * CHUNK, CHUNK, 0)
        finish_rows(me, big * CHUNK, CHUNK, CHUNK)

        def put(cols, result, rows=rows):
            to_pair[1, rows, cols] = result[0:CHUNK].astype(jnp.bfloat16)
            mine[rows, cols] = result[CHUNK : 2 * CHUNK]

        spread(2 * CHUNK, put)
        close.append(
            remote(
                to_pair.at[1, rows, :], from_pair.at[1, rows, :], back_send.at[2], close_sem.at[big],
                "tp", pair,
            )
        )
        close[big].start()
    for big in range(bigs):
        rows = pl.ds(big * CHUNK, CHUNK)
        close[big].wait_recv()
        mine[rows, :] = mine[rows, :] + from_pair[1, rows, :].astype(jnp.float32)
    summed = pl.ds(STRAIGHT, columns - STRAIGHT)
    first_whole = remote(
        to_cross.at[head_rows, summed], from_cross.at[head_rows, summed], first_send.at[1], first_done.at[0],
        "tp", cross,
    )
    remote(straight_in, straight_in, straight_sem.at[0], straight_sem.at[1], "tp", cross).wait_recv()
    across = straight_in[0].astype(jnp.float32) + straight_in[1].astype(jnp.float32)
    out_ref[head_rows, 0:STRAIGHT] = (mine[head_rows, 0:STRAIGHT] + across).astype(jnp.bfloat16)
    for p in range(RETURNS):
        rows = pl.ds(p * turn, turn)
        (first_whole if p == 0 else returned[p]).wait_recv()
        cols = summed if p == 0 else pl.ds(0, columns)
        out_ref[rows, cols] = (mine[rows, cols] + from_cross[rows, cols].astype(jnp.float32)).astype(jnp.bfloat16)

    def sent(ref, sem):
        remote(ref, ref, sem, near_sem.at[0], "tp", pair).wait_send()

    rest = pl.ds(turn, block - turn)
    for k in range(3):
        sent(near_rows.at[0], send_sem.at[k])
    sent(pack, pack_send.at[0])
    logs.wait_send()
    sent(other_stats, stat_send.at[0])
    sent(to_pair.at[0, head_rows, summed], first_send.at[0])
    sent(to_cross.at[head_rows, summed], first_send.at[1])
    sent(straight_in, straight_sem.at[0])
    sent(to_pair.at[0, rest, :], back_send.at[0])
    sent(to_cross.at[rest, :], back_send.at[1])
    sent(to_pair.at[1], back_send.at[2])
    pl.when(ahead)(edge.wait_send)

    @pl.when(onward)
    def _():
        sent(chain_out, chain_send.at[0])


def on_device(
    tokens, norm_gain, w_query, w_forget, w_value, w_rgate, w_glu_value, w_glu_gate, forget_gap,
    decay_shift, head_gain, conv_taps, conv_gain, out_rec, out_conv,
):
    weights = (w_forget, w_value, w_glu_value, w_glu_gate, w_query, w_rgate)
    block, depth = tokens.shape
    width, columns = out_rec.shape
    head = head_gain.shape[0]
    heads = width // head
    rows = block * lax.axis_size("tp")
    groups = width // LANES
    chunks = rows // CHUNK
    turn = block // RETURNS
    bf16, f32 = jnp.bfloat16, jnp.float32
    vmem = lambda shape, kind: pltpu.VMEM(shape, kind)
    sems = lambda *shape: pltpu.SemaphoreType.DMA(shape)
    return pl.pallas_call(
        functools.partial(layer_kernel, head),
        in_specs=[pl.BlockSpec(memory_space=pl.ANY)] * 15,
        out_specs=pl.BlockSpec(memory_space=pltpu.VMEM),
        out_shape=pltpu.VMEM((block, columns), bf16),
        scratch_shapes=[
            vmem((1, depth), f32),
            vmem((1, width), f32),
            vmem((heads, rows), f32),
            vmem(conv_taps.shape, f32),
            vmem((1, width), f32),
            vmem((1, head), f32),
            vmem((block, depth), bf16),
            vmem((2, block, depth), bf16),
            vmem((block // CHUNK, 2 * CHUNK, depth), bf16),
            vmem((len(weights), depth, width), bf16),
            vmem((2 * width, columns), bf16),
            vmem((len(weights), rows, width), bf16),
            vmem((rows, width), f32),
            vmem((rows, width), bf16),
            vmem((chunks, heads, head, head), f32),
            vmem((chunks, 1, width), f32),
            vmem((chunks, 1, width), f32),
            vmem((chunks, heads, head, head), bf16),
            vmem((heads, head, head), f32),
            vmem((1, width), f32),
            vmem((heads, head, head), bf16),
            vmem((heads, head, head), bf16),
            vmem((1, width), f32),
            vmem((chunks, 1, width), f32),
            vmem((chunks, heads, head, head), f32),
            vmem((heads, head, head), f32),
            vmem((1, width), f32),
            vmem((heads, head, head), bf16),
            vmem((heads, head, head), bf16),
            vmem((2, REACH, width), bf16),
            vmem((groups, REACH + rows, LANES), f32),
            vmem((rows, width), f32),
            vmem((2, rows), f32),
            vmem((3, 2, rows), f32),
            vmem((2, rows, LANES), f32),
            vmem((2 * CHUNK, 2 * width), bf16),
            vmem((2 * turn, columns), f32),
            vmem((2, turn, STRAIGHT), bf16),
            vmem((2, turn, STRAIGHT), bf16),
            vmem((2, turn, columns), f32),
            vmem((2, block, columns), bf16),
            vmem((2, block, columns), bf16),
            vmem((block, columns), bf16),
            vmem((block, columns), bf16),
            vmem((block, columns), f32),
            sems(6),
            sems(2),
            sems(len(weights) + 2),
            sems(2),
            sems(3),
            sems(SENDS),
            sems(1),
            sems(block // CHUNK),
            sems(1),
            sems(heads, 2),
            sems(1),
            sems(heads, 2),
            sems(2),
            sems(1),
            sems(1),
            sems(3),
            sems(RETURNS - 1),
            sems(RETURNS - 1),
            sems(block // CHUNK),
            sems(2),
            sems(columns // SPAN),
            sems(1),
            sems(2),
        ],
        compiler_params=pltpu.CompilerParams(
            collective_id=0, has_side_effects=True, vmem_limit_bytes=58000 * 1024
        ),
    )(
        norm_gain[None], forget_gap[None], decay_shift.T, conv_taps, conv_gain[None], head_gain[None],
        tokens, *weights, out_rec, out_conv,
    )


def solution(mesh):
    placed = (
        P(("sp", "tp"), None),
        P(),
        P(None, "tp"),
        P(None, "tp"),
        P(None, "tp"),
        P(None, "tp"),
        P(None, "tp"),
        P(None, "tp"),
        P("tp"),
        P("sp", "tp"),
        P(),
        P(None, "tp"),
        P("tp"),
        P("tp", None),
        P("tp", None),
    )
    return jax.shard_map(
        on_device, mesh=mesh, in_specs=placed, out_specs=P(("sp", "tp"), None), check_vma=False
    )
```
